32 devices in a mesh: sp: 16 (over z, y, x), tp: 2 (over core).
Axes of the slice: x: 2, y: 2, z: 4, core: 2. Of those that a mesh axis runs over, the one named last changes fastest.
Arguments:
- tokens: bfloat16 [8192, 4096], P('sp', 'tp'), may hold values from -6 to 6
- norm_gain: float32 [4096], replicated, may hold values from 0.1 to 1.9
- w_query: bfloat16 [4096, 2048], P('sp', 'tp'), may hold values from -0.09375 to 0.09375
- w_key: bfloat16 [4096, 512], P('sp', 'tp'), may hold values from -0.09375 to 0.09375
- w_value: bfloat16 [4096, 512], P('sp', 'tp'), may hold values from -0.09375 to 0.09375
- w_pool_in: bfloat16 [4096, 2048], P('sp', 'tp'), may hold values from -0.09375 to 0.09375
- query_gain: float32 [64], replicated, may hold values from 0.4 to 9
- key_gain: float32 [64], replicated, may hold values from 0.4 to 9
- sinks: float32 [32], P('tp'), may hold values from 2 to 7
- w_mix: bfloat16 [8, 256, 256], P('tp'), may hold values from -0.375 to 0.375
- pool_scale: float32 [2048], P('tp'), may hold values from 0.1 to 1.9
- w_out_attn: bfloat16 [2048, 4096], P('sp', 'tp'), may hold values from -0.5 to 0.5
- w_out_pool: bfloat16 [2048, 4096], P('sp', 'tp'), may hold values from -0.125 to 0.125
Outputs:
- layer_out: bfloat16 [8192, 4096], P('sp', 'tp')
The draws below stay inside these ranges and needn't reach their ends.
All inputs are finite; a program needn't handle non-finite values.
Results may differ from the reference program's by a relative error of at most 0.0075.
The reference program's roundings to bfloat16 on the way count: a program that leaves them out, or rounds other values in their place, can miss the bound.
Values may be sent and summed in bfloat16 or wider, within the bound.
A program may use at most 128 MiB of HBM per device.

```python
import jax
import jax.numpy as jnp
from jax import lax

D = 4096
HEAD = 64
QHEADS = 32
KVHEADS = 8
POOL_GROUPS = 8
GROUP_DIM = 256
WINDOW = 128
TOKENS = 8192
ATTN_W = 2048
KV_W = 512
POOL_W = 2048


def draw_query_gain(key, part):
    subkey = jax.random.fold_in(key, 7)
    return jax.random.uniform(subkey, (HEAD,), jnp.float32, 0.4, 1.6)


def draw_key_gain(key, part):
    subkey = jax.random.fold_in(key, 11)
    return jax.random.uniform(subkey, (HEAD,), jnp.float32, 0.4, 1.6)


def level_of(stream_key, dims, split, low, high):
    loudness, own = 1.0, jax.random.fold_in(stream_key, 6)
    for dim, shards_of in split:
        steps = jnp.exp(jax.random.uniform(jax.random.fold_in(own, dim), (shards_of,), jnp.float32, low / len(split), high / len(split)))
        loudness = loudness * jnp.repeat(steps, dims[dim] // shards_of).reshape([-1 if axis == dim else 1 for axis in range(len(dims))])
    return loudness


def bell_draw(stream_key, shape, deviation, bound, split=(), kind=jnp.bfloat16):
    values = deviation * jax.random.normal(stream_key, shape, jnp.float32)
    if split:
        values = values * level_of(stream_key, shape, split, -0.22, 0.18)
    return jnp.clip(values, -bound, bound).astype(kind)


def setup_inputs(seed: int = 0) -> dict:
    seeds = jax.random.split(jax.random.key(seed), 14)
    tokens = bell_draw(seeds[0], (TOKENS, D), 1.0, 6.0, ((0, 16), (1, 2)))
    norm_gain = jnp.clip(1.0 + 0.18 * jax.random.normal(seeds[1], (D,), jnp.float32), 0.1, 1.9)
    w_query = bell_draw(seeds[2], (D, ATTN_W), D ** -0.5, 0.09375, ((0, 16), (1, 2)))
    w_key = bell_draw(seeds[3], (D, KV_W), D ** -0.5, 0.09375, ((0, 16), (1, 2)))
    w_value = bell_draw(seeds[4], (D, KV_W), D ** -0.5, 0.09375, ((0, 16), (1, 2)))
    w_pool_in = bell_draw(seeds[5], (D, POOL_W), D ** -0.5, 0.09375, ((0, 16), (1, 2)))
    query_gain = draw_query_gain(jax.random.fold_in(seeds[13], 71), 0)
    key_gain = draw_key_gain(jax.random.fold_in(seeds[13], 71), 0)
    sinks = jnp.clip(2.0 + 5.0 * jax.random.uniform(seeds[8], (QHEADS,), jnp.float32) ** level_of(seeds[8], (QHEADS,), ((0, 2),), -0.2, 0.2), 2.0, 7.0)
    w_mix = bell_draw(seeds[9], (POOL_GROUPS, GROUP_DIM, GROUP_DIM), GROUP_DIM ** -0.5, 0.375, ((0, 2),))
    pool_scale = jnp.clip(1.0 + 0.18 * jax.random.normal(seeds[10], (POOL_W,), jnp.float32), 0.1, 1.9)
    w_out_attn = bell_draw(seeds[11], (ATTN_W, D), (ATTN_W // 16) ** -0.5, 0.5, ((0, 16), (1, 2)))
    w_out_pool = bell_draw(seeds[12], (POOL_W, D), POOL_W ** -0.5, 0.125, ((0, 16), (1, 2)))
    return dict(tokens=tokens, norm_gain=norm_gain, w_query=w_query, w_key=w_key, w_value=w_value, w_pool_in=w_pool_in, query_gain=query_gain, key_gain=key_gain, sinks=sinks, w_mix=w_mix, pool_scale=pool_scale, w_out_attn=w_out_attn, w_out_pool=w_out_pool)


epsilon = 1e-06
longest_lag = 15

def row_norm(values, gain):
    return values * lax.rsqrt(lax.optimization_barrier(jnp.mean(values * values, axis=-1, keepdims=True)) + epsilon) * gain

def banded(source, blocks, padding):
    earlier = jnp.concatenate([padding, source[:-WINDOW]], axis=0).reshape(blocks, WINDOW, KVHEADS, HEAD)
    current = source.reshape(blocks, WINDOW, KVHEADS, HEAD)
    return jnp.concatenate([earlier, current], axis=1)

def reference(tokens, norm_gain, w_query, w_key, w_value, w_pool_in, query_gain, key_gain, sinks, w_mix, pool_scale, w_out_attn, w_out_pool):
    length = tokens.shape[0]
    normed = row_norm(tokens.astype(jnp.float32), norm_gain.astype(jnp.float32)).astype(jnp.bfloat16)
    queries = row_norm(jnp.dot(normed, w_query, preferred_element_type=jnp.float32).reshape(length, QHEADS, HEAD), query_gain.astype(jnp.float32)).astype(jnp.bfloat16)
    key_rows = row_norm(jnp.dot(normed, w_key, preferred_element_type=jnp.float32).reshape(length, KVHEADS, HEAD), key_gain.astype(jnp.float32)).astype(jnp.bfloat16)
    values = jnp.dot(normed, w_value, preferred_element_type=jnp.float32).astype(jnp.bfloat16).reshape(length, KVHEADS, HEAD)
    pool_in = jnp.dot(normed, w_pool_in, preferred_element_type=jnp.float32).astype(jnp.bfloat16)
    blocks = length // WINDOW
    per_kv = QHEADS // KVHEADS
    padding = jnp.zeros((WINDOW, KVHEADS, HEAD), jnp.bfloat16)
    band_keys = banded(key_rows, blocks, padding)
    band_values = banded(values, blocks, padding)
    query_blocks = queries.reshape(blocks, WINDOW, KVHEADS, per_kv, HEAD)
    query_index = jnp.arange(WINDOW)[:, None]
    key_index = jnp.arange(2 * WINDOW)[None, :]
    distance = query_index + WINDOW - key_index
    key_pos = jnp.arange(blocks)[:, None, None] * WINDOW - WINDOW + key_index[None]
    valid = (distance[None] >= 0) & (distance[None] < WINDOW) & (key_pos >= 0)
    sink_logit = sinks.astype(jnp.float32).reshape(KVHEADS, per_kv)

    def one_head(operands):
        head_queries, head_keys, head_values, head_sink = operands
        scores = jnp.einsum('bqgd,bjd->bgqj', head_queries.astype(jnp.float32), head_keys.astype(jnp.float32)) * HEAD ** (-0.5)
        scores = jnp.where(valid[:, None], scores, -1e+30)
        sink_col = head_sink[None, :, None, None]
        row_top = jnp.maximum(scores.max(axis=-1, keepdims=True), sink_col)
        lifted = jnp.exp(scores - row_top)
        weights = (lifted / (lifted.sum(axis=-1, keepdims=True) + jnp.exp(sink_col - row_top))).astype(jnp.bfloat16)
        return jnp.einsum('bgqj,bjd->bqgd', weights.astype(jnp.float32), head_values.astype(jnp.float32)).astype(jnp.bfloat16)
    head_out = lax.map(one_head, (jnp.moveaxis(query_blocks, 2, 0), jnp.moveaxis(band_keys, 2, 0), jnp.moveaxis(band_values, 2, 0), sink_logit))
    attended = jnp.transpose(head_out, (1, 2, 0, 3, 4)).reshape(length, ATTN_W)
    spans = 2 ** (1 + jnp.arange(POOL_W) // GROUP_DIM % 4)
    pool_wide = pool_in.astype(jnp.float32)
    extended = jnp.concatenate([jnp.zeros((longest_lag, POOL_W), jnp.float32), pool_wide], axis=0)
    window_sum = jnp.zeros((length, POOL_W), jnp.float32)
    for back_step in range(longest_lag + 1):
        shifted = extended[longest_lag - back_step:longest_lag - back_step + length]
        window_sum = window_sum + jnp.where(back_step < spans[None, :], shifted, 0.0)
    divisor = jnp.minimum(jnp.arange(1, length + 1).astype(jnp.float32)[:, None], spans.astype(jnp.float32)[None, :])
    contrast = (window_sum / divisor - pool_wide).astype(jnp.bfloat16)
    mixed = jnp.einsum('tgc,gcd->tgd', contrast.reshape(length, POOL_GROUPS, GROUP_DIM).astype(jnp.float32), w_mix.astype(jnp.float32)).reshape(length, POOL_W)
    pooled = (mixed * pool_scale.astype(jnp.float32)).astype(jnp.bfloat16)
    result = jnp.dot(attended, w_out_attn, preferred_element_type=jnp.float32) + jnp.dot(pooled, w_out_pool, preferred_element_type=jnp.float32)
    return result.astype(jnp.bfloat16)
```

```python
import functools

import jax
import jax.numpy as jnp
from jax import lax
from jax.experimental import pallas as pl
from jax.experimental.pallas import tpu as pltpu
from jax.sharding import Mesh
from jax.sharding import PartitionSpec as P

WINDOW = 128


epsilon = 1e-06
longest_lag = 15


def from_behind(block, axis):
    devices = range(lax.axis_size(axis))
    route = [(i - 1, i) for i in devices if i - 1 in devices]
    return lax.ppermute(block, axis, route)


def swap(block, axis):
    count = lax.axis_size(axis)
    return lax.ppermute(block, axis, [(i, count - 1 - i) for i in range(count)])


def row_norm(values, gain):
    return values * lax.rsqrt(jnp.mean(values * values, axis=-1, keepdims=True) + epsilon) * gain


def after(value, *others):
    return lax.optimization_barrier((value,) + others)[0]


def ordered(mine, theirs, index, dim):
    return jnp.where(
        index == 0,
        jnp.concatenate([mine, theirs], axis=dim),
        jnp.concatenate([theirs, mine], axis=dim),
    )


def both_cores(block, dim):
    if lax.axis_size("tp") == 2:
        return ordered(block, swap(block, "tp"), lax.axis_index("tp"), dim)
    return lax.all_gather(block, "tp", axis=dim, tiled=True)


def per_device(
    tokens,
    norm_gain,
    w_query,
    w_key,
    w_value,
    w_pool_in,
    query_gain,
    key_gain,
    sinks,
    w_mix,
    pool_scale,
    w_out_attn,
    w_out_pool,
):
    pair = lax.axis_size("si")
    place = lax.axis_index("si")
    outer = lax.axis_index("so")

    def share(array, owner, dim):
        size = array.shape[dim] // pair
        return lax.dynamic_slice_in_dim(array, owner * size, size, dim)

    def mine(arrays):
        return [share(a, place, 1) for a in arrays]

    def other(arrays):
        return [share(a, pair - 1 - place, 1) for a in arrays]

    def joined(own, came, dim):
        return own if pair == 1 else ordered(own, came, place, dim)

    def gathered(rows):
        return lax.all_gather(rows, "so", axis=0, tiled=True)

    qkv_parts = (w_query, w_key, w_value)
    qkv_own = jnp.concatenate(mine(qkv_parts), axis=1)
    if pair == 1:
        qkv_rows, pool_rows, attn_rows, mixed_rows = qkv_own, w_pool_in, w_out_attn, w_out_pool
        row_half = tokens
    else:
        qkv_came = swap(jnp.concatenate(other(qkv_parts), axis=1), "si")
        qkv_rows = joined(qkv_own, qkv_came, 0)
        late = lax.optimization_barrier((w_pool_in, w_out_attn, w_out_pool, qkv_came))[:3]
        came = [swap(share(w, pair - 1 - place, 1), "si") for w in late]
        pool_rows, attn_rows, mixed_rows = [
            joined(share(w, place, 1), c, 0) for w, c in zip((w_pool_in, w_out_attn, w_out_pool), came)
        ]
        row_half = joined(tokens, swap(after(tokens, qkv_came), "si"), 0)
    w_qkv = gathered(qkv_rows)
    w_pool = gathered(after(pool_rows, w_qkv))
    w_attn = gathered(after(attn_rows, w_pool))
    w_mixed = gathered(after(mixed_rows, w_attn))

    whole = both_cores(row_half, 1)
    row_count = whole.shape[0]
    normed = row_norm(whole.astype(jnp.float32), norm_gain).astype(jnp.bfloat16)
    qkv_raw = jnp.dot(normed, w_qkv, preferred_element_type=jnp.float32)
    head_size = query_gain.shape[0]
    query_width = w_query.shape[1] // pair
    kv_width = w_key.shape[1] // pair
    query_heads = query_width // head_size
    kv_local = kv_width // head_size
    per_kv = query_heads // kv_local
    query_raw = qkv_raw[:, :query_width]
    key_raw = qkv_raw[:, query_width : query_width + kv_width]
    value_raw = qkv_raw[:, query_width + kv_width :]
    queries = row_norm(query_raw.reshape(row_count, query_heads, head_size), query_gain).astype(
        jnp.bfloat16
    )
    key_rows = row_norm(key_raw.reshape(row_count, kv_local, head_size), key_gain).astype(
        jnp.bfloat16
    )
    values = value_raw.astype(jnp.bfloat16).reshape(row_count, kv_local, head_size)
    kv_tail = jnp.concatenate(
        [key_rows[-WINDOW:].reshape(WINDOW, -1), values[-WINDOW:].reshape(WINDOW, -1)], axis=1
    )
    kv_prev = from_behind(kv_tail, "so").reshape(WINDOW, 2, kv_local, head_size)
    offset = outer * row_count
    blocks = row_count // WINDOW

    def banded(previous, source):
        earlier = jnp.concatenate([previous, source[: row_count - WINDOW]], axis=0).reshape(
            blocks, WINDOW, kv_local, head_size
        )
        return jnp.concatenate(
            [earlier, source.reshape(blocks, WINDOW, kv_local, head_size)], axis=1
        )

    band_keys = banded(kv_prev[:, 0], key_rows)
    band_values = banded(kv_prev[:, 1], values)
    query_blocks = queries.reshape(blocks, WINDOW, kv_local, per_kv, head_size)
    scores = jnp.einsum(
        "bqkgd,bjkd->bkgqj", query_blocks, band_keys, preferred_element_type=jnp.float32
    ) * head_size ** (-0.5)
    query_index = jnp.arange(WINDOW)[:, None]
    key_index = jnp.arange(2 * WINDOW)[None, :]
    distance = query_index + WINDOW - key_index
    key_pos = offset + jnp.arange(blocks)[:, None, None] * WINDOW - WINDOW + key_index[None]
    valid = (distance[None] >= 0) & (distance[None] < WINDOW) & (key_pos >= 0)
    sink_logit = share(sinks, place, 0).reshape(kv_local, per_kv)[None, :, :, None, None]
    scores = jnp.where(valid[:, None, None], scores, -1e30)
    row_top = jnp.maximum(scores.max(axis=-1, keepdims=True), sink_logit)
    lifted = jnp.exp(scores - row_top)
    weights = (
        lifted / (lifted.sum(axis=-1, keepdims=True) + jnp.exp(sink_logit - row_top))
    ).astype(jnp.bfloat16)
    attended = (
        jnp.einsum("bkgqj,bjkd->bqkgd", weights, band_values, preferred_element_type=jnp.float32)
        .astype(jnp.bfloat16)
        .reshape(row_count, query_heads * head_size)
    )

    def all_heads(block):
        if pair == 2:
            block = joined(block, swap(block, "si"), 1)
        return both_cores(block, 1)

    attended_all = all_heads(attended)

    pool_in = jnp.dot(normed, w_pool, preferred_element_type=jnp.float32).astype(jnp.bfloat16)
    pool_prev = from_behind(pool_in[-longest_lag:], "so")
    mix = share(w_mix, place, 0)
    groups_local = mix.shape[0]
    group_dim = mix.shape[1]
    first_group = (lax.axis_index("tp") * pair + place) * groups_local
    group_ids = first_group + jnp.arange(groups_local, dtype=jnp.int32)
    spans = jnp.repeat(jnp.left_shift(jnp.int32(2), group_ids % 4), group_dim)
    extended = jnp.concatenate([pool_prev, pool_in], axis=0).astype(jnp.float32)
    window_sum = jnp.zeros((row_count, spans.shape[0]), jnp.float32)
    for back_step in range(longest_lag + 1):
        shifted = extended[longest_lag - back_step : longest_lag - back_step + row_count]
        window_sum = window_sum + jnp.where(back_step < spans[None, :], shifted, 0.0)
    positions = (offset + jnp.arange(1, row_count + 1, dtype=jnp.int32)).astype(jnp.float32)
    divisor = jnp.minimum(positions[:, None], spans.astype(jnp.float32)[None, :])
    contrast = (window_sum / divisor - extended[longest_lag:]).astype(jnp.bfloat16)
    mixed = jnp.einsum(
        "tgc,gcd->tgd",
        contrast.reshape(row_count, groups_local, group_dim),
        mix,
        preferred_element_type=jnp.float32,
    ).reshape(row_count, -1)
    pooled = (mixed * share(pool_scale, place, 0)).astype(jnp.bfloat16)
    pooled_all = all_heads(pooled)

    def project(owner):
        total = jnp.dot(share(attended_all, owner, 0), w_attn, preferred_element_type=jnp.float32)
        result = total + jnp.dot(
            share(pooled_all, owner, 0), w_mixed, preferred_element_type=jnp.float32
        )
        return result.astype(jnp.bfloat16)

    if pair == 1:
        return project(0)
    away = project(pair - 1 - place)
    came_back = swap(away, "si")
    return joined(project(place), came_back, 1)


MESH = pl.DeviceIdType.MESH
NEGATIVE = -1e30


def remote(src, dst, send_sem, recv_sem, device):
    return pltpu.make_async_remote_copy(
        src_ref=src,
        dst_ref=dst,
        send_sem=send_sem,
        recv_sem=recv_sem,
        device_id=device,
        device_id_type=MESH,
    )


class Place:
    def __init__(self, planes):
        self.sp, self.c = lax.axis_index("sp"), lax.axis_index("tp")
        self.planes = planes
        self.z, self.p = lax.div(self.sp, 4), lax.rem(self.sp, 4)
        x, y = lax.rem(self.p, 2), lax.div(self.p, 2)
        self.xn, self.yn, self.dg = self.p + 1 - 2 * x, self.p + 2 - 4 * y, 3 - self.p
        self.mates = (self.xn, self.yn, self.dg)

    def mate(self, p):
        return (self.z * 4 + p, self.c)

    def partner(self):
        return (self.sp, 1 - self.c)

    def above(self):
        return (lax.rem(self.sp + 4, 4 * self.planes), self.c)

    def below(self):
        return (lax.rem(self.sp + 4 * self.planes - 4, 4 * self.planes), self.c)

    def barrier(self):
        sem = pltpu.get_barrier_semaphore()
        for p in self.mates:
            pl.semaphore_signal(sem, inc=1, device_id=self.mate(p), device_id_type=MESH)
        pl.semaphore_signal(sem, inc=1, device_id=self.partner(), device_id_type=MESH)

        @pl.when(self.z < self.planes - 1)
        def _():
            pl.semaphore_signal(sem, inc=1, device_id=self.above(), device_id_type=MESH)

        @pl.when(self.z > 0)
        def _():
            pl.semaphore_signal(sem, inc=1, device_id=self.below(), device_id_type=MESH)

        inner = (self.z > 0) & (self.z < self.planes - 1)

        @pl.when(inner)
        def _():
            pl.semaphore_wait(sem, 6)

        @pl.when(jnp.logical_not(inner))
        def _():
            pl.semaphore_wait(sem, 5)


class Rows:
    def __init__(self, at, own, held, local_sem, near, recv, up, down):
        self.at, self.own, self.held = at, own, held
        self.local_sem, self.near, self.recv, self.up, self.down = local_sem, near, recv, up, down

    def local(self):
        at = self.at
        return pltpu.make_async_copy(self.own.at[at.p], self.held.at[at.z, at.p], self.local_sem)

    def to_mate(self, index, p):
        at = self.at
        return remote(
            self.own.at[p],
            self.held.at[at.z, at.p],
            self.near.at[index],
            self.recv.at[at.z, at.p],
            at.mate(p),
        )

    def hop(self, plane, p, src, upward):
        at = self.at
        return remote(
            src,
            self.held.at[plane, p],
            (self.up if upward else self.down).at[plane, p],
            self.recv.at[plane, p],
            at.above() if upward else at.below(),
        )

    def send_up(self, plane, p, src=None):
        src = self.held.at[plane, p] if src is None else src

        @pl.when(self.at.z < self.at.planes - 1)
        def _():
            self.hop(plane, p, src, True).start()

    def send_down(self, plane, p, src=None):
        src = self.held.at[plane, p] if src is None else src

        @pl.when(self.at.z > 0)
        def _():
            self.hop(plane, p, src, False).start()

    def begin(self):
        at = self.at
        self.send_up(at.z, at.p, self.own.at[at.p])
        self.send_down(at.z, at.p, self.own.at[at.p])
        for index, p in enumerate(at.mates):
            self.to_mate(index, p).start()
        self.local().start()

    def arrived(self, plane, p):
        self.hop(plane, p, self.held.at[plane, p], True).wait_recv()

    def pass_near(self):
        at = self.at
        for p in at.mates:
            self.arrived(at.z, p)
            self.send_up(at.z, p)
            self.send_down(at.z, p)

    def pass_far(self, distance, index):
        at = self.at
        p = (at.p,) + at.mates
        p = p[index]
        low, high = at.z - distance, at.z + distance

        @pl.when(low >= 0)
        def _():
            self.arrived(low, p)
            self.send_up(low, p)

        @pl.when(high < at.planes)
        def _():
            self.arrived(high, p)
            self.send_down(high, p)

    def finish(self):
        at = self.at
        for index, p in enumerate(at.mates):
            self.to_mate(index, p).wait_send()
        for plane in range(at.planes):
            for p in range(4):

                @pl.when((at.z < at.planes - 1) & (at.z >= plane))
                def _():
                    self.hop(plane, p, self.held.at[plane, p], True).wait_send()

                @pl.when((at.z > 0) & (at.z <= plane))
                def _():
                    self.hop(plane, p, self.held.at[plane, p], False).wait_send()


def project_kernel(
    planes,
    head,
    tok,
    gain,
    own_w,
    query_gain,
    key_gain,
    q_out,
    kv_out,
    pool_out,
    raw,
    xs,
    ws,
    raw_sems,
    t_send,
    t_recv,
    d_send,
    d_recv,
    w_local,
    w_near,
    w_recv,
    w_up,
    w_down,
    h_send,
    h_recv,
):
    at = Place(planes)
    c, p, z = at.c, at.p, at.z
    count, half = tok.shape
    part = count // 2
    deep = xs.shape[3]
    blocks = half // deep
    rows = Rows(at, own_w, ws, w_local, w_near, w_recv, w_up, w_down)
    at.barrier()
    raw_local = pltpu.make_async_copy(tok, raw.at[c], raw_sems.at[0])
    raw_away = remote(tok, raw.at[c], raw_sems.at[1], raw_sems.at[2], at.partner())
    raw_away.start()
    raw_local.start()
    rows.begin()
    raw_local.wait()
    raw_away.wait_recv()

    step = 32

    def norm_step(index, carry):
        span = pl.ds(pl.multiple_of(index * step, step), step)
        halves = [raw[k, span, :].astype(jnp.float32) for k in range(2)]
        total = sum(jnp.sum(v * v, axis=-1, keepdims=True) for v in halves)
        scale = lax.rsqrt(total / (2 * half) + epsilon)
        for k in range(2):
            out = (halves[k] * scale * gain[:, k * half : (k + 1) * half]).astype(jnp.bfloat16)
            for b in range(blocks):
                xs[p, k * blocks + b, span, :] = out[:, b * deep : (b + 1) * deep]
        return carry

    lax.fori_loop(0, count // step, norm_step, 0)

    def piece(place, h):
        return xs.at[place, pl.ds(c * blocks, blocks), pl.ds(h * part, part), :]

    def tokens_to(index, place, h, to):
        return remote(
            piece(place, h), piece(place, h), t_send.at[index], t_recv.at[place, h], at.mate(to)
        )

    def tokens_over(index, place, h):
        return remote(
            piece(place, h), piece(place, h), d_send.at[index], d_recv.at[place, h], at.partner()
        )

    def tokens_came(place, h):
        remote(
            piece(place, h), piece(place, h), t_send.at[0], t_recv.at[place, h], at.partner()
        ).wait_recv()

    tokens_to(0, p, 0, at.xn).start()
    tokens_to(1, p, 1, at.yn).start()
    tokens_to(2, p, 1, at.xn).start()
    tokens_to(3, p, 0, at.yn).start()
    rows.pass_near()

    def first_tokens():
        tokens_came(at.xn, 0)
        tokens_to(4, at.xn, 0, at.yn).start()
        tokens_over(0, at.xn, 0).start()
        tokens_came(at.yn, 1)
        tokens_to(5, at.yn, 1, at.xn).start()
        tokens_over(1, at.yn, 1).start()

    def second_tokens():
        tokens_came(at.xn, 1)
        tokens_over(2, at.xn, 1).start()
        tokens_came(at.yn, 0)
        tokens_over(3, at.yn, 0).start()

    def last_tokens():
        for h in range(2):
            tokens_came(at.dg, h)
            tokens_over(4 + h, at.dg, h).start()

    for distance in range(1, planes):
        for index in range(4):
            rows.pass_far(distance, index)
            at_step = (distance - 1) * 4 + index
            if at_step == 4 * planes // 3:
                first_tokens()
            if at_step == 2 * planes:
                second_tokens()
    last_tokens()
    for place in at.mates:
        for h in range(2):
            other = xs.at[place, pl.ds((1 - c) * blocks, blocks), pl.ds(h * part, part), :]
            remote(other, other, d_send.at[0], d_recv.at[place, h], at.partner()).wait_recv()
    rows.local().wait()

    width = q_out.shape[1]
    pairs = width // (2 * head)
    kv_rows, pool_rows = kv_out.shape[0] - 4 * count, pool_out.shape[0] - 4 * count
    lane = lax.broadcasted_iota(jnp.int32, (part, 2 * head), 1)
    low = lane < head

    def halo(out, size):
        return out.at[pl.ds(4 * count, size), :], out.at[pl.ds(0, size), :]

    def halo_send(k, out, size):
        src, dst = halo(out, size)
        return remote(src, dst, h_send.at[k], h_recv.at[k], at.above())

    def project_step(index, carry):
        tile = 7 - index
        place, h = lax.div(tile, 2), lax.rem(tile, 2)
        span = pl.ds(pl.multiple_of(h * part, part), part)
        total = None
        for b in range(planes):
            term = jnp.dot(
                xs[place, b, span, :],
                ws[b].reshape(deep, ws.shape[3]),
                preferred_element_type=jnp.float32,
            )
            total = term if total is None else total + term
        base = pl.multiple_of(tile * part, part)
        for k in range(pairs):
            v = total[:, 2 * head * k : 2 * head * (k + 1)]
            square = v * v
            lo = jnp.sum(jnp.where(low, square, 0.0), axis=-1, keepdims=True) / head
            hi = jnp.sum(jnp.where(low, 0.0, square), axis=-1, keepdims=True) / head
            scale = jnp.where(low, lax.rsqrt(lo + epsilon), lax.rsqrt(hi + epsilon))
            q_out[pl.ds(base, part), 2 * head * k : 2 * head * (k + 1)] = (
                v * scale * query_gain[...]
            ).astype(jnp.bfloat16)
        v = total[:, width : width + 2 * head]
        lo = jnp.sum(jnp.where(low, v * v, 0.0), axis=-1, keepdims=True) / head
        kv = jnp.where(low, v * lax.rsqrt(lo + epsilon) * key_gain[...], v)
        kv_out[pl.ds(base + kv_rows, part), : 2 * head] = kv.astype(jnp.bfloat16)
        kv_out[pl.ds(base + kv_rows, part), 2 * head :] = pltpu.roll(kv, head, 1).astype(
            jnp.bfloat16
        )
        pool_out[pl.ds(base + pool_rows, part), :] = total[:, width + 2 * head :].astype(
            jnp.bfloat16
        )

        @pl.when((index == 1) & (z < planes - 1))
        def _():
            halo_send(0, kv_out, kv_rows).start()
            halo_send(1, pool_out, pool_rows).start()

        return carry

    @pl.when(z == 0)
    def _():
        kv_out[0:kv_rows, :] = jnp.zeros((kv_rows, kv_out.shape[1]), jnp.bfloat16)
        pool_out[0:pool_rows, :] = jnp.zeros((pool_rows, pool_out.shape[1]), jnp.bfloat16)

    lax.fori_loop(0, 8, project_step, 0)

    @pl.when(z > 0)
    def _():
        halo_send(0, kv_out, kv_rows).wait_recv()
        halo_send(1, pool_out, pool_rows).wait_recv()

    raw_away.wait_send()
    tokens_to(0, p, 0, at.xn).wait_send()
    tokens_to(1, p, 1, at.yn).wait_send()
    tokens_to(2, p, 1, at.xn).wait_send()
    tokens_to(3, p, 0, at.yn).wait_send()
    tokens_to(4, at.xn, 0, at.yn).wait_send()
    tokens_to(5, at.yn, 1, at.xn).wait_send()
    tokens_over(0, at.xn, 0).wait_send()
    tokens_over(1, at.yn, 1).wait_send()
    tokens_over(2, at.xn, 1).wait_send()
    tokens_over(3, at.yn, 0).wait_send()
    for h in range(2):
        tokens_over(4 + h, at.dg, h).wait_send()
    rows.finish()

    @pl.when(z < planes - 1)
    def _():
        halo_send(0, kv_out, kv_rows).wait_send()
        halo_send(1, pool_out, pool_rows).wait_send()


def mix_kernel(
    planes,
    head,
    q,
    kv,
    pool,
    own_w,
    mix,
    pool_scale,
    sinks,
    out,
    ma,
    ws,
    ys,
    w_local,
    w_near,
    w_recv,
    w_up,
    w_down,
    m_send,
    m_recv,
    f_send,
    f_recv,
    d_send,
    d_recv,
    r_send,
    r_recv,
    r_local,
):
    at = Place(planes)
    c, p, z = at.c, at.p, at.z
    pair = 2 * head
    steps, tall, wide = ma.shape[1:]
    block = tall // 4
    count = q.shape[0] // 4
    width = q.shape[1]
    heads = width // head
    channels = pool.shape[1]
    pool_halo = pool.shape[0] - q.shape[0]
    rows = Rows(at, own_w, ws, w_local, w_near, w_recv, w_up, w_down)
    at.barrier()
    rows.begin()

    query = lax.broadcasted_iota(jnp.int32, (block, 2 * block), 0)
    key = lax.broadcasted_iota(jnp.int32, (block, 2 * block), 1)
    band = (key > query) & (key <= query + block)
    low = lax.broadcasted_iota(jnp.int32, (2 * block, pair), 1) < head
    line = lax.broadcasted_iota(jnp.int32, (block, channels), 0)
    span = lax.shift_left(jnp.int32(2), p).astype(jnp.float32)
    slot = c * 4 + p

    def mixers(j, place):
        base = pl.multiple_of(place * count + j * block, block)
        kvs = kv[pl.ds(base, 2 * block), :]
        straight, turned = kvs[:, :pair], kvs[:, pair:]
        zero = jnp.zeros_like(straight)
        keys = (jnp.where(low, straight, zero), jnp.where(low, zero, turned))
        values = (jnp.where(low, turned, zero), jnp.where(low, zero, straight))
        start = (z == 0) & (place == 0) & (j == 0)
        valid = band & (key >= jnp.where(start, block, 0))
        span_rows = pl.ds(pl.multiple_of(place * block, block), block)
        for k in range(heads // 2):
            q_pair = q[pl.ds(base, block), pair * k : pair * (k + 1)]
            total = None
            for side in range(2):
                sink = sinks[p * heads + 2 * k + side]
                scores = lax.dot_general(
                    q_pair,
                    keys[side],
                    (((1,), (1,)), ((), ())),
                    preferred_element_type=jnp.float32,
                ) * head ** (-0.5)
                scores = jnp.where(valid, scores, NEGATIVE)
                top = jnp.maximum(jnp.max(scores, axis=-1, keepdims=True), sink)
                lifted = jnp.exp(scores - top)
                under = jnp.sum(lifted, axis=-1, keepdims=True) + jnp.exp(sink - top)
                weights = (lifted / under).astype(jnp.bfloat16)
                term = jnp.dot(weights, values[side], preferred_element_type=jnp.float32)
                total = term if total is None else total + term
            ma[slot, j, span_rows, 2 * pair * k : 2 * pair * k + pair] = total.astype(jnp.bfloat16)
        wide_rows = pool[pl.ds(base, pool_halo + block), :].astype(jnp.float32)
        sums, lag = [wide_rows], 1
        while 2 * lag <= pool_halo:
            sums.append(sums[-1] + pltpu.roll(sums[-1], lag, 0))
            lag *= 2
        window_sum = sums[-1]
        for k in range(len(sums) - 2, 0, -1):
            window_sum = jnp.where(p == k - 1, sums[k], window_sum)
        position = (z * 4 * count + place * count + j * block + 1 + line).astype(jnp.float32)
        contrast = (
            window_sum[pool_halo:] / jnp.minimum(position, span) - wide_rows[pool_halo:]
        ).astype(jnp.bfloat16)
        mixed = jnp.dot(contrast, mix[p], preferred_element_type=jnp.float32) * pool_scale[p]
        for k in range(channels // pair):
            ma[slot, j, span_rows, (2 * k + 1) * pair : (2 * k + 2) * pair] = mixed[
                :, pair * k : pair * (k + 1)
            ].astype(jnp.bfloat16)

    def to_mate(index, j, to):
        block_ref = ma.at[slot, j]
        return remote(block_ref, block_ref, m_send.at[index, j], m_recv.at[p, j], at.mate(to))

    def onward(k, j, place, to):
        half = ma.at[c * 4 + place, j, pl.ds(k * (tall // 2), tall // 2), :]
        return remote(half, half, f_send.at[k, j], f_recv.at[k, j], at.mate(to))

    def over(index, j, place, core):
        block_ref = ma.at[core * 4 + place, j]
        return remote(
            block_ref, block_ref, d_send.at[index, j], d_recv.at[place, j], at.partner()
        )

    def came(place, j):
        block_ref = ma.at[c * 4 + place, j]
        remote(
            block_ref, block_ref, m_send.at[0, j], m_recv.at[place, j], at.partner()
        ).wait_recv()

    def first(j, carry):
        def one(place, inner):
            mixers(j, place)
            return inner

        lax.fori_loop(0, 4, one, 0)
        to_mate(0, j, at.xn).start()
        to_mate(1, j, at.yn).start()
        over(0, j, p, c).start()

        @pl.when(j == 0)
        def _():
            rows.pass_near()

        return carry

    lax.fori_loop(0, steps, first, 0)

    def pass_on(j):
        came(at.xn, j)
        onward(0, j, at.xn, at.yn).start()
        over(1, j, at.xn, c).start()
        came(at.yn, j)
        onward(1, j, at.yn, at.xn).start()
        over(2, j, at.yn, c).start()

    passed = 0
    total_far = 4 * (planes - 1)
    for at_step in range(total_far):
        rows.pass_far(at_step // 4 + 1, at_step % 4)
        while passed < steps and at_step + 1 >= (passed + 1) * total_far // (steps + 1):
            pass_on(passed)
            passed += 1
    while passed < steps:
        pass_on(passed)
        passed += 1
    rows.local().wait()

    columns = ws.shape[3]

    def result(index, j, to):
        return remote(
            ys.at[j, pl.ds(pl.multiple_of(to * block, block), block), :],
            out.at[
                pl.ds(pl.multiple_of(j * block, block), block),
                pl.ds(pl.multiple_of(p * columns, columns), columns),
            ],
            r_send.at[index, j],
            r_recv.at[p, j],
            at.mate(to),
        )

    def result_here(j):
        return pltpu.make_async_copy(
            ys.at[j, pl.ds(pl.multiple_of(p * block, block), block), :],
            out.at[
                pl.ds(pl.multiple_of(j * block, block), block),
                pl.ds(pl.multiple_of(p * columns, columns), columns),
            ],
            r_local.at[j],
        )

    def last(j, carry):
        for k in range(2):
            onward(k, j, at.dg, at.xn).wait_recv()
        over(3, j, at.dg, c).start()
        for place in range(4):
            over(0, j, place, 1 - c).wait_recv()
        total = None
        for i in range(8):
            first_slot = 2 * i
            weight = ws[first_slot // 4, first_slot % 4 : first_slot % 4 + 2].reshape(wide, columns)
            term = jnp.dot(ma[i, j], weight, preferred_element_type=jnp.float32)
            total = term if total is None else total + term
        ys[j] = total.astype(jnp.bfloat16)
        for index, to in enumerate(at.mates):
            result(index, j, to).start()
        result_here(j).start()
        return carry

    lax.fori_loop(0, steps, last, 0)

    def finish(j, carry):
        for index, to in enumerate(at.mates):
            remote(
                ys.at[j, pl.ds(0, block), :],
                out.at[
                    pl.ds(pl.multiple_of(j * block, block), block),
                    pl.ds(pl.multiple_of(to * columns, columns), columns),
                ],
                r_send.at[index, j],
                r_recv.at[to, j],
                at.mate(to),
            ).wait_recv()
        result_here(j).wait()
        for index, to in enumerate(at.mates):
            result(index, j, to).wait_send()
        to_mate(0, j, at.xn).wait_send()
        to_mate(1, j, at.yn).wait_send()
        onward(0, j, at.xn, at.yn).wait_send()
        onward(1, j, at.yn, at.xn).wait_send()
        over(0, j, p, c).wait_send()
        over(1, j, at.xn, c).wait_send()
        over(2, j, at.yn, c).wait_send()
        over(3, j, at.dg, c).wait_send()
        return carry

    lax.fori_loop(0, steps, finish, 0)
    rows.finish()


def row_scratch(planes, rows, columns):
    return [
        pltpu.SemaphoreType.DMA,
        pltpu.SemaphoreType.DMA((3,)),
        pltpu.SemaphoreType.DMA((planes, 4)),
        pltpu.SemaphoreType.DMA((planes, 4)),
        pltpu.SemaphoreType.DMA((planes, 4)),
    ]


def per_device_planes(
    tokens,
    norm_gain,
    w_query,
    w_key,
    w_value,
    w_pool_in,
    query_gain,
    key_gain,
    sinks,
    w_mix,
    pool_scale,
    w_out_attn,
    w_out_pool,
):
    planes = lax.axis_size("sp") // 4
    head = query_gain.shape[0]
    count, half = tokens.shape
    in_rows = w_query.shape[0]

    def quarters(array):
        return array.reshape(array.shape[0], 4, -1)

    w_in = jnp.concatenate([quarters(w) for w in (w_query, w_key, w_value, w_pool_in)], axis=2)
    w_in = jnp.transpose(w_in, (1, 0, 2))
    w_out = jnp.concatenate([quarters(w_out_attn), quarters(w_out_pool)], axis=0)
    w_out = jnp.transpose(w_out, (1, 0, 2))
    width, channels = w_query.shape[1] // 4, w_pool_in.shape[1] // 4
    pair = 2 * head
    deep = 4 * in_rows
    vmem = pl.BlockSpec(memory_space=pltpu.VMEM)
    anywhere = pl.BlockSpec(memory_space=pl.ANY)
    dma = pltpu.SemaphoreType.DMA
    q, kv, pool = pl.pallas_call(
        functools.partial(project_kernel, planes, head),
        out_shape=(
            jax.ShapeDtypeStruct((4 * count, width), jnp.bfloat16),
            jax.ShapeDtypeStruct((4 * count + WINDOW, 2 * pair), jnp.bfloat16),
            jax.ShapeDtypeStruct((4 * count + longest_lag + 1, channels), jnp.bfloat16),
        ),
        in_specs=[anywhere, vmem, anywhere, vmem, vmem],
        out_specs=(vmem, vmem, vmem),
        scratch_shapes=[
            pltpu.VMEM((2, count, half), jnp.bfloat16),
            pltpu.VMEM((4, planes, count, deep), jnp.bfloat16),
            pltpu.VMEM((planes, 4, in_rows, w_in.shape[2]), jnp.bfloat16),
            dma((3,)),
            dma((6,)),
            dma((4, 2)),
            dma((6,)),
            dma((4, 2)),
        ]
        + row_scratch(planes, in_rows, w_in.shape[2])
        + [dma((2,)), dma((2,))],
        compiler_params=pltpu.CompilerParams(
            collective_id=0, has_side_effects=True, vmem_limit_bytes=60 * 2**20
        ),
        name="project",
    )(
        tokens,
        norm_gain.reshape(1, -1),
        w_in,
        jnp.tile(query_gain, 2).reshape(1, -1),
        jnp.concatenate([key_gain, jnp.ones_like(key_gain)]).reshape(1, -1),
    )
    steps = count // WINDOW
    wide = width + channels
    columns = w_out.shape[2]
    out_rows = w_out.shape[1]
    return pl.pallas_call(
        functools.partial(mix_kernel, planes, head),
        out_shape=jax.ShapeDtypeStruct(tokens.shape, jnp.bfloat16),
        in_specs=[vmem, vmem, vmem, anywhere, vmem, vmem, pl.BlockSpec(memory_space=pltpu.SMEM)],
        out_specs=anywhere,
        scratch_shapes=[
            pltpu.VMEM((8, steps, 4 * WINDOW, wide), jnp.bfloat16),
            pltpu.VMEM((planes, 4, out_rows, columns), jnp.bfloat16),
            pltpu.VMEM((steps, 4 * WINDOW, columns), jnp.bfloat16),
        ]
        + row_scratch(planes, out_rows, columns)
        + [
            dma((2, steps)),
            dma((4, steps)),
            dma((2, steps)),
            dma((2, steps)),
            dma((4, steps)),
            dma((4, steps)),
            dma((3, steps)),
            dma((4, steps)),
            dma((steps,)),
        ],
        compiler_params=pltpu.CompilerParams(
            collective_id=1, has_side_effects=True, vmem_limit_bytes=60 * 2**20
        ),
        name="mix",
    )(q, kv, pool, w_out, w_mix, pool_scale.reshape(4, 1, -1), sinks)


def suits_planes(mesh, args):
    sp, tp = mesh.shape["sp"], mesh.shape["tp"]
    tokens, w_query, w_key, w_pool_in = args[0], args[2], args[3], args[5]
    head, groups = args[6].shape[0], args[9].shape[0]
    w_out_attn, w_out_pool = args[11], args[12]
    if tp != 2 or sp % 8 or 2 * head != 128:
        return False
    share = 4 * tp
    rows = tokens.shape[0] // sp
    width, channels = w_query.shape[1] // share, w_pool_in.shape[1] // share
    held = 2 * 4 * rows * tokens.shape[1] + 2 * w_query.shape[0] * (width + 128 + channels)
    return (
        w_key.shape[1] == share * head
        and groups == share
        and rows % (2 * WINDOW) == 0
        and width % 128 == 0
        and width == channels
        and 2 * w_out_attn.shape[0] // sp == width
        and 2 * w_out_pool.shape[0] // sp == channels
        and w_out_attn.shape[0] // sp == 2 * head
        and w_query.shape[0] // sp % 16 == 0
        and w_out_attn.shape[1] % (share * 128) == 0
        and held < 36 * 2**20
    )


def solution(mesh):
    sp, tp = mesh.shape["sp"], mesh.shape["tp"]

    def call(*args):
        if suits_planes(mesh, args):
            return jax.shard_map(
                per_device_planes,
                mesh=mesh,
                in_specs=(
                    P("sp", "tp"),
                    P(),
                    P("sp", "tp"),
                    P("sp", "tp"),
                    P("sp", "tp"),
                    P("sp", "tp"),
                    P(),
                    P(),
                    P("tp"),
                    P("tp", None, None),
                    P("tp"),
                    P("sp", "tp"),
                    P("sp", "tp"),
                ),
                out_specs=P("sp", "tp"),
                check_vma=False,
            )(*args)
        kv_local = args[3].shape[1] // args[6].shape[0] // tp
        groups_local = args[9].shape[0] // tp
        fits = sp % 2 == 0 and kv_local % 2 == 0 and groups_local % 2 == 0
        pair = 2 if fits else 1
        inner = Mesh(mesh.devices.reshape(sp // pair, pair, tp), ("so", "si", "tp"))
        rows = ("so", "si")
        return jax.shard_map(
            per_device,
            mesh=inner,
            in_specs=(
                P(rows, "tp"),
                P(),
                P(rows, "tp"),
                P(rows, "tp"),
                P(rows, "tp"),
                P(rows, "tp"),
                P(),
                P(),
                P("tp"),
                P("tp", None, None),
                P("tp"),
                P(rows, "tp"),
                P(rows, "tp"),
            ),
            out_specs=P(rows, "tp"),
            check_vma=False,
        )(*args)

    return call
```

```python
import functools

import jax
import jax.numpy as jnp
from jax import lax
from jax.experimental import pallas as pl
from jax.experimental.pallas import tpu as pltpu
from jax.sharding import Mesh
from jax.sharding import PartitionSpec as P

WINDOW = 128


epsilon = 1e-06
longest_lag = 15


def from_behind(block, axis):
    devices = range(lax.axis_size(axis))
    route = [(i - 1, i) for i in devices if i - 1 in devices]
    return lax.ppermute(block, axis, route)


def swap(block, axis):
    count = lax.axis_size(axis)
    return lax.ppermute(block, axis, [(i, count - 1 - i) for i in range(count)])


def row_norm(values, gain):
    return values * lax.rsqrt(jnp.mean(values * values, axis=-1, keepdims=True) + epsilon) * gain


def after(value, *others):
    return lax.optimization_barrier((value,) + others)[0]


def ordered(mine, theirs, index, dim):
    return jnp.where(
        index == 0,
        jnp.concatenate([mine, theirs], axis=dim),
        jnp.concatenate([theirs, mine], axis=dim),
    )


def both_cores(block, dim):
    if lax.axis_size("tp") == 2:
        return ordered(block, swap(block, "tp"), lax.axis_index("tp"), dim)
    return lax.all_gather(block, "tp", axis=dim, tiled=True)


def per_device(
    tokens,
    norm_gain,
    w_query,
    w_key,
    w_value,
    w_pool_in,
    query_gain,
    key_gain,
    sinks,
    w_mix,
    pool_scale,
    w_out_attn,
    w_out_pool,
):
    pair = lax.axis_size("si")
    place = lax.axis_index("si")
    outer = lax.axis_index("so")

    def share(array, owner, dim):
        size = array.shape[dim] // pair
        return lax.dynamic_slice_in_dim(array, owner * size, size, dim)

    def mine(arrays):
        return [share(a, place, 1) for a in arrays]

    def other(arrays):
        return [share(a, pair - 1 - place, 1) for a in arrays]

    def joined(own, came, dim):
        return own if pair == 1 else ordered(own, came, place, dim)

    def gathered(rows):
        return lax.all_gather(rows, "so", axis=0, tiled=True)

    qkv_parts = (w_query, w_key, w_value)
    qkv_own = jnp.concatenate(mine(qkv_parts), axis=1)
    if pair == 1:
        qkv_rows, pool_rows, attn_rows, mixed_rows = qkv_own, w_pool_in, w_out_attn, w_out_pool
        row_half = tokens
    else:
        qkv_came = swap(jnp.concatenate(other(qkv_parts), axis=1), "si")
        qkv_rows = joined(qkv_own, qkv_came, 0)
        late = lax.optimization_barrier((w_pool_in, w_out_attn, w_out_pool, qkv_came))[:3]
        came = [swap(share(w, pair - 1 - place, 1), "si") for w in late]
        pool_rows, attn_rows, mixed_rows = [
            joined(share(w, place, 1), c, 0) for w, c in zip((w_pool_in, w_out_attn, w_out_pool), came)
        ]
        row_half = joined(tokens, swap(after(tokens, qkv_came), "si"), 0)
    w_qkv = gathered(qkv_rows)
    w_pool = gathered(after(pool_rows, w_qkv))
    w_attn = gathered(after(attn_rows, w_pool))
    w_mixed = gathered(after(mixed_rows, w_attn))

    whole = both_cores(row_half, 1)
    row_count = whole.shape[0]
    normed = row_norm(whole.astype(jnp.float32), norm_gain).astype(jnp.bfloat16)
    qkv_raw = jnp.dot(normed, w_qkv, preferred_element_type=jnp.float32)
    head_size = query_gain.shape[0]
    query_width = w_query.shape[1] // pair
    kv_width = w_key.shape[1] // pair
    query_heads = query_width // head_size
    kv_local = kv_width // head_size
    per_kv = query_heads // kv_local
    query_raw = qkv_raw[:, :query_width]
    key_raw = qkv_raw[:, query_width : query_width + kv_width]
    value_raw = qkv_raw[:, query_width + kv_width :]
    queries = row_norm(query_raw.reshape(row_count, query_heads, head_size), query_gain).astype(
        jnp.bfloat16
    )
    key_rows = row_norm(key_raw.reshape(row_count, kv_local, head_size), key_gain).astype(
        jnp.bfloat16
    )
    values = value_raw.astype(jnp.bfloat16).reshape(row_count, kv_local, head_size)
    kv_tail = jnp.concatenate(
        [key_rows[-WINDOW:].reshape(WINDOW, -1), values[-WINDOW:].reshape(WINDOW, -1)], axis=1
    )
    kv_prev = from_behind(kv_tail, "so").reshape(WINDOW, 2, kv_local, head_size)
    offset = outer * row_count
    blocks = row_count // WINDOW

    def banded(previous, source):
        earlier = jnp.concatenate([previous, source[: row_count - WINDOW]], axis=0).reshape(
            blocks, WINDOW, kv_local, head_size
        )
        return jnp.concatenate(
            [earlier, source.reshape(blocks, WINDOW, kv_local, head_size)], axis=1
        )

    band_keys = banded(kv_prev[:, 0], key_rows)
    band_values = banded(kv_prev[:, 1], values)
    query_blocks = queries.reshape(blocks, WINDOW, kv_local, per_kv, head_size)
    scores = jnp.einsum(
        "bqkgd,bjkd->bkgqj", query_blocks, band_keys, preferred_element_type=jnp.float32
    ) * head_size ** (-0.5)
    query_index = jnp.arange(WINDOW)[:, None]
    key_index = jnp.arange(2 * WINDOW)[None, :]
    distance = query_index + WINDOW - key_index
    key_pos = offset + jnp.arange(blocks)[:, None, None] * WINDOW - WINDOW + key_index[None]
    valid = (distance[None] >= 0) & (distance[None] < WINDOW) & (key_pos >= 0)
    sink_logit = share(sinks, place, 0).reshape(kv_local, per_kv)[None, :, :, None, None]
    scores = jnp.where(valid[:, None, None], scores, -1e30)
    row_top = jnp.maximum(scores.max(axis=-1, keepdims=True), sink_logit)
    lifted = jnp.exp(scores - row_top)
    weights = (
        lifted / (lifted.sum(axis=-1, keepdims=True) + jnp.exp(sink_logit - row_top))
    ).astype(jnp.bfloat16)
    attended = (
        jnp.einsum("bkgqj,bjkd->bqkgd", weights, band_values, preferred_element_type=jnp.float32)
        .astype(jnp.bfloat16)
        .reshape(row_count, query_heads * head_size)
    )

    def all_heads(block):
        if pair == 2:
            block = joined(block, swap(block, "si"), 1)
        return both_cores(block, 1)

    attended_all = all_heads(attended)

    pool_in = jnp.dot(normed, w_pool, preferred_element_type=jnp.float32).astype(jnp.bfloat16)
    pool_prev = from_behind(pool_in[-longest_lag:], "so")
    mix = share(w_mix, place, 0)
    groups_local = mix.shape[0]
    group_dim = mix.shape[1]
    first_group = (lax.axis_index("tp") * pair + place) * groups_local
    group_ids = first_group + jnp.arange(groups_local, dtype=jnp.int32)
    spans = jnp.repeat(jnp.left_shift(jnp.int32(2), group_ids % 4), group_dim)
    extended = jnp.concatenate([pool_prev, pool_in], axis=0).astype(jnp.float32)
    window_sum = jnp.zeros((row_count, spans.shape[0]), jnp.float32)
    for back_step in range(longest_lag + 1):
        shifted = extended[longest_lag - back_step : longest_lag - back_step + row_count]
        window_sum = window_sum + jnp.where(back_step < spans[None, :], shifted, 0.0)
    positions = (offset + jnp.arange(1, row_count + 1, dtype=jnp.int32)).astype(jnp.float32)
    divisor = jnp.minimum(positions[:, None], spans.astype(jnp.float32)[None, :])
    contrast = (window_sum / divisor - extended[longest_lag:]).astype(jnp.bfloat16)
    mixed = jnp.einsum(
        "tgc,gcd->tgd",
        contrast.reshape(row_count, groups_local, group_dim),
        mix,
        preferred_element_type=jnp.float32,
    ).reshape(row_count, -1)
    pooled = (mixed * share(pool_scale, place, 0)).astype(jnp.bfloat16)
    pooled_all = all_heads(pooled)

    def project(owner):
        total = jnp.dot(share(attended_all, owner, 0), w_attn, preferred_element_type=jnp.float32)
        result = total + jnp.dot(
            share(pooled_all, owner, 0), w_mixed, preferred_element_type=jnp.float32
        )
        return result.astype(jnp.bfloat16)

    if pair == 1:
        return project(0)
    away = project(pair - 1 - place)
    came_back = swap(away, "si")
    return joined(project(place), came_back, 1)


MESH = pl.DeviceIdType.MESH
NEGATIVE = -1e30


def remote(src, dst, send_sem, recv_sem, device):
    return pltpu.make_async_remote_copy(
        src_ref=src,
        dst_ref=dst,
        send_sem=send_sem,
        recv_sem=recv_sem,
        device_id=device,
        device_id_type=MESH,
    )


def aligned(index, size):
    return pl.ds(pl.multiple_of(index * size, size), size)


class Place:
    def __init__(self, planes):
        self.sp, self.c = lax.axis_index("sp"), lax.axis_index("tp")
        self.planes = planes
        self.z, self.p = lax.div(self.sp, 4), lax.rem(self.sp, 4)
        x, y = lax.rem(self.p, 2), lax.div(self.p, 2)
        self.xn, self.yn, self.dg = self.p + 1 - 2 * x, self.p + 2 - 4 * y, 3 - self.p
        self.mates = (self.xn, self.yn, self.dg)
        self.has_above, self.has_below = self.z < planes - 1, self.z > 0

    def mate(self, p):
        return (self.z * 4 + p, self.c)

    def partner(self):
        return (self.sp, 1 - self.c)

    def above(self):
        return (lax.rem(self.sp + 4, 4 * self.planes), self.c)

    def below(self):
        return (lax.rem(self.sp + 4 * self.planes - 4, 4 * self.planes), self.c)

    def barrier(self):
        sem = pltpu.get_barrier_semaphore()
        for p in self.mates:
            pl.semaphore_signal(sem, inc=1, device_id=self.mate(p), device_id_type=MESH)
        pl.semaphore_signal(sem, inc=1, device_id=self.partner(), device_id_type=MESH)

        @pl.when(self.has_above)
        def _():
            pl.semaphore_signal(sem, inc=1, device_id=self.above(), device_id_type=MESH)

        @pl.when(self.has_below)
        def _():
            pl.semaphore_signal(sem, inc=1, device_id=self.below(), device_id_type=MESH)

        inner = self.has_above & self.has_below

        @pl.when(inner)
        def _():
            pl.semaphore_wait(sem, 6)

        @pl.when(jnp.logical_not(inner))
        def _():
            pl.semaphore_wait(sem, 5)


class Rows:
    def __init__(self, at, own, held, sems):
        self.at, self.own, self.held = at, own, held
        self.local_sem, self.near, self.recv, self.up, self.down = sems

    def slot(self, plane, p, cut=None):
        if cut is None:
            return self.held.at[plane, p]
        return self.held.at[plane, p, cut[0], cut[1]]

    def to_mate(self, index, p):
        at = self.at
        return [
            remote(
                src,
                self.slot(at.z, at.p, cut),
                self.near.at[index],
                self.recv.at[at.z, at.p],
                at.mate(p),
            )
            for src, cut, _ in self.own(p)
        ]

    def here(self):
        at = self.at
        return [
            pltpu.make_async_copy(src, self.slot(at.z, at.p, cut), self.local_sem.at[k])
            for k, (src, cut, copied) in enumerate(self.own(at.p))
            if copied
        ]

    def hop(self, plane, p, upward, src=None, cut=None):
        at = self.at
        dst = self.slot(plane, p, cut)
        return remote(
            dst if src is None else src,
            dst,
            (self.up if upward else self.down).at[plane, p],
            self.recv.at[plane, p],
            at.above() if upward else at.below(),
        )

    def send(self, plane, p, upward):
        @pl.when(self.at.has_above if upward else self.at.has_below)
        def _():
            self.hop(plane, p, upward).start()

    def begin_far(self):
        at = self.at
        for upward in (True, False):

            @pl.when(at.has_above if upward else at.has_below)
            def _():
                for src, cut, _ in self.own(at.p):
                    self.hop(at.z, at.p, upward, src, cut).start()

    def begin_near(self):
        for index, p in enumerate(self.at.mates):
            for copy in self.to_mate(index, p):
                copy.start()
        for copy in self.here():
            copy.start()

    def arrived(self, plane, p):
        self.hop(plane, p, True).wait_recv()

    def pass_near(self):
        at = self.at
        for p in at.mates:
            self.arrived(at.z, p)
            self.send(at.z, p, True)
            self.send(at.z, p, False)

    def pass_far(self, distance, index):
        at = self.at
        p = ((at.p,) + at.mates)[index]
        low, high = at.z - distance, at.z + distance

        @pl.when(low >= 0)
        def _():
            self.arrived(low, p)
            self.send(low, p, True)

        @pl.when(high < at.planes)
        def _():
            self.arrived(high, p)
            self.send(high, p, False)

    def finish(self):
        at = self.at
        whole = self.slot(at.z, at.p)
        for index, p in enumerate(at.mates):
            remote(
                whole, whole, self.near.at[index], self.recv.at[at.z, at.p], at.mate(p)
            ).wait_send()
        for plane in range(at.planes):
            for p in range(4):

                @pl.when(at.has_above & (at.z >= plane))
                def _():
                    self.hop(plane, p, True).wait_send()

                @pl.when(at.has_below & (at.z <= plane))
                def _():
                    self.hop(plane, p, False).wait_send()


def layer_kernel(planes, head, *refs):
    (tok, gain, w_query, w_key, w_value, w_pool, query_gain, key_gain) = refs[:8]
    (sinks, mix, pool_scale, w_attn, w_mixed, out) = refs[8:14]
    (raw, xs, ws, kvw, acc, q, kv, pool, kv_halo, pool_halo, ma, ws_out, ys) = refs[14:27]
    kv_before, pool_before = refs[-2:]
    in_sems, out_sems = refs[27:32], refs[32:37]
    (raw_sems, t_send, t_recv, td_send, td_recv, h_send, h_recv) = refs[37:44]
    (m_send, m_recv, f_send, f_recv, d_send, d_recv, r_send, r_recv, r_local) = refs[44:-2]

    at = Place(planes)
    c, p, z = at.c, at.p, at.z
    pair = 2 * head
    count, half = tok.shape
    part = count // 2
    deep = xs.shape[3]
    blocks = half // deep
    width, channels = q.shape[1], pool.shape[1]
    steps, tall, wide = ma.shape[1:]
    block = tall // 4
    columns = ws_out.shape[3]
    lag_rows = pool_halo.shape[0]

    low_lane = lax.broadcasted_iota(jnp.int32, (w_key.shape[0], pair), 1) < head
    for k in range(4):
        tile = slice(k // 2 * pair, (k // 2 + 1) * pair)
        key_tile, value_tile = w_key[:, tile], w_value[:, tile]
        if k % 2:
            key_tile = pltpu.roll(key_tile.astype(jnp.float32), head, 1).astype(jnp.bfloat16)
        else:
            value_tile = pltpu.roll(value_tile.astype(jnp.float32), head, 1).astype(jnp.bfloat16)
        kvw[k] = jnp.where(low_lane, key_tile, value_tile)
    ws[z, p, :, width : width + pair] = kvw[p]

    every = pl.ds(0, w_query.shape[0])

    def own_in(place):
        return [
            (w_query.at[:, aligned(place, width)], (every, pl.ds(0, width)), True),
            (kvw.at[place], (every, pl.ds(width, pair)), False),
            (w_pool.at[:, aligned(place, channels)], (every, pl.ds(width + pair, channels)), True),
        ]

    def own_out(place):
        rows = w_attn.shape[0]
        return [
            (w_attn.at[:, aligned(place, columns)], (pl.ds(0, rows), pl.ds(0, columns)), True),
            (w_mixed.at[:, aligned(place, columns)], (pl.ds(rows, rows), pl.ds(0, columns)), True),
        ]

    rows_in = Rows(at, own_in, ws, in_sems)
    rows_out = Rows(at, own_out, ws_out, out_sems)

    at.barrier()
    raw_local = pltpu.make_async_copy(tok, raw.at[c], raw_sems.at[0])
    raw_away = remote(tok, raw.at[c], raw_sems.at[1], raw_sems.at[2], at.partner())
    raw_away.start()
    raw_local.start()
    rows_in.begin_far()
    rows_in.begin_near()
    raw_local.wait()
    raw_away.wait_recv()

    norm_rows = 32

    def norm_step(index, carry):
        span = aligned(index, norm_rows)
        halves = [raw[k, span, :].astype(jnp.float32) for k in range(2)]
        total = sum(jnp.sum(v * v, axis=-1, keepdims=True) for v in halves)
        scale = lax.rsqrt(total / (2 * half) + epsilon)
        for k in range(2):
            normed = halves[k] * scale * gain[:, k * half : (k + 1) * half]
            normed = normed.astype(jnp.bfloat16)
            for b in range(blocks):
                xs[p, k * blocks + b, span, :] = normed[:, b * deep : (b + 1) * deep]
        return carry

    lax.fori_loop(0, count // norm_rows, norm_step, 0)

    def piece(place, h, core):
        return xs.at[place, pl.ds(core * blocks, blocks), pl.ds(h * part, part), :]

    def tokens_to(index, place, h, to):
        ref = piece(place, h, c)
        return remote(ref, ref, t_send.at[index], t_recv.at[place, h], at.mate(to))

    def tokens_over(index, place, h, core):
        ref = piece(place, h, core)
        return remote(ref, ref, td_send.at[index], td_recv.at[place, h], at.partner())

    sent = [(p, 0, at.xn), (p, 1, at.yn), (p, 1, at.xn), (p, 0, at.yn)]
    sent += [(at.xn, 0, at.yn), (at.yn, 1, at.xn)]
    crossed = [(at.xn, 0), (at.yn, 1), (at.xn, 1), (at.yn, 0), (at.dg, 0), (at.dg, 1)]
    for index in range(4):
        tokens_to(index, *sent[index]).start()
    rows_in.pass_near()

    def take_tokens(index, onward=None):
        place, h = crossed[index]
        tokens_to(0, place, h, at.xn).wait_recv()
        if onward is not None:
            tokens_to(onward, *sent[onward]).start()
        tokens_over(index, place, h, c).start()

    def first_tokens():
        take_tokens(0, 4)
        take_tokens(1, 5)

    def second_tokens():
        take_tokens(2)
        take_tokens(3)
        rows_out.begin_far()
        rows_out.begin_near()
        for place, h in crossed[:4]:
            tokens_over(0, place, h, 1 - c).wait_recv()
        for copy in rows_in.here():
            copy.wait()

    def product(place, b, span):
        return jnp.dot(
            xs[place, b, span, :],
            ws[b].reshape(deep, ws.shape[3]),
            preferred_element_type=jnp.float32,
        )

    def near_place(k):
        return jnp.where(k == 0, p, jnp.where(k == 1, at.xn, at.yn))

    def accumulate(b, fresh=False):
        def one(index, carry):
            k, h = lax.div(index, 2), lax.rem(index, 2)
            span = aligned(h, part)
            term = product(near_place(k), b, span)
            acc[k, span, :] = term if fresh else acc[k, span, :] + term
            return carry

        lax.fori_loop(0, 6, one, 0)

    def accumulate_own():
        accumulate(z, True)

    def accumulate_far(distance, sign):
        def run():
            b = z + sign * distance

            @pl.when((b >= 0) & (b < planes))
            def _():
                accumulate(b)

        return run

    units = [(0, accumulate_own)]
    for distance in range(1, planes):
        units += [(distance, accumulate_far(distance, -1)), (distance, accumulate_far(distance, 1))]
    events = [first_tokens, second_tokens]
    due = [4 * planes // 3, 2 * planes]
    for at_step in range(4 * (planes - 1)):
        rows_in.pass_far(at_step // 4 + 1, at_step % 4)
        while events and at_step >= due[0]:
            events.pop(0)()
            due.pop(0)
        for _ in range(2):
            if not events and units and units[0][0] <= (at_step + 1) // 4:
                units.pop(0)[1]()
    for event in events:
        event()
    for _, unit in units:
        unit()
    take_tokens(4)
    take_tokens(5)

    low_part = lax.broadcasted_iota(jnp.int32, (part, pair), 1) < head
    query_pair = jnp.concatenate([query_gain[...]] * 2, axis=1)
    key_pair = jnp.concatenate([key_gain[...]] * 2, axis=1)

    def settle(total, place, h):
        span = aligned(place * 2 + h, part)
        for k in range(width // pair):
            v = total[:, pair * k : pair * (k + 1)]
            square = v * v
            lo = jnp.sum(jnp.where(low_part, square, 0.0), axis=-1, keepdims=True) / head
            hi = jnp.sum(jnp.where(low_part, 0.0, square), axis=-1, keepdims=True) / head
            scale = jnp.where(low_part, lax.rsqrt(lo + epsilon), lax.rsqrt(hi + epsilon))
            q[span, pair * k : pair * (k + 1)] = (v * scale * query_pair).astype(jnp.bfloat16)
        v = total[:, width : width + pair]
        lo = jnp.sum(jnp.where(low_part, v * v, 0.0), axis=-1, keepdims=True) / head
        both = jnp.where(low_part, v * lax.rsqrt(lo + epsilon) * key_pair, v)
        kv[span, :pair] = both.astype(jnp.bfloat16)
        kv[span, pair:] = pltpu.roll(both, head, 1).astype(jnp.bfloat16)
        pool[span, :] = total[:, width + pair :].astype(jnp.bfloat16)

    def settle_near(index, carry):
        k, h = lax.div(index, 2), lax.rem(index, 2)
        settle(acc[k, aligned(h, part), :], near_place(k), h)
        return carry

    lax.fori_loop(0, 6, settle_near, 0)
    for h in range(2):
        tokens_over(0, at.dg, h, 1 - c).wait_recv()

    def settle_across(h, carry):
        total = None
        for b in range(planes):
            term = product(at.dg, b, aligned(h, part))
            total = term if total is None else total + term
        settle(total, at.dg, h)
        return carry

    lax.fori_loop(0, 2, settle_across, 0)

    def halo(k):
        src, dst = (kv, kv_halo) if k == 0 else (pool, pool_halo)
        rows = dst.shape[0]
        return remote(
            src.at[pl.ds(4 * count - rows, rows), :], dst, h_send.at[k], h_recv.at[k], at.above()
        )

    @pl.when(at.has_above)
    def _():
        halo(0).start()
        halo(1).start()

    @pl.when(z == 0)
    def _():
        kv_halo[...] = jnp.zeros_like(kv_halo)
        pool_halo[...] = jnp.zeros_like(pool_halo)

    query = lax.broadcasted_iota(jnp.int32, (block, 2 * block), 0)
    key = lax.broadcasted_iota(jnp.int32, (block, 2 * block), 1)
    band = (key > query) & (key <= query + block)
    low_keys = lax.broadcasted_iota(jnp.int32, (2 * block, pair), 1) < head
    line = lax.broadcasted_iota(jnp.int32, (block, channels), 0)
    window = lax.shift_left(jnp.int32(2), p).astype(jnp.float32)
    heads = width // head
    slot = c * 4 + p

    def mixers(j, place):
        index = place * steps + j
        base = pl.multiple_of(index * block, block)
        first = index == 0
        before = pl.multiple_of(jnp.maximum(base - block, 0), block)
        lag_before = pl.multiple_of(jnp.maximum(base - lag_rows, 0), lag_rows)

        @pl.when(first)
        def _():
            kv_before[...] = kv_halo[...]
            pool_before[...] = pool_halo[...]

        @pl.when(jnp.logical_not(first))
        def _():
            kv_before[...] = kv[pl.ds(before, block), :]
            pool_before[...] = pool[pl.ds(lag_before, lag_rows), :]

        kvs = jnp.concatenate([kv_before[...], kv[pl.ds(base, block), :]], axis=0)
        straight, turned = kvs[:, :pair], kvs[:, pair:]
        zero = jnp.zeros_like(straight)
        keys = (jnp.where(low_keys, straight, zero), jnp.where(low_keys, zero, turned))
        values = (jnp.where(low_keys, turned, zero), jnp.where(low_keys, zero, straight))
        valid = band & (key >= jnp.where((z == 0) & first, block, 0))
        span = aligned(place, block)
        for k in range(heads // 2):
            q_pair = q[pl.ds(base, block), pair * k : pair * (k + 1)]
            total = None
            for side in range(2):
                sink = sinks[p * heads + 2 * k + side]
                scores = lax.dot_general(
                    q_pair,
                    keys[side],
                    (((1,), (1,)), ((), ())),
                    preferred_element_type=jnp.float32,
                ) * head ** (-0.5)
                scores = jnp.where(valid, scores, NEGATIVE)
                top = jnp.maximum(jnp.max(scores, axis=-1, keepdims=True), sink)
                lifted = jnp.exp(scores - top)
                under = jnp.sum(lifted, axis=-1, keepdims=True) + jnp.exp(sink - top)
                weights = (lifted / under).astype(jnp.bfloat16)
                term = jnp.dot(weights, values[side], preferred_element_type=jnp.float32)
                total = term if total is None else total + term
            ma[slot, j, span, 2 * pair * k : 2 * pair * k + pair] = total.astype(jnp.bfloat16)
        series = jnp.concatenate([pool_before[...], pool[pl.ds(base, block), :]], axis=0)
        series = series.astype(jnp.float32)
        sums, lag = [series], 1
        while 2 * lag <= lag_rows:
            sums.append(sums[-1] + pltpu.roll(sums[-1], lag, 0))
            lag *= 2
        window_sum = sums[-1]
        for k in range(len(sums) - 2, 0, -1):
            window_sum = jnp.where(p == k - 1, sums[k], window_sum)
        position = (z * 4 * count + base + 1 + line).astype(jnp.float32)
        contrast = window_sum[lag_rows:] / jnp.minimum(position, window) - series[lag_rows:]
        mixed = jnp.dot(contrast.astype(jnp.bfloat16), mix[p], preferred_element_type=jnp.float32)
        mixed = (mixed * pool_scale[:, aligned(p, channels)]).astype(jnp.bfloat16)
        for k in range(channels // pair):
            ma[slot, j, span, (2 * k + 1) * pair : (2 * k + 2) * pair] = mixed[
                :, pair * k : pair * (k + 1)
            ]

    def to_mate(index, j, to):
        ref = ma.at[slot, j]
        return remote(ref, ref, m_send.at[index, j], m_recv.at[p, j], at.mate(to))

    def onward(k, j, place, to):
        ref = ma.at[c * 4 + place, j, pl.ds(k * (tall // 2), tall // 2), :]
        return remote(ref, ref, f_send.at[k, j], f_recv.at[k, j], at.mate(to))

    def over(index, j, place, core):
        ref = ma.at[core * 4 + place, j]
        return remote(ref, ref, d_send.at[index, j], d_recv.at[place, j], at.partner())

    def came(place, j):
        ref = ma.at[c * 4 + place, j]
        remote(ref, ref, m_send.at[0, j], m_recv.at[place, j], at.partner()).wait_recv()

    def mix_step(index, carry):
        j = steps - 1 - index

        @pl.when((j == 0) & at.has_below)
        def _():
            halo(0).wait_recv()
            halo(1).wait_recv()

        def one(place, inner):
            mixers(j, place)
            return inner

        lax.fori_loop(0, 4, one, 0)
        to_mate(0, j, at.xn).start()
        to_mate(1, j, at.yn).start()
        over(0, j, p, c).start()

        @pl.when(index == 0)
        def _():
            rows_out.pass_near()

        return carry

    lax.fori_loop(0, steps, mix_step, 0)

    def pass_on(j):
        came(at.xn, j)
        onward(0, j, at.xn, at.yn).start()
        over(1, j, at.xn, c).start()
        came(at.yn, j)
        onward(1, j, at.yn, at.xn).start()
        over(2, j, at.yn, c).start()

    waiting = list(range(steps - 1, -1, -1))
    total_far = 4 * (planes - 1)
    for at_step in range(total_far):
        rows_out.pass_far(at_step // 4 + 1, at_step % 4)
        passed = steps - len(waiting)
        while waiting and at_step + 1 >= (passed + 1) * total_far // (steps + 1):
            pass_on(waiting.pop(0))
            passed += 1
    for j in waiting:
        pass_on(j)
    for copy in rows_out.here():
        copy.wait()

    def landing(j, place):
        return out.at[aligned(j, block), aligned(place, columns)]

    def result(index, j, to):
        return remote(
            ys.at[j, aligned(to, block), :],
            landing(j, p),
            r_send.at[index, j],
            r_recv.at[p, j],
            at.mate(to),
        )

    def result_here(j):
        return pltpu.make_async_copy(ys.at[j, aligned(p, block), :], landing(j, p), r_local.at[j])

    def last_step(index, carry):
        j = steps - 1 - index
        for k in range(2):
            onward(k, j, at.dg, at.xn).wait_recv()
        over(3, j, at.dg, c).start()
        for place in range(4):
            over(0, j, place, 1 - c).wait_recv()
        total = None
        for i in range(8):
            first = 2 * i
            weight = ws_out[first // 4, first % 4 : first % 4 + 2].reshape(wide, columns)
            term = jnp.dot(ma[i, j], weight, preferred_element_type=jnp.float32)
            total = term if total is None else total + term
        ys[j] = total.astype(jnp.bfloat16)
        for k, to in enumerate(at.mates):
            result(k, j, to).start()
        result_here(j).start()
        return carry

    lax.fori_loop(0, steps, last_step, 0)

    def finish_step(j, carry):
        for k, to in enumerate(at.mates):
            remote(
                ys.at[j, pl.ds(0, block), :],
                landing(j, to),
                r_send.at[k, j],
                r_recv.at[to, j],
                at.mate(to),
            ).wait_recv()
        result_here(j).wait()
        for k, to in enumerate(at.mates):
            result(k, j, to).wait_send()
        to_mate(0, j, at.xn).wait_send()
        to_mate(1, j, at.yn).wait_send()
        onward(0, j, at.xn, at.yn).wait_send()
        onward(1, j, at.yn, at.xn).wait_send()
        for k, place in enumerate((p,) + at.mates):
            over(k, j, place, c).wait_send()
        return carry

    lax.fori_loop(0, steps, finish_step, 0)
    raw_away.wait_send()
    for index in range(6):
        tokens_to(index, *sent[index]).wait_send()
        tokens_over(index, *crossed[index], c).wait_send()

    @pl.when(at.has_above)
    def _():
        halo(0).wait_send()
        halo(1).wait_send()

    rows_in.finish()
    rows_out.finish()


def per_device_planes(
    tokens,
    norm_gain,
    w_query,
    w_key,
    w_value,
    w_pool_in,
    query_gain,
    key_gain,
    sinks,
    w_mix,
    pool_scale,
    w_out_attn,
    w_out_pool,
):
    planes = lax.axis_size("sp") // 4
    head = query_gain.shape[0]
    count, half = tokens.shape
    in_rows, out_rows = w_query.shape[0], 2 * w_out_attn.shape[0]
    width, channels = w_query.shape[1] // 4, w_pool_in.shape[1] // 4
    columns = w_out_attn.shape[1] // 4
    pair, deep, steps = 2 * head, 4 * in_rows, count // WINDOW
    in_width = width + pair + channels
    vmem = pl.BlockSpec(memory_space=pltpu.VMEM)
    anywhere = pl.BlockSpec(memory_space=pl.ANY)
    smem = pl.BlockSpec(memory_space=pltpu.SMEM)
    dma = pltpu.SemaphoreType.DMA

    def held(*shape):
        return pltpu.VMEM(shape, jnp.bfloat16)

    row_sems = [dma((3,)), dma((3,)), dma((planes, 4)), dma((planes, 4)), dma((planes, 4))]
    return pl.pallas_call(
        functools.partial(layer_kernel, planes, head),
        out_shape=jax.ShapeDtypeStruct(tokens.shape, jnp.bfloat16),
        in_specs=[anywhere, vmem, anywhere, vmem, vmem, anywhere, vmem, vmem]
        + [smem, vmem, vmem, anywhere, anywhere],
        out_specs=anywhere,
        scratch_shapes=[
            held(2, count, half),
            held(4, planes, count, deep),
            held(planes, 4, in_rows, in_width),
            held(4, in_rows, pair),
            pltpu.VMEM((3, count, in_width), jnp.float32),
            held(4 * count, width),
            held(4 * count, 2 * pair),
            held(4 * count, channels),
            held(WINDOW, 2 * pair),
            held(longest_lag + 1, channels),
            held(8, steps, 4 * WINDOW, width + channels),
            held(planes, 4, out_rows, columns),
            held(steps, 4 * WINDOW, columns),
        ]
        + row_sems
        + row_sems
        + [dma((3,)), dma((6,)), dma((4, 2)), dma((6,)), dma((4, 2)), dma((2,)), dma((2,))]
        + [dma((2, steps)), dma((4, steps)), dma((2, steps)), dma((2, steps))]
        + [dma((4, steps)), dma((4, steps)), dma((3, steps)), dma((4, steps)), dma((steps,))]
        + [held(WINDOW, 2 * pair), held(longest_lag + 1, channels)],
        compiler_params=pltpu.CompilerParams(
            collective_id=0, has_side_effects=True, vmem_limit_bytes=63 * 2**20
        ),
        name="layer",
    )(
        tokens,
        norm_gain.reshape(1, -1),
        w_query,
        w_key,
        w_value,
        w_pool_in,
        query_gain.reshape(1, -1),
        key_gain.reshape(1, -1),
        sinks,
        w_mix,
        pool_scale.reshape(1, -1),
        w_out_attn,
        w_out_pool,
    )


def suits_planes(mesh, args):
    sp, tp = mesh.shape["sp"], mesh.shape["tp"]
    tokens, w_query, w_key, w_pool_in = args[0], args[2], args[3], args[5]
    head, groups = args[6].shape[0], args[9].shape[0]
    w_out_attn, w_out_pool = args[11], args[12]
    if tp != 2 or sp % 8 or 2 * head != 128:
        return False
    share = 4 * tp
    rows = tokens.shape[0] // sp
    width, channels = w_query.shape[1] // share, w_pool_in.shape[1] // share
    held = 2 * 4 * rows * tokens.shape[1] + 2 * w_query.shape[0] * (width + 128 + channels)
    return (
        w_key.shape[1] == share * head
        and groups == share
        and rows % (2 * WINDOW) == 0
        and width % 128 == 0
        and width == channels
        and 2 * w_out_attn.shape[0] // sp == width
        and 2 * w_out_pool.shape[0] // sp == channels
        and w_out_attn.shape[0] // sp == 2 * head
        and w_query.shape[0] // sp % 16 == 0
        and w_out_attn.shape[1] % (share * 128) == 0
        and held < 22 * 2**20
    )


def solution(mesh):
    sp, tp = mesh.shape["sp"], mesh.shape["tp"]

    def call(*args):
        if suits_planes(mesh, args):
            return jax.shard_map(
                per_device_planes,
                mesh=mesh,
                in_specs=(
                    P("sp", "tp"),
                    P(),
                    P("sp", "tp"),
                    P("sp", "tp"),
                    P("sp", "tp"),
                    P("sp", "tp"),
                    P(),
                    P(),
                    P("tp"),
                    P("tp", None, None),
                    P("tp"),
                    P("sp", "tp"),
                    P("sp", "tp"),
                ),
                out_specs=P("sp", "tp"),
                check_vma=False,
            )(*args)
        kv_local = args[3].shape[1] // args[6].shape[0] // tp
        groups_local = args[9].shape[0] // tp
        fits = sp % 2 == 0 and kv_local % 2 == 0 and groups_local % 2 == 0
        pair = 2 if fits else 1
        inner = Mesh(mesh.devices.reshape(sp // pair, pair, tp), ("so", "si", "tp"))
        rows = ("so", "si")
        return jax.shard_map(
            per_device,
            mesh=inner,
            in_specs=(
                P(rows, "tp"),
                P(),
                P(rows, "tp"),
                P(rows, "tp"),
                P(rows, "tp"),
                P(rows, "tp"),
                P(),
                P(),
                P("tp"),
                P("tp", None, None),
                P("tp"),
                P(rows, "tp"),
                P(rows, "tp"),
            ),
            out_specs=P(rows, "tp"),
            check_vma=False,
        )(*args)

    return call
```

```python
import functools

import jax
import jax.numpy as jnp
from jax import lax
from jax.experimental import pallas as pl
from jax.experimental.pallas import tpu as pltpu
from jax.sharding import Mesh
from jax.sharding import PartitionSpec as P

WINDOW = 128


epsilon = 1e-06
longest_lag = 15


def from_behind(block, axis):
    devices = range(lax.axis_size(axis))
    route = [(i - 1, i) for i in devices if i - 1 in devices]
    return lax.ppermute(block, axis, route)


def swap(block, axis):
    count = lax.axis_size(axis)
    return lax.ppermute(block, axis, [(i, count - 1 - i) for i in range(count)])


def row_norm(values, gain):
    return values * lax.rsqrt(jnp.mean(values * values, axis=-1, keepdims=True) + epsilon) * gain


def after(value, *others):
    return lax.optimization_barrier((value,) + others)[0]


def ordered(mine, theirs, index, dim):
    return jnp.where(
        index == 0,
        jnp.concatenate([mine, theirs], axis=dim),
        jnp.concatenate([theirs, mine], axis=dim),
    )


def both_cores(block, dim):
    if lax.axis_size("tp") == 2:
        return ordered(block, swap(block, "tp"), lax.axis_index("tp"), dim)
    return lax.all_gather(block, "tp", axis=dim, tiled=True)


def per_device(
    tokens,
    norm_gain,
    w_query,
    w_key,
    w_value,
    w_pool_in,
    query_gain,
    key_gain,
    sinks,
    w_mix,
    pool_scale,
    w_out_attn,
    w_out_pool,
):
    pair = lax.axis_size("si")
    place = lax.axis_index("si")
    outer = lax.axis_index("so")

    def share(array, owner, dim):
        size = array.shape[dim] // pair
        return lax.dynamic_slice_in_dim(array, owner * size, size, dim)

    def mine(arrays):
        return [share(a, place, 1) for a in arrays]

    def other(arrays):
        return [share(a, pair - 1 - place, 1) for a in arrays]

    def joined(own, came, dim):
        return own if pair == 1 else ordered(own, came, place, dim)

    def gathered(rows):
        return lax.all_gather(rows, "so", axis=0, tiled=True)

    qkv_parts = (w_query, w_key, w_value)
    qkv_own = jnp.concatenate(mine(qkv_parts), axis=1)
    if pair == 1:
        qkv_rows, pool_rows, attn_rows, mixed_rows = qkv_own, w_pool_in, w_out_attn, w_out_pool
        row_half = tokens
    else:
        qkv_came = swap(jnp.concatenate(other(qkv_parts), axis=1), "si")
        qkv_rows = joined(qkv_own, qkv_came, 0)
        late = lax.optimization_barrier((w_pool_in, w_out_attn, w_out_pool, qkv_came))[:3]
        came = [swap(share(w, pair - 1 - place, 1), "si") for w in late]
        pool_rows, attn_rows, mixed_rows = [
            joined(share(w, place, 1), c, 0) for w, c in zip((w_pool_in, w_out_attn, w_out_pool), came)
        ]
        row_half = joined(tokens, swap(after(tokens, qkv_came), "si"), 0)
    w_qkv = gathered(qkv_rows)
    w_pool = gathered(after(pool_rows, w_qkv))
    w_attn = gathered(after(attn_rows, w_pool))
    w_mixed = gathered(after(mixed_rows, w_attn))

    whole = both_cores(row_half, 1)
    row_count = whole.shape[0]
    normed = row_norm(whole.astype(jnp.float32), norm_gain).astype(jnp.bfloat16)
    qkv_raw = jnp.dot(normed, w_qkv, preferred_element_type=jnp.float32)
    head_size = query_gain.shape[0]
    query_width = w_query.shape[1] // pair
    kv_width = w_key.shape[1] // pair
    query_heads = query_width // head_size
    kv_local = kv_width // head_size
    per_kv = query_heads // kv_local
    query_raw = qkv_raw[:, :query_width]
    key_raw = qkv_raw[:, query_width : query_width + kv_width]
    value_raw = qkv_raw[:, query_width + kv_width :]
    queries = row_norm(query_raw.reshape(row_count, query_heads, head_size), query_gain).astype(
        jnp.bfloat16
    )
    key_rows = row_norm(key_raw.reshape(row_count, kv_local, head_size), key_gain).astype(
        jnp.bfloat16
    )
    values = value_raw.astype(jnp.bfloat16).reshape(row_count, kv_local, head_size)
    kv_tail = jnp.concatenate(
        [key_rows[-WINDOW:].reshape(WINDOW, -1), values[-WINDOW:].reshape(WINDOW, -1)], axis=1
    )
    kv_prev = from_behind(kv_tail, "so").reshape(WINDOW, 2, kv_local, head_size)
    offset = outer * row_count
    blocks = row_count // WINDOW

    def banded(previous, source):
        earlier = jnp.concatenate([previous, source[: row_count - WINDOW]], axis=0).reshape(
            blocks, WINDOW, kv_local, head_size
        )
        return jnp.concatenate(
            [earlier, source.reshape(blocks, WINDOW, kv_local, head_size)], axis=1
        )

    band_keys = banded(kv_prev[:, 0], key_rows)
    band_values = banded(kv_prev[:, 1], values)
    query_blocks = queries.reshape(blocks, WINDOW, kv_local, per_kv, head_size)
    scores = jnp.einsum(
        "bqkgd,bjkd->bkgqj", query_blocks, band_keys, preferred_element_type=jnp.float32
    ) * head_size ** (-0.5)
    query_index = jnp.arange(WINDOW)[:, None]
    key_index = jnp.arange(2 * WINDOW)[None, :]
    distance = query_index + WINDOW - key_index
    key_pos = offset + jnp.arange(blocks)[:, None, None] * WINDOW - WINDOW + key_index[None]
    valid = (distance[None] >= 0) & (distance[None] < WINDOW) & (key_pos >= 0)
    sink_logit = share(sinks, place, 0).reshape(kv_local, per_kv)[None, :, :, None, None]
    scores = jnp.where(valid[:, None, None], scores, -1e30)
    row_top = jnp.maximum(scores.max(axis=-1, keepdims=True), sink_logit)
    lifted = jnp.exp(scores - row_top)
    weights = (
        lifted / (lifted.sum(axis=-1, keepdims=True) + jnp.exp(sink_logit - row_top))
    ).astype(jnp.bfloat16)
    attended = (
        jnp.einsum("bkgqj,bjkd->bqkgd", weights, band_values, preferred_element_type=jnp.float32)
        .astype(jnp.bfloat16)
        .reshape(row_count, query_heads * head_size)
    )

    def all_heads(block):
        if pair == 2:
            block = joined(block, swap(block, "si"), 1)
        return both_cores(block, 1)

    attended_all = all_heads(attended)

    pool_in = jnp.dot(normed, w_pool, preferred_element_type=jnp.float32).astype(jnp.bfloat16)
    pool_prev = from_behind(pool_in[-longest_lag:], "so")
    mix = share(w_mix, place, 0)
    groups_local = mix.shape[0]
    group_dim = mix.shape[1]
    first_group = (lax.axis_index("tp") * pair + place) * groups_local
    group_ids = first_group + jnp.arange(groups_local, dtype=jnp.int32)
    spans = jnp.repeat(jnp.left_shift(jnp.int32(2), group_ids % 4), group_dim)
    extended = jnp.concatenate([pool_prev, pool_in], axis=0).astype(jnp.float32)
    window_sum = jnp.zeros((row_count, spans.shape[0]), jnp.float32)
    for back_step in range(longest_lag + 1):
        shifted = extended[longest_lag - back_step : longest_lag - back_step + row_count]
        window_sum = window_sum + jnp.where(back_step < spans[None, :], shifted, 0.0)
    positions = (offset + jnp.arange(1, row_count + 1, dtype=jnp.int32)).astype(jnp.float32)
    divisor = jnp.minimum(positions[:, None], spans.astype(jnp.float32)[None, :])
    contrast = (window_sum / divisor - extended[longest_lag:]).astype(jnp.bfloat16)
    mixed = jnp.einsum(
        "tgc,gcd->tgd",
        contrast.reshape(row_count, groups_local, group_dim),
        mix,
        preferred_element_type=jnp.float32,
    ).reshape(row_count, -1)
    pooled = (mixed * share(pool_scale, place, 0)).astype(jnp.bfloat16)
    pooled_all = all_heads(pooled)

    def project(owner):
        total = jnp.dot(share(attended_all, owner, 0), w_attn, preferred_element_type=jnp.float32)
        result = total + jnp.dot(
            share(pooled_all, owner, 0), w_mixed, preferred_element_type=jnp.float32
        )
        return result.astype(jnp.bfloat16)

    if pair == 1:
        return project(0)
    away = project(pair - 1 - place)
    came_back = swap(away, "si")
    return joined(project(place), came_back, 1)


MESH = pl.DeviceIdType.MESH
NEGATIVE = -1e30


def remote(src, dst, send_sem, recv_sem, device):
    return pltpu.make_async_remote_copy(
        src_ref=src,
        dst_ref=dst,
        send_sem=send_sem,
        recv_sem=recv_sem,
        device_id=device,
        device_id_type=MESH,
    )


def aligned(index, size):
    return pl.ds(pl.multiple_of(index * size, size), size)


class Place:
    def __init__(self, planes):
        self.sp, self.c = lax.axis_index("sp"), lax.axis_index("tp")
        self.planes = planes
        self.z, self.p = lax.div(self.sp, 4), lax.rem(self.sp, 4)
        x, y = lax.rem(self.p, 2), lax.div(self.p, 2)
        self.xn, self.yn, self.dg = self.p + 1 - 2 * x, self.p + 2 - 4 * y, 3 - self.p
        self.mates = (self.xn, self.yn, self.dg)
        self.has_above, self.has_below = self.z < planes - 1, self.z > 0

    def mate(self, p):
        return (self.z * 4 + p, self.c)

    def partner(self):
        return (self.sp, 1 - self.c)

    def above(self):
        return (lax.rem(self.sp + 4, 4 * self.planes), self.c)

    def below(self):
        return (lax.rem(self.sp + 4 * self.planes - 4, 4 * self.planes), self.c)

    def barrier(self):
        sem = pltpu.get_barrier_semaphore()
        for p in self.mates:
            pl.semaphore_signal(sem, inc=1, device_id=self.mate(p), device_id_type=MESH)
        pl.semaphore_signal(sem, inc=1, device_id=self.partner(), device_id_type=MESH)

        @pl.when(self.has_above)
        def _():
            pl.semaphore_signal(sem, inc=1, device_id=self.above(), device_id_type=MESH)

        @pl.when(self.has_below)
        def _():
            pl.semaphore_signal(sem, inc=1, device_id=self.below(), device_id_type=MESH)

        inner = self.has_above & self.has_below

        @pl.when(inner)
        def _():
            pl.semaphore_wait(sem, 6)

        @pl.when(jnp.logical_not(inner))
        def _():
            pl.semaphore_wait(sem, 5)


class Rows:
    def __init__(self, at, own, held, sems):
        self.at, self.own, self.held = at, own, held
        self.local_sem, self.near, self.recv, self.up, self.down = sems

    def slot(self, plane, p, cut=None):
        if cut is None:
            return self.held.at[plane, p]
        return self.held.at[plane, p, cut[0], cut[1]]

    def to_mate(self, index, p):
        at = self.at
        return [
            remote(
                src,
                self.slot(at.z, at.p, cut),
                self.near.at[index],
                self.recv.at[at.z, at.p],
                at.mate(p),
            )
            for src, cut, _ in self.own(p)
        ]

    def here(self):
        at = self.at
        return [
            pltpu.make_async_copy(src, self.slot(at.z, at.p, cut), self.local_sem.at[k])
            for k, (src, cut, copied) in enumerate(self.own(at.p))
            if copied
        ]

    def hop(self, plane, p, upward, src=None, cut=None):
        at = self.at
        dst = self.slot(plane, p, cut)
        return remote(
            dst if src is None else src,
            dst,
            (self.up if upward else self.down).at[plane, p],
            self.recv.at[plane, p],
            at.above() if upward else at.below(),
        )

    def send(self, plane, p, upward):
        @pl.when(self.at.has_above if upward else self.at.has_below)
        def _():
            self.hop(plane, p, upward).start()

    def begin_far(self):
        at = self.at
        for upward in (True, False):

            @pl.when(at.has_above if upward else at.has_below)
            def _():
                for src, cut, _ in self.own(at.p):
                    self.hop(at.z, at.p, upward, src, cut).start()

    def begin_near(self):
        for index, p in enumerate(self.at.mates):
            for copy in self.to_mate(index, p):
                copy.start()
        for copy in self.here():
            copy.start()

    def arrived(self, plane, p):
        self.hop(plane, p, True).wait_recv()

    def pass_near(self):
        at = self.at
        for p in at.mates:
            self.arrived(at.z, p)
            self.send(at.z, p, True)
            self.send(at.z, p, False)

    def pass_far(self, distance, index):
        at = self.at
        p = ((at.p,) + at.mates)[index]
        low, high = at.z - distance, at.z + distance

        @pl.when(low >= 0)
        def _():
            self.arrived(low, p)
            self.send(low, p, True)

        @pl.when(high < at.planes)
        def _():
            self.arrived(high, p)
            self.send(high, p, False)

    def finish(self):
        at = self.at
        whole = self.slot(at.z, at.p)
        for index, p in enumerate(at.mates):
            remote(
                whole, whole, self.near.at[index], self.recv.at[at.z, at.p], at.mate(p)
            ).wait_send()
        for plane in range(at.planes):
            for p in range(4):

                @pl.when(at.has_above & (at.z >= plane))
                def _():
                    self.hop(plane, p, True).wait_send()

                @pl.when(at.has_below & (at.z <= plane))
                def _():
                    self.hop(plane, p, False).wait_send()


def layer_kernel(planes, head, *refs):
    (tok, gain, w_query, w_key, w_value, w_pool, query_gain, key_gain) = refs[:8]
    (sinks, mix, pool_scale, w_attn, w_mixed, out) = refs[8:14]
    (raw, xs, ws, kvw, acc, q, kv, pool, kv_halo, pool_halo, ma, ws_out, ys) = refs[14:27]
    kv_before, pool_before = refs[-2:]
    in_sems, out_sems = refs[27:32], refs[32:37]
    (raw_sems, t_send, t_recv, td_send, td_recv, h_send, h_recv) = refs[37:44]
    (m_send, m_recv, f_send, f_recv, d_send, d_recv, r_send, r_recv, r_local) = refs[44:-2]

    at = Place(planes)
    c, p, z = at.c, at.p, at.z
    pair = 2 * head
    count, half = tok.shape
    part = count // 2
    deep = xs.shape[3]
    blocks = half // deep
    width, channels = q.shape[1], pool.shape[1]
    steps, tall, wide = ma.shape[1:]
    block = tall // 4
    columns = ws_out.shape[3]
    lag_rows = pool_halo.shape[0]

    low_lane = lax.broadcasted_iota(jnp.int32, (w_key.shape[0], pair), 1) < head
    for k in range(4):
        tile = slice(k // 2 * pair, (k // 2 + 1) * pair)
        key_tile, value_tile = w_key[:, tile], w_value[:, tile]
        if k % 2:
            key_tile = pltpu.roll(key_tile.astype(jnp.float32), head, 1).astype(jnp.bfloat16)
        else:
            value_tile = pltpu.roll(value_tile.astype(jnp.float32), head, 1).astype(jnp.bfloat16)
        kvw[k] = jnp.where(low_lane, key_tile, value_tile)
    ws[z, p, :, width : width + pair] = kvw[p]

    every = pl.ds(0, w_query.shape[0])

    def own_in(place):
        return [
            (w_query.at[:, aligned(place, width)], (every, pl.ds(0, width)), True),
            (kvw.at[place], (every, pl.ds(width, pair)), False),
            (w_pool.at[:, aligned(place, channels)], (every, pl.ds(width + pair, channels)), True),
        ]

    def own_out(place):
        rows = w_attn.shape[0]
        return [
            (w_attn.at[:, aligned(place, columns)], (pl.ds(0, rows), pl.ds(0, columns)), True),
            (w_mixed.at[:, aligned(place, columns)], (pl.ds(rows, rows), pl.ds(0, columns)), True),
        ]

    rows_in = Rows(at, own_in, ws, in_sems)
    rows_out = Rows(at, own_out, ws_out, out_sems)

    at.barrier()
    raw_local = pltpu.make_async_copy(tok, raw.at[c], raw_sems.at[0])
    raw_away = remote(tok, raw.at[c], raw_sems.at[1], raw_sems.at[2], at.partner())
    raw_away.start()
    raw_local.start()
    rows_in.begin_far()
    rows_in.begin_near()
    raw_local.wait()
    raw_away.wait_recv()

    norm_rows = 32

    def norm_step(index, carry):
        span = aligned(index, norm_rows)
        halves = [raw[k, span, :].astype(jnp.float32) for k in range(2)]
        total = sum(jnp.sum(v * v, axis=-1, keepdims=True) for v in halves)
        scale = lax.rsqrt(total / (2 * half) + epsilon)
        for k in range(2):
            normed = halves[k] * scale * gain[:, k * half : (k + 1) * half]
            normed = normed.astype(jnp.bfloat16)
            for b in range(blocks):
                xs[p, k * blocks + b, span, :] = normed[:, b * deep : (b + 1) * deep]
        return carry

    lax.fori_loop(0, count // norm_rows, norm_step, 0)

    def piece(place, h, core):
        return xs.at[place, pl.ds(core * blocks, blocks), pl.ds(h * part, part), :]

    def tokens_to(index, place, h, to):
        ref = piece(place, h, c)
        return remote(ref, ref, t_send.at[index], t_recv.at[place, h], at.mate(to))

    def tokens_over(index, place, h, core):
        ref = piece(place, h, core)
        return remote(ref, ref, td_send.at[index], td_recv.at[place, h], at.partner())

    sent = [(p, 0, at.xn), (p, 1, at.yn), (p, 1, at.xn), (p, 0, at.yn)]
    sent += [(at.xn, 0, at.yn), (at.yn, 1, at.xn)]
    crossed = [(at.xn, 0), (at.yn, 1), (at.xn, 1), (at.yn, 0), (at.dg, 0), (at.dg, 1)]
    for index in range(4):
        tokens_to(index, *sent[index]).start()
    rows_in.pass_near()

    def take_tokens(index, onward=None):
        place, h = crossed[index]
        tokens_to(0, place, h, at.xn).wait_recv()
        if onward is not None:
            tokens_to(onward, *sent[onward]).start()
        tokens_over(index, place, h, c).start()

    def first_tokens():
        take_tokens(0, 4)
        take_tokens(1, 5)

    def second_tokens():
        take_tokens(2)
        take_tokens(3)
        rows_out.begin_far()
        rows_out.begin_near()
        for place, h in crossed[:4]:
            tokens_over(0, place, h, 1 - c).wait_recv()
        for copy in rows_in.here():
            copy.wait()

    def product(place, b, span, slots):
        if slots is None:
            return jnp.dot(
                xs[place, b, span, :],
                ws[b].reshape(deep, ws.shape[3]),
                preferred_element_type=jnp.float32,
            )
        total = None
        for source in slots:
            term = jnp.dot(
                xs[place, b, span, aligned(source, deep // 4)],
                ws[b, source],
                preferred_element_type=jnp.float32,
            )
            total = term if total is None else total + term
        return total

    def place_of(k):
        return jnp.where(k == 0, p, jnp.where(k == 1, at.xn, jnp.where(k == 2, at.yn, at.dg)))

    def accumulate(b, places, slots=None, fresh=False):
        def one(index, carry):
            k, span = places[0] + lax.div(index, 2), aligned(lax.rem(index, 2), part)
            term = product(place_of(k), b, span, slots)
            acc[k, span, :] = term if fresh else acc[k, span, :] + term
            return carry

        lax.fori_loop(0, 2 * (places[1] - places[0]), one, 0)

    near, across, everywhere = (0, 3), (3, 4), (0, 4)
    early, late = (p, at.xn, at.yn), (at.dg,)

    def far_unit(distance, places, slots=None):
        def run():
            for b in (z - distance, z + distance):

                @pl.when((b >= 0) & (b < planes))
                def _():
                    accumulate(b, places, slots)

        return run

    def last_tokens():
        take_tokens(4)
        take_tokens(5)
        for h in range(2):
            tokens_over(0, at.dg, h, 1 - c).wait_recv()

    def across_unit():
        accumulate(z, across, fresh=True)
        for distance in range(1, planes - 1):
            far_unit(distance, across)()
        far_unit(planes - 1, across, early)()

    final = 4 * (planes - 1) - 1
    events = {4 * planes // 3: [first_tokens], 2 * planes: [second_tokens]}
    events[2 * planes].append(lambda: accumulate(z, near, fresh=True))
    for distance in range(1, planes - 1):
        step = max(2 * planes + (distance > 1), 4 * distance - 1)
        events.setdefault(min(step, final - 1), []).append(far_unit(distance, near))
    events.setdefault(final - 1, []).extend(
        [far_unit(planes - 1, near, early), last_tokens, across_unit]
    )
    for at_step in range(final + 1):
        rows_in.pass_far(at_step // 4 + 1, at_step % 4)
        for event in events.get(at_step, []):
            event()
    far_unit(planes - 1, everywhere, late)()

    low_part = lax.broadcasted_iota(jnp.int32, (part, pair), 1) < head
    query_pair = jnp.concatenate([query_gain[...]] * 2, axis=1)
    key_pair = jnp.concatenate([key_gain[...]] * 2, axis=1)

    def settle(total, place, h):
        span = aligned(place * 2 + h, part)
        for k in range(width // pair):
            v = total[:, pair * k : pair * (k + 1)]
            square = v * v
            lo = jnp.sum(jnp.where(low_part, square, 0.0), axis=-1, keepdims=True) / head
            hi = jnp.sum(jnp.where(low_part, 0.0, square), axis=-1, keepdims=True) / head
            scale = jnp.where(low_part, lax.rsqrt(lo + epsilon), lax.rsqrt(hi + epsilon))
            q[span, pair * k : pair * (k + 1)] = (v * scale * query_pair).astype(jnp.bfloat16)
        v = total[:, width : width + pair]
        lo = jnp.sum(jnp.where(low_part, v * v, 0.0), axis=-1, keepdims=True) / head
        both = jnp.where(low_part, v * lax.rsqrt(lo + epsilon) * key_pair, v)
        kv[span, :pair] = both.astype(jnp.bfloat16)
        kv[span, pair:] = pltpu.roll(both, head, 1).astype(jnp.bfloat16)
        pool[span, :] = total[:, width + pair :].astype(jnp.bfloat16)

    def settle_half(h):
        def one(k, carry):
            settle(acc[k, aligned(h, part), :], place_of(k), h)
            return carry

        lax.fori_loop(0, 4, one, 0)

    settle_half(1)

    def halo(k):
        src, dst = (kv, kv_halo) if k == 0 else (pool, pool_halo)
        rows = dst.shape[0]
        return remote(
            src.at[pl.ds(4 * count - rows, rows), :], dst, h_send.at[k], h_recv.at[k], at.above()
        )

    @pl.when(at.has_above)
    def _():
        halo(0).start()
        halo(1).start()

    @pl.when(z == 0)
    def _():
        kv_halo[...] = jnp.zeros_like(kv_halo)
        pool_halo[...] = jnp.zeros_like(pool_halo)

    query = lax.broadcasted_iota(jnp.int32, (block, block), 0)
    key = lax.broadcasted_iota(jnp.int32, (block, block), 1)
    current = key <= query
    low_keys = lax.broadcasted_iota(jnp.int32, (2 * block, pair), 1) < head
    log2_e = 1.4426950408889634
    line = lax.broadcasted_iota(jnp.int32, (block, channels), 0)
    window = lax.shift_left(jnp.int32(2), p).astype(jnp.float32)
    heads = width // head
    slot = c * 4 + p

    def mixers(j, place):
        index = place * steps + j
        base = pl.multiple_of(index * block, block)
        first = index == 0
        before = pl.multiple_of(jnp.maximum(base - block, 0), block)
        lag_before = pl.multiple_of(jnp.maximum(base - lag_rows, 0), lag_rows)

        @pl.when(first)
        def _():
            kv_before[...] = kv_halo[...]
            pool_before[...] = pool_halo[...]

        @pl.when(jnp.logical_not(first))
        def _():
            kv_before[...] = kv[pl.ds(before, block), :]
            pool_before[...] = pool[pl.ds(lag_before, lag_rows), :]

        kvs = jnp.concatenate([kv_before[...], kv[pl.ds(base, block), :]], axis=0)
        straight, turned = kvs[:, :pair], kvs[:, pair:]
        zero = jnp.zeros_like(straight)
        keys = (jnp.where(low_keys, straight, zero), jnp.where(low_keys, zero, turned))
        values = (jnp.where(low_keys, turned, zero), jnp.where(low_keys, zero, straight))
        absent = jnp.where((z == 0) & first, NEGATIVE, 0.0)
        span = aligned(place, block)
        for k in range(heads // 2):
            q_pair = q[pl.ds(base, block), pair * k : pair * (k + 1)]
            total = None
            for side in range(2):
                sink = sinks[p * heads + 2 * k + side] * log2_e
                scores = lax.dot_general(
                    q_pair,
                    keys[side],
                    (((1,), (1,)), ((), ())),
                    preferred_element_type=jnp.float32,
                )
                scores = jnp.where(current, scores[:, block:], scores[:, :block] + absent)
                scores = scores * (head ** (-0.5) * log2_e)
                top = jnp.maximum(jnp.max(scores, axis=-1, keepdims=True), sink)
                lifted = jnp.exp2(scores - top)
                under = jnp.sum(lifted, axis=-1, keepdims=True) + jnp.exp2(sink - top)
                weights = lifted * (1.0 / under)
                weights = jnp.concatenate(
                    [jnp.where(current, 0.0, weights), jnp.where(current, weights, 0.0)], axis=1
                ).astype(jnp.bfloat16)
                term = jnp.dot(weights, values[side], preferred_element_type=jnp.float32)
                total = term if total is None else total + term
            ma[slot, j, span, 2 * pair * k : 2 * pair * k + pair] = total.astype(jnp.bfloat16)
        series = jnp.concatenate([pool_before[...], pool[pl.ds(base, block), :]], axis=0)
        series = series.astype(jnp.float32)
        sums, lag = [series], 1
        while 2 * lag <= lag_rows:
            sums.append(sums[-1] + pltpu.roll(sums[-1], lag, 0))
            lag *= 2
        window_sum = sums[-1]
        for k in range(len(sums) - 2, 0, -1):
            window_sum = jnp.where(p == k - 1, sums[k], window_sum)
        position = (z * 4 * count + base + 1 + line).astype(jnp.float32)
        contrast = window_sum[lag_rows:] / jnp.minimum(position, window) - series[lag_rows:]
        mixed = jnp.dot(contrast.astype(jnp.bfloat16), mix[p], preferred_element_type=jnp.float32)
        mixed = (mixed * pool_scale[:, aligned(p, channels)]).astype(jnp.bfloat16)
        for k in range(channels // pair):
            ma[slot, j, span, (2 * k + 1) * pair : (2 * k + 2) * pair] = mixed[
                :, pair * k : pair * (k + 1)
            ]

    def to_mate(index, j, to):
        ref = ma.at[slot, j]
        return remote(ref, ref, m_send.at[index, j], m_recv.at[p, j], at.mate(to))

    def onward(k, j, place, to):
        ref = ma.at[c * 4 + place, j, pl.ds(k * (tall // 2), tall // 2), :]
        return remote(ref, ref, f_send.at[k, j], f_recv.at[k, j], at.mate(to))

    def over(index, j, place, core):
        ref = ma.at[core * 4 + place, j]
        return remote(ref, ref, d_send.at[index, j], d_recv.at[place, j], at.partner())

    def came(place, j):
        ref = ma.at[c * 4 + place, j]
        remote(ref, ref, m_send.at[0, j], m_recv.at[place, j], at.partner()).wait_recv()

    def mix_step(index, carry):
        j = steps - 1 - index

        @pl.when(index == 1)
        def _():
            settle_half(0)

        @pl.when((j == 0) & at.has_below)
        def _():
            halo(0).wait_recv()
            halo(1).wait_recv()

        def one(place, inner):
            mixers(j, place)
            return inner

        lax.fori_loop(0, 4, one, 0)
        to_mate(0, j, at.xn).start()
        to_mate(1, j, at.yn).start()
        over(0, j, p, c).start()

        @pl.when(index == 0)
        def _():
            rows_out.pass_near()

        return carry

    lax.fori_loop(0, steps, mix_step, 0)

    def pass_on(j):
        came(at.xn, j)
        onward(0, j, at.xn, at.yn).start()
        over(1, j, at.xn, c).start()
        came(at.yn, j)
        onward(1, j, at.yn, at.xn).start()
        over(2, j, at.yn, c).start()

    waiting = list(range(steps - 1, -1, -1))
    total_far = 4 * (planes - 1)
    for at_step in range(total_far):
        rows_out.pass_far(at_step // 4 + 1, at_step % 4)
        passed = steps - len(waiting)
        while waiting and at_step + 1 >= (passed + 1) * total_far // (steps + 1):
            pass_on(waiting.pop(0))
            passed += 1
    for j in waiting:
        pass_on(j)
    for copy in rows_out.here():
        copy.wait()

    def landing(j, place):
        return out.at[aligned(j, block), aligned(place, columns)]

    def result(index, j, to):
        return remote(
            ys.at[j, aligned(to, block), :],
            landing(j, p),
            r_send.at[index, j],
            r_recv.at[p, j],
            at.mate(to),
        )

    def result_here(j):
        return pltpu.make_async_copy(ys.at[j, aligned(p, block), :], landing(j, p), r_local.at[j])

    def last_step(index, carry):
        j = steps - 1 - index
        for k in range(2):
            onward(k, j, at.dg, at.xn).wait_recv()
        over(3, j, at.dg, c).start()
        for place in range(4):
            over(0, j, place, 1 - c).wait_recv()
        total = None
        for i in range(8):
            first = 2 * i
            weight = ws_out[first // 4, first % 4 : first % 4 + 2].reshape(wide, columns)
            term = jnp.dot(ma[i, j], weight, preferred_element_type=jnp.float32)
            total = term if total is None else total + term
        ys[j] = total.astype(jnp.bfloat16)
        for k, to in enumerate(at.mates):
            result(k, j, to).start()
        result_here(j).start()
        return carry

    lax.fori_loop(0, steps, last_step, 0)

    def finish_step(j, carry):
        for k, to in enumerate(at.mates):
            remote(
                ys.at[j, pl.ds(0, block), :],
                landing(j, to),
                r_send.at[k, j],
                r_recv.at[to, j],
                at.mate(to),
            ).wait_recv()
        result_here(j).wait()
        for k, to in enumerate(at.mates):
            result(k, j, to).wait_send()
        to_mate(0, j, at.xn).wait_send()
        to_mate(1, j, at.yn).wait_send()
        onward(0, j, at.xn, at.yn).wait_send()
        onward(1, j, at.yn, at.xn).wait_send()
        for k, place in enumerate((p,) + at.mates):
            over(k, j, place, c).wait_send()
        return carry

    lax.fori_loop(0, steps, finish_step, 0)
    raw_away.wait_send()
    for index in range(6):
        tokens_to(index, *sent[index]).wait_send()
        tokens_over(index, *crossed[index], c).wait_send()

    @pl.when(at.has_above)
    def _():
        halo(0).wait_send()
        halo(1).wait_send()

    rows_in.finish()
    rows_out.finish()


def per_device_planes(
    tokens,
    norm_gain,
    w_query,
    w_key,
    w_value,
    w_pool_in,
    query_gain,
    key_gain,
    sinks,
    w_mix,
    pool_scale,
    w_out_attn,
    w_out_pool,
):
    planes = lax.axis_size("sp") // 4
    head = query_gain.shape[0]
    count, half = tokens.shape
    in_rows, out_rows = w_query.shape[0], 2 * w_out_attn.shape[0]
    width, channels = w_query.shape[1] // 4, w_pool_in.shape[1] // 4
    columns = w_out_attn.shape[1] // 4
    pair, deep, steps = 2 * head, 4 * in_rows, count // WINDOW
    in_width = width + pair + channels
    vmem = pl.BlockSpec(memory_space=pltpu.VMEM)
    anywhere = pl.BlockSpec(memory_space=pl.ANY)
    smem = pl.BlockSpec(memory_space=pltpu.SMEM)
    dma = pltpu.SemaphoreType.DMA

    def held(*shape):
        return pltpu.VMEM(shape, jnp.bfloat16)

    row_sems = [dma((3,)), dma((3,)), dma((planes, 4)), dma((planes, 4)), dma((planes, 4))]
    return pl.pallas_call(
        functools.partial(layer_kernel, planes, head),
        out_shape=jax.ShapeDtypeStruct(tokens.shape, jnp.bfloat16),
        in_specs=[anywhere, vmem, anywhere, vmem, vmem, anywhere, vmem, vmem]
        + [smem, vmem, vmem, anywhere, anywhere],
        out_specs=anywhere,
        scratch_shapes=[
            held(2, count, half),
            held(4, planes, count, deep),
            held(planes, 4, in_rows, in_width),
            held(4, in_rows, pair),
            pltpu.VMEM((4, count, in_width), jnp.float32),
            held(4 * count, width),
            held(4 * count, 2 * pair),
            held(4 * count, channels),
            held(WINDOW, 2 * pair),
            held(longest_lag + 1, channels),
            held(8, steps, 4 * WINDOW, width + channels),
            held(planes, 4, out_rows, columns),
            held(steps, 4 * WINDOW, columns),
        ]
        + row_sems
        + row_sems
        + [dma((3,)), dma((6,)), dma((4, 2)), dma((6,)), dma((4, 2)), dma((2,)), dma((2,))]
        + [dma((2, steps)), dma((4, steps)), dma((2, steps)), dma((2, steps))]
        + [dma((4, steps)), dma((4, steps)), dma((3, steps)), dma((4, steps)), dma((steps,))]
        + [held(WINDOW, 2 * pair), held(longest_lag + 1, channels)],
        compiler_params=pltpu.CompilerParams(
            collective_id=0, has_side_effects=True, vmem_limit_bytes=63 * 2**20
        ),
        name="layer",
    )(
        tokens,
        norm_gain.reshape(1, -1),
        w_query,
        w_key,
        w_value,
        w_pool_in,
        query_gain.reshape(1, -1),
        key_gain.reshape(1, -1),
        sinks,
        w_mix,
        pool_scale.reshape(1, -1),
        w_out_attn,
        w_out_pool,
    )


def suits_planes(mesh, args):
    sp, tp = mesh.shape["sp"], mesh.shape["tp"]
    tokens, w_query, w_key, w_pool_in = args[0], args[2], args[3], args[5]
    head, groups = args[6].shape[0], args[9].shape[0]
    w_out_attn, w_out_pool = args[11], args[12]
    if tp != 2 or sp % 4 or sp < 12 or 2 * head != 128:
        return False
    share = 4 * tp
    rows = tokens.shape[0] // sp
    width, channels = w_query.shape[1] // share, w_pool_in.shape[1] // share
    held = 2 * 4 * rows * tokens.shape[1] + 2 * w_query.shape[0] * (width + 128 + channels)
    return (
        w_key.shape[1] == share * head
        and groups == share
        and rows % (4 * WINDOW) == 0
        and width % 128 == 0
        and width == channels
        and 2 * w_out_attn.shape[0] // sp == width
        and 2 * w_out_pool.shape[0] // sp == channels
        and w_out_attn.shape[0] // sp == 2 * head
        and w_query.shape[0] // sp % 16 == 0
        and w_out_attn.shape[1] % (share * 128) == 0
        and held < 22 * 2**20
    )


def solution(mesh):
    sp, tp = mesh.shape["sp"], mesh.shape["tp"]

    def call(*args):
        if suits_planes(mesh, args):
            return jax.shard_map(
                per_device_planes,
                mesh=mesh,
                in_specs=(
                    P("sp", "tp"),
                    P(),
                    P("sp", "tp"),
                    P("sp", "tp"),
                    P("sp", "tp"),
                    P("sp", "tp"),
                    P(),
                    P(),
                    P("tp"),
                    P("tp", None, None),
                    P("tp"),
                    P("sp", "tp"),
                    P("sp", "tp"),
                ),
                out_specs=P("sp", "tp"),
                check_vma=False,
            )(*args)
        kv_local = args[3].shape[1] // args[6].shape[0] // tp
        groups_local = args[9].shape[0] // tp
        fits = sp % 2 == 0 and kv_local % 2 == 0 and groups_local % 2 == 0
        pair = 2 if fits else 1
        inner = Mesh(mesh.devices.reshape(sp // pair, pair, tp), ("so", "si", "tp"))
        rows = ("so", "si")
        return jax.shard_map(
            per_device,
            mesh=inner,
            in_specs=(
                P(rows, "tp"),
                P(),
                P(rows, "tp"),
                P(rows, "tp"),
                P(rows, "tp"),
                P(rows, "tp"),
                P(),
                P(),
                P("tp"),
                P("tp", None, None),
                P("tp"),
                P(rows, "tp"),
                P(rows, "tp"),
            ),
            out_specs=P(rows, "tp"),
            check_vma=False,
        )(*args)

    return call
```

```python
import functools

import jax
import jax.numpy as jnp
from jax import lax
from jax.experimental import pallas as pl
from jax.experimental.pallas import tpu as pltpu
from jax.sharding import Mesh
from jax.sharding import PartitionSpec as P

WINDOW = 128


epsilon = 1e-06
longest_lag = 15


def from_behind(block, axis):
    devices = range(lax.axis_size(axis))
    route = [(i - 1, i) for i in devices if i - 1 in devices]
    return lax.ppermute(block, axis, route)


def swap(block, axis):
    count = lax.axis_size(axis)
    return lax.ppermute(block, axis, [(i, count - 1 - i) for i in range(count)])


def row_norm(values, gain):
    return values * lax.rsqrt(jnp.mean(values * values, axis=-1, keepdims=True) + epsilon) * gain


def after(value, *others):
    return lax.optimization_barrier((value,) + others)[0]


def ordered(mine, theirs, index, dim):
    return jnp.where(
        index == 0,
        jnp.concatenate([mine, theirs], axis=dim),
        jnp.concatenate([theirs, mine], axis=dim),
    )


def both_cores(block, dim):
    if lax.axis_size("tp") == 2:
        return ordered(block, swap(block, "tp"), lax.axis_index("tp"), dim)
    return lax.all_gather(block, "tp", axis=dim, tiled=True)


def per_device(
    tokens,
    norm_gain,
    w_query,
    w_key,
    w_value,
    w_pool_in,
    query_gain,
    key_gain,
    sinks,
    w_mix,
    pool_scale,
    w_out_attn,
    w_out_pool,
):
    pair = lax.axis_size("si")
    place = lax.axis_index("si")
    outer = lax.axis_index("so")

    def share(array, owner, dim):
        size = array.shape[dim] // pair
        return lax.dynamic_slice_in_dim(array, owner * size, size, dim)

    def mine(arrays):
        return [share(a, place, 1) for a in arrays]

    def other(arrays):
        return [share(a, pair - 1 - place, 1) for a in arrays]

    def joined(own, came, dim):
        return own if pair == 1 else ordered(own, came, place, dim)

    def gathered(rows):
        return lax.all_gather(rows, "so", axis=0, tiled=True)

    qkv_parts = (w_query, w_key, w_value)
    qkv_own = jnp.concatenate(mine(qkv_parts), axis=1)
    if pair == 1:
        qkv_rows, pool_rows, attn_rows, mixed_rows = qkv_own, w_pool_in, w_out_attn, w_out_pool
        row_half = tokens
    else:
        qkv_came = swap(jnp.concatenate(other(qkv_parts), axis=1), "si")
        qkv_rows = joined(qkv_own, qkv_came, 0)
        late = lax.optimization_barrier((w_pool_in, w_out_attn, w_out_pool, qkv_came))[:3]
        came = [swap(share(w, pair - 1 - place, 1), "si") for w in late]
        pool_rows, attn_rows, mixed_rows = [
            joined(share(w, place, 1), c, 0) for w, c in zip((w_pool_in, w_out_attn, w_out_pool), came)
        ]
        row_half = joined(tokens, swap(after(tokens, qkv_came), "si"), 0)
    w_qkv = gathered(qkv_rows)
    w_pool = gathered(after(pool_rows, w_qkv))
    w_attn = gathered(after(attn_rows, w_pool))
    w_mixed = gathered(after(mixed_rows, w_attn))

    whole = both_cores(row_half, 1)
    row_count = whole.shape[0]
    normed = row_norm(whole.astype(jnp.float32), norm_gain).astype(jnp.bfloat16)
    qkv_raw = jnp.dot(normed, w_qkv, preferred_element_type=jnp.float32)
    head_size = query_gain.shape[0]
    query_width = w_query.shape[1] // pair
    kv_width = w_key.shape[1] // pair
    query_heads = query_width // head_size
    kv_local = kv_width // head_size
    per_kv = query_heads // kv_local
    query_raw = qkv_raw[:, :query_width]
    key_raw = qkv_raw[:, query_width : query_width + kv_width]
    value_raw = qkv_raw[:, query_width + kv_width :]
    queries = row_norm(query_raw.reshape(row_count, query_heads, head_size), query_gain).astype(
        jnp.bfloat16
    )
    key_rows = row_norm(key_raw.reshape(row_count, kv_local, head_size), key_gain).astype(
        jnp.bfloat16
    )
    values = value_raw.astype(jnp.bfloat16).reshape(row_count, kv_local, head_size)
    kv_tail = jnp.concatenate(
        [key_rows[-WINDOW:].reshape(WINDOW, -1), values[-WINDOW:].reshape(WINDOW, -1)], axis=1
    )
    kv_prev = from_behind(kv_tail, "so").reshape(WINDOW, 2, kv_local, head_size)
    offset = outer * row_count
    blocks = row_count // WINDOW

    def banded(previous, source):
        earlier = jnp.concatenate([previous, source[: row_count - WINDOW]], axis=0).reshape(
            blocks, WINDOW, kv_local, head_size
        )
        return jnp.concatenate(
            [earlier, source.reshape(blocks, WINDOW, kv_local, head_size)], axis=1
        )

    band_keys = banded(kv_prev[:, 0], key_rows)
    band_values = banded(kv_prev[:, 1], values)
    query_blocks = queries.reshape(blocks, WINDOW, kv_local, per_kv, head_size)
    scores = jnp.einsum(
        "bqkgd,bjkd->bkgqj", query_blocks, band_keys, preferred_element_type=jnp.float32
    ) * head_size ** (-0.5)
    query_index = jnp.arange(WINDOW)[:, None]
    key_index = jnp.arange(2 * WINDOW)[None, :]
    distance = query_index + WINDOW - key_index
    key_pos = offset + jnp.arange(blocks)[:, None, None] * WINDOW - WINDOW + key_index[None]
    valid = (distance[None] >= 0) & (distance[None] < WINDOW) & (key_pos >= 0)
    sink_logit = share(sinks, place, 0).reshape(kv_local, per_kv)[None, :, :, None, None]
    scores = jnp.where(valid[:, None, None], scores, -1e30)
    row_top = jnp.maximum(scores.max(axis=-1, keepdims=True), sink_logit)
    lifted = jnp.exp(scores - row_top)
    weights = (
        lifted / (lifted.sum(axis=-1, keepdims=True) + jnp.exp(sink_logit - row_top))
    ).astype(jnp.bfloat16)
    attended = (
        jnp.einsum("bkgqj,bjkd->bqkgd", weights, band_values, preferred_element_type=jnp.float32)
        .astype(jnp.bfloat16)
        .reshape(row_count, query_heads * head_size)
    )

    def all_heads(block):
        if pair == 2:
            block = joined(block, swap(block, "si"), 1)
        return both_cores(block, 1)

    attended_all = all_heads(attended)

    pool_in = jnp.dot(normed, w_pool, preferred_element_type=jnp.float32).astype(jnp.bfloat16)
    pool_prev = from_behind(pool_in[-longest_lag:], "so")
    mix = share(w_mix, place, 0)
    groups_local = mix.shape[0]
    group_dim = mix.shape[1]
    first_group = (lax.axis_index("tp") * pair + place) * groups_local
    group_ids = first_group + jnp.arange(groups_local, dtype=jnp.int32)
    spans = jnp.repeat(jnp.left_shift(jnp.int32(2), group_ids % 4), group_dim)
    extended = jnp.concatenate([pool_prev, pool_in], axis=0).astype(jnp.float32)
    window_sum = jnp.zeros((row_count, spans.shape[0]), jnp.float32)
    for back_step in range(longest_lag + 1):
        shifted = extended[longest_lag - back_step : longest_lag - back_step + row_count]
        window_sum = window_sum + jnp.where(back_step < spans[None, :], shifted, 0.0)
    positions = (offset + jnp.arange(1, row_count + 1, dtype=jnp.int32)).astype(jnp.float32)
    divisor = jnp.minimum(positions[:, None], spans.astype(jnp.float32)[None, :])
    contrast = (window_sum / divisor - extended[longest_lag:]).astype(jnp.bfloat16)
    mixed = jnp.einsum(
        "tgc,gcd->tgd",
        contrast.reshape(row_count, groups_local, group_dim),
        mix,
        preferred_element_type=jnp.float32,
    ).reshape(row_count, -1)
    pooled = (mixed * share(pool_scale, place, 0)).astype(jnp.bfloat16)
    pooled_all = all_heads(pooled)

    def project(owner):
        total = jnp.dot(share(attended_all, owner, 0), w_attn, preferred_element_type=jnp.float32)
        result = total + jnp.dot(
            share(pooled_all, owner, 0), w_mixed, preferred_element_type=jnp.float32
        )
        return result.astype(jnp.bfloat16)

    if pair == 1:
        return project(0)
    away = project(pair - 1 - place)
    came_back = swap(away, "si")
    return joined(project(place), came_back, 1)


MESH = pl.DeviceIdType.MESH
NEGATIVE = -1e30


def remote(src, dst, send_sem, recv_sem, device):
    return pltpu.make_async_remote_copy(
        src_ref=src,
        dst_ref=dst,
        send_sem=send_sem,
        recv_sem=recv_sem,
        device_id=device,
        device_id_type=MESH,
    )


def aligned(index, size):
    return pl.ds(pl.multiple_of(index * size, size), size)


class Place:
    def __init__(self, planes):
        self.sp, self.c = lax.axis_index("sp"), lax.axis_index("tp")
        self.planes = planes
        self.z, self.p = lax.div(self.sp, 4), lax.rem(self.sp, 4)
        x, y = lax.rem(self.p, 2), lax.div(self.p, 2)
        self.xn, self.yn, self.dg = self.p + 1 - 2 * x, self.p + 2 - 4 * y, 3 - self.p
        self.mates = (self.xn, self.yn, self.dg)
        self.has_above, self.has_below = self.z < planes - 1, self.z > 0

    def mate(self, p):
        return (self.z * 4 + p, self.c)

    def partner(self):
        return (self.sp, 1 - self.c)

    def above(self):
        return (lax.rem(self.sp + 4, 4 * self.planes), self.c)

    def below(self):
        return (lax.rem(self.sp + 4 * self.planes - 4, 4 * self.planes), self.c)

    def barrier(self):
        sem = pltpu.get_barrier_semaphore()
        for p in self.mates:
            pl.semaphore_signal(sem, inc=1, device_id=self.mate(p), device_id_type=MESH)
        pl.semaphore_signal(sem, inc=1, device_id=self.partner(), device_id_type=MESH)

        @pl.when(self.has_above)
        def _():
            pl.semaphore_signal(sem, inc=1, device_id=self.above(), device_id_type=MESH)

        @pl.when(self.has_below)
        def _():
            pl.semaphore_signal(sem, inc=1, device_id=self.below(), device_id_type=MESH)

        inner = self.has_above & self.has_below

        @pl.when(inner)
        def _():
            pl.semaphore_wait(sem, 6)

        @pl.when(jnp.logical_not(inner))
        def _():
            pl.semaphore_wait(sem, 5)


class Rows:
    def __init__(self, at, own, held, sems):
        self.at, self.own, self.held = at, own, held
        self.local_sem, self.near, self.recv, self.up, self.down = sems

    def slot(self, plane, p, cut=None):
        if cut is None:
            return self.held.at[plane, p]
        return self.held.at[plane, p, cut[0], cut[1]]

    def to_mate(self, index, p):
        at = self.at
        return [
            remote(
                src,
                self.slot(at.z, at.p, cut),
                self.near.at[index],
                self.recv.at[at.z, at.p],
                at.mate(p),
            )
            for src, cut, _ in self.own(p)
        ]

    def here(self):
        at = self.at
        return [
            pltpu.make_async_copy(src, self.slot(at.z, at.p, cut), self.local_sem.at[k])
            for k, (src, cut, copied) in enumerate(self.own(at.p))
            if copied
        ]

    def hop(self, plane, p, upward, src=None, cut=None):
        at = self.at
        dst = self.slot(plane, p, cut)
        return remote(
            dst if src is None else src,
            dst,
            (self.up if upward else self.down).at[plane, p],
            self.recv.at[plane, p],
            at.above() if upward else at.below(),
        )

    def send(self, plane, p, upward):
        @pl.when(self.at.has_above if upward else self.at.has_below)
        def _():
            self.hop(plane, p, upward).start()

    def begin_far(self):
        at = self.at
        for upward in (True, False):

            @pl.when(at.has_above if upward else at.has_below)
            def _():
                for src, cut, _ in self.own(at.p):
                    self.hop(at.z, at.p, upward, src, cut).start()

    def begin_near(self):
        for index, p in enumerate(self.at.mates):
            for copy in self.to_mate(index, p):
                copy.start()
        for copy in self.here():
            copy.start()

    def arrived(self, plane, p):
        self.hop(plane, p, True).wait_recv()

    def pass_near(self):
        at = self.at
        for p in at.mates:
            self.arrived(at.z, p)
            self.send(at.z, p, True)
            self.send(at.z, p, False)

    def pass_far(self, distance, index):
        at = self.at
        p = ((at.p,) + at.mates)[index]
        low, high = at.z - distance, at.z + distance

        @pl.when(low >= 0)
        def _():
            self.arrived(low, p)
            self.send(low, p, True)

        @pl.when(high < at.planes)
        def _():
            self.arrived(high, p)
            self.send(high, p, False)

    def finish(self):
        at = self.at
        whole = self.slot(at.z, at.p)
        for index, p in enumerate(at.mates):
            remote(
                whole, whole, self.near.at[index], self.recv.at[at.z, at.p], at.mate(p)
            ).wait_send()
        for plane in range(at.planes):
            for p in range(4):

                @pl.when(at.has_above & (at.z >= plane))
                def _():
                    self.hop(plane, p, True).wait_send()

                @pl.when(at.has_below & (at.z <= plane))
                def _():
                    self.hop(plane, p, False).wait_send()


def layer_kernel(planes, head, *refs):
    (tok, gain, w_query, w_key, w_value, w_pool, query_gain, key_gain) = refs[:8]
    (sinks, mix, pool_scale, w_attn, w_mixed, out) = refs[8:14]
    (raw, xs, ws, kvw, acc, q, kv, pool, kv_halo, pool_halo, ma, ws_out, ys) = refs[14:27]
    kv_before, pool_before = refs[-2:]
    in_sems, out_sems = refs[27:32], refs[32:37]
    (raw_sems, t_send, t_recv, td_send, td_recv, h_send, h_recv) = refs[37:44]
    (m_send, m_recv, f_send, f_recv, d_send, d_recv, r_send, r_recv, r_local) = refs[44:-2]

    at = Place(planes)
    c, p, z = at.c, at.p, at.z
    pair = 2 * head
    count, half = tok.shape
    part = count // 2
    deep = xs.shape[3]
    blocks = half // deep
    width, channels = q.shape[1], pool.shape[1]
    steps, tall, wide = ma.shape[1:]
    block = tall // 4
    columns = ws_out.shape[3]
    lag_rows = pool_halo.shape[0]

    low_lane = lax.broadcasted_iota(jnp.int32, (w_key.shape[0], pair), 1) < head
    for k in range(4):
        tile = slice(k // 2 * pair, (k // 2 + 1) * pair)
        key_tile, value_tile = w_key[:, tile], w_value[:, tile]
        if k % 2:
            key_tile = pltpu.roll(key_tile.astype(jnp.float32), head, 1).astype(jnp.bfloat16)
        else:
            value_tile = pltpu.roll(value_tile.astype(jnp.float32), head, 1).astype(jnp.bfloat16)
        kvw[k] = jnp.where(low_lane, key_tile, value_tile)
    ws[z, p, :, width : width + pair] = kvw[p]

    every = pl.ds(0, w_query.shape[0])

    def own_in(place):
        return [
            (w_query.at[:, aligned(place, width)], (every, pl.ds(0, width)), True),
            (kvw.at[place], (every, pl.ds(width, pair)), False),
            (w_pool.at[:, aligned(place, channels)], (every, pl.ds(width + pair, channels)), True),
        ]

    def own_out(place):
        rows = w_attn.shape[0]
        return [
            (w_attn.at[:, aligned(place, columns)], (pl.ds(0, rows), pl.ds(0, columns)), True),
            (w_mixed.at[:, aligned(place, columns)], (pl.ds(rows, rows), pl.ds(0, columns)), True),
        ]

    rows_in = Rows(at, own_in, ws, in_sems)
    rows_out = Rows(at, own_out, ws_out, out_sems)

    at.barrier()
    raw_local = pltpu.make_async_copy(tok, raw.at[c], raw_sems.at[0])
    raw_away = remote(tok, raw.at[c], raw_sems.at[1], raw_sems.at[2], at.partner())
    raw_away.start()
    raw_local.start()
    rows_in.begin_far()
    rows_in.begin_near()
    raw_local.wait()
    raw_away.wait_recv()

    norm_rows = 32

    def norm_step(index, carry):
        span = aligned(index, norm_rows)
        halves = [raw[k, span, :].astype(jnp.float32) for k in range(2)]
        total = sum(jnp.sum(v * v, axis=-1, keepdims=True) for v in halves)
        scale = lax.rsqrt(total / (2 * half) + epsilon)
        for k in range(2):
            normed = halves[k] * scale * gain[:, k * half : (k + 1) * half]
            normed = normed.astype(jnp.bfloat16)
            for b in range(blocks):
                xs[p, k * blocks + b, span, :] = normed[:, b * deep : (b + 1) * deep]
        return carry

    lax.fori_loop(0, count // norm_rows, norm_step, 0)

    def piece(place, h, core):
        return xs.at[place, pl.ds(core * blocks, blocks), pl.ds(h * part, part), :]

    def tokens_to(index, place, h, to):
        ref = piece(place, h, c)
        return remote(ref, ref, t_send.at[index], t_recv.at[place, h], at.mate(to))

    def tokens_over(index, place, h, core):
        ref = piece(place, h, core)
        return remote(ref, ref, td_send.at[index], td_recv.at[place, h], at.partner())

    sent = [(p, 0, at.xn), (p, 1, at.yn), (p, 1, at.xn), (p, 0, at.yn)]
    sent += [(at.xn, 0, at.yn), (at.yn, 1, at.xn)]
    crossed = [(at.xn, 0), (at.yn, 1), (at.xn, 1), (at.yn, 0), (at.dg, 0), (at.dg, 1)]
    for index in range(4):
        tokens_to(index, *sent[index]).start()
    rows_in.pass_near()

    def take_tokens(index, onward=None):
        place, h = crossed[index]
        tokens_to(0, place, h, at.xn).wait_recv()
        if onward is not None:
            tokens_to(onward, *sent[onward]).start()
        tokens_over(index, place, h, c).start()

    def first_tokens():
        take_tokens(0, 4)
        take_tokens(1, 5)

    def second_tokens():
        take_tokens(2)
        take_tokens(3)
        rows_out.begin_far()
        rows_out.begin_near()
        for place, h in crossed[:4]:
            tokens_over(0, place, h, 1 - c).wait_recv()

    def product(place, b, span, slots):
        if slots is None:
            return jnp.dot(
                xs[place, b, span, :],
                ws[b].reshape(deep, ws.shape[3]),
                preferred_element_type=jnp.float32,
            )
        total = None
        for source in slots:
            term = jnp.dot(
                xs[place, b, span, aligned(source, deep // 4)],
                ws[b, source],
                preferred_element_type=jnp.float32,
            )
            total = term if total is None else total + term
        return total

    def place_of(k):
        return jnp.where(k == 0, p, jnp.where(k == 1, at.xn, jnp.where(k == 2, at.yn, at.dg)))

    def accumulate(b, places, slots=None, fresh=False, halves=(0, 2)):
        tall_count = halves[1] - halves[0]

        def one(index, carry):
            k = places[0] + lax.div(index, tall_count)
            span = aligned(halves[0] + lax.rem(index, tall_count), part)
            term = product(place_of(k), b, span, slots)
            acc[k, span, :] = term if fresh else acc[k, span, :] + term
            return carry

        lax.fori_loop(0, tall_count * (places[1] - places[0]), one, 0)

    mine, sides, near, everywhere = (0, 1), (1, 3), (0, 3), (0, 4)
    early, late = (p, at.xn, at.yn), (at.dg,)

    def far_unit(distance, places, slots=None, halves=(0, 2)):
        for b in (z - distance, z + distance):

            @pl.when((b >= 0) & (b < planes))
            def _():
                accumulate(b, places, slots, False, halves)

    def across(h):
        span = aligned(h, part)

        def whole(first, last, partial):
            total = None if partial is None else product(at.dg, partial, span, early)
            for b in range(first, last):
                term = product(at.dg, b, span, None)
                total = term if total is None else total + term
            acc[3, span, :] = total

        @pl.when(at.has_above & at.has_below)
        def _():
            whole(0, planes, None)

        @pl.when(jnp.logical_not(at.has_below))
        def _():
            whole(0, planes - 1, planes - 1)

        @pl.when(jnp.logical_not(at.has_above))
        def _():
            whole(1, planes, 0)

    def last_tokens():
        take_tokens(4)
        take_tokens(5)
        for h in range(2):
            tokens_over(0, at.dg, h, 1 - c).wait_recv()

    def start_mine():
        for copy in rows_in.here():
            copy.wait()
        accumulate(z, mine, fresh=True)

    def one_half(h, wait):
        far_unit(planes - 1, near, early, (h, h + 1))
        if wait:
            last_tokens()
        across(h)
        if wait:
            rows_in.pass_far(planes - 1, 3)
        far_unit(planes - 1, everywhere, late, (h, h + 1))
        settle_half(h)

    final = 4 * (planes - 1) - 1
    events = {}

    def plan(step, event):
        events.setdefault(min(step, final - 1), []).append(event)

    plan(4 * planes // 3 - 1, start_mine)
    plan(4 * planes // 3, first_tokens)
    for distance in range(1, planes - 1):
        plan(max(4 * planes // 3, 4 * distance - 1), functools.partial(far_unit, distance, mine))
    plan(2 * planes - 1, second_tokens)
    plan(2 * planes - 1, lambda: accumulate(z, sides, fresh=True))
    for distance in range(1, planes - 1):
        turn = max(2 * planes - 2 + distance, 4 * distance - 1)
        plan(turn, functools.partial(far_unit, distance, sides))
    for at_step in range(final):
        rows_in.pass_far(at_step // 4 + 1, at_step % 4)
        for event in events.get(at_step, []):
            event()

    low_part = lax.broadcasted_iota(jnp.int32, (part, pair), 1) < head
    query_pair = jnp.concatenate([query_gain[...]] * 2, axis=1)
    key_pair = jnp.concatenate([key_gain[...]] * 2, axis=1)

    def settle(total, place, h):
        span = aligned(place * 2 + h, part)
        for k in range(width // pair):
            v = total[:, pair * k : pair * (k + 1)]
            square = v * v
            lo = jnp.sum(jnp.where(low_part, square, 0.0), axis=-1, keepdims=True) / head
            hi = jnp.sum(jnp.where(low_part, 0.0, square), axis=-1, keepdims=True) / head
            scale = jnp.where(low_part, lax.rsqrt(lo + epsilon), lax.rsqrt(hi + epsilon))
            q[span, pair * k : pair * (k + 1)] = (v * scale * query_pair).astype(jnp.bfloat16)
        v = total[:, width : width + pair]
        lo = jnp.sum(jnp.where(low_part, v * v, 0.0), axis=-1, keepdims=True) / head
        both = jnp.where(low_part, v * lax.rsqrt(lo + epsilon) * key_pair, v)
        kv[span, :pair] = both.astype(jnp.bfloat16)
        kv[span, pair:] = pltpu.roll(both, head, 1).astype(jnp.bfloat16)
        pool[span, :] = total[:, width + pair :].astype(jnp.bfloat16)

    def settle_half(h):
        def one(k, carry):
            settle(acc[k, aligned(h, part), :], place_of(k), h)
            return carry

        lax.fori_loop(0, 4, one, 0)

    one_half(1, True)

    def halo(k):
        src, dst = (kv, kv_halo) if k == 0 else (pool, pool_halo)
        rows = dst.shape[0]
        return remote(
            src.at[pl.ds(4 * count - rows, rows), :], dst, h_send.at[k], h_recv.at[k], at.above()
        )

    @pl.when(at.has_above)
    def _():
        halo(0).start()
        halo(1).start()

    @pl.when(z == 0)
    def _():
        kv_halo[...] = jnp.zeros_like(kv_halo)
        pool_halo[...] = jnp.zeros_like(pool_halo)

    heads = width // head
    pairs = heads // 2
    query = lax.rem(lax.broadcasted_iota(jnp.int32, (pairs * block, block), 0), block)
    key = lax.broadcasted_iota(jnp.int32, (pairs * block, block), 1)
    current = key <= query
    low_keys = lax.broadcasted_iota(jnp.int32, (2 * block, pair), 1) < head
    log2_e = 1.4426950408889634
    line = lax.broadcasted_iota(jnp.int32, (block, 1), 0)
    window = lax.shift_left(jnp.int32(2), p).astype(jnp.float32)
    slot = c * 4 + p

    def stage(j, place, side_by):
        index = place * steps + j
        before = pl.multiple_of(jnp.maximum(index - 1, 0) * block, block)
        lag_before = pl.multiple_of(jnp.maximum(index * block - lag_rows, 0), lag_rows)

        @pl.when(index == 0)
        def _():
            kv_before[side_by] = kv_halo[...]
            pool_before[side_by] = pool_halo[...]

        @pl.when(index > 0)
        def _():
            kv_before[side_by] = kv[pl.ds(before, block), :]
            pool_before[side_by] = pool[pl.ds(lag_before, lag_rows), :]

    def mixers(j, place, side_by):
        index = place * steps + j
        base = pl.multiple_of(index * block, block)
        first = index == 0
        kvs = jnp.concatenate([kv_before[side_by], kv[pl.ds(base, block), :]], axis=0)
        straight, turned = kvs[:, :pair], kvs[:, pair:]
        zero = jnp.zeros_like(straight)
        keys = (jnp.where(low_keys, straight, zero), jnp.where(low_keys, zero, turned))
        values = (jnp.where(low_keys, turned, zero), jnp.where(low_keys, zero, straight))
        absent = jnp.where((z == 0) & first, NEGATIVE, 0.0)
        span = aligned(place, block)
        q_pairs = [q[pl.ds(base, block), pair * k : pair * (k + 1)] for k in range(pairs)]
        q_stack = jnp.concatenate(q_pairs, axis=0)
        total = None
        for side in range(2):
            sink = jnp.concatenate(
                [
                    jnp.full((block, 1), sinks[p * heads + 2 * k + side] * log2_e, jnp.float32)
                    for k in range(pairs)
                ],
                axis=0,
            )
            scores = lax.dot_general(
                q_stack,
                keys[side],
                (((1,), (1,)), ((), ())),
                preferred_element_type=jnp.float32,
            )
            scores = jnp.where(current, scores[:, block:], scores[:, :block] + absent)
            scores = scores * (head ** (-0.5) * log2_e)
            top = jnp.maximum(jnp.max(scores, axis=-1, keepdims=True), sink)
            lifted = jnp.exp2(scores - top)
            under = jnp.sum(lifted, axis=-1, keepdims=True) + jnp.exp2(sink - top)
            weights = lifted * (1.0 / under)
            weights = jnp.concatenate(
                [jnp.where(current, 0.0, weights), jnp.where(current, weights, 0.0)], axis=1
            ).astype(jnp.bfloat16)
            term = jnp.dot(weights, values[side], preferred_element_type=jnp.float32)
            total = term if total is None else total + term
        for k in range(pairs):
            ma[slot, j, span, 2 * pair * k : 2 * pair * k + pair] = total[
                block * k : block * (k + 1)
            ].astype(jnp.bfloat16)
        series = jnp.concatenate([pool_before[side_by], pool[pl.ds(base, block), :]], axis=0)
        series = series.astype(jnp.float32)
        sums, lag = [series], 1
        while 2 * lag <= lag_rows:
            sums.append(sums[-1] + pltpu.roll(sums[-1], lag, 0))
            lag *= 2
        window_sum = sums[-1]
        for k in range(len(sums) - 2, 0, -1):
            window_sum = jnp.where(p == k - 1, sums[k], window_sum)
        position = (z * 4 * count + base + 1 + line).astype(jnp.float32)
        share = 1.0 / jnp.minimum(position, window)
        contrast = window_sum[lag_rows:] * share - series[lag_rows:]
        mixed = jnp.dot(contrast.astype(jnp.bfloat16), mix[p], preferred_element_type=jnp.float32)
        mixed = (mixed * pool_scale[:, aligned(p, channels)]).astype(jnp.bfloat16)
        for k in range(channels // pair):
            ma[slot, j, span, (2 * k + 1) * pair : (2 * k + 2) * pair] = mixed[
                :, pair * k : pair * (k + 1)
            ]

    def to_mate(index, j, to):
        ref = ma.at[slot, j]
        return remote(ref, ref, m_send.at[index, j], m_recv.at[p, j], at.mate(to))

    def onward(k, j, place, to):
        ref = ma.at[c * 4 + place, j, pl.ds(k * (tall // 2), tall // 2), :]
        return remote(ref, ref, f_send.at[k, j], f_recv.at[k, j], at.mate(to))

    def over(index, j, place, core):
        ref = ma.at[core * 4 + place, j]
        return remote(ref, ref, d_send.at[index, j], d_recv.at[place, j], at.partner())

    def came(place, j):
        ref = ma.at[c * 4 + place, j]
        remote(ref, ref, m_send.at[0, j], m_recv.at[place, j], at.partner()).wait_recv()

    def mix_step(index, carry):
        j = steps - 1 - index

        @pl.when(index == 1)
        def _():
            one_half(0, False)

        @pl.when((j == 0) & at.has_below)
        def _():
            halo(0).wait_recv()
            halo(1).wait_recv()

        def two(turn, inner):
            for side_by in range(2):
                stage(j, 2 * turn + side_by, side_by)
            for side_by in range(2):
                mixers(j, 2 * turn + side_by, side_by)
            return inner

        lax.fori_loop(0, 2, two, 0)
        to_mate(0, j, at.xn).start()
        to_mate(1, j, at.yn).start()
        over(0, j, p, c).start()

        @pl.when(index == 0)
        def _():
            rows_out.pass_near()

        return carry

    lax.fori_loop(0, steps, mix_step, 0)

    def pass_on(j):
        came(at.xn, j)
        onward(0, j, at.xn, at.yn).start()
        over(1, j, at.xn, c).start()
        came(at.yn, j)
        onward(1, j, at.yn, at.xn).start()
        over(2, j, at.yn, c).start()

    waiting = list(range(steps - 1, -1, -1))
    total_far = 4 * (planes - 1)
    for at_step in range(total_far):
        rows_out.pass_far(at_step // 4 + 1, at_step % 4)
        passed = steps - len(waiting)
        while waiting and at_step + 1 >= (passed + 1) * total_far // (steps + 1):
            pass_on(waiting.pop(0))
            passed += 1
    for j in waiting:
        pass_on(j)
    for copy in rows_out.here():
        copy.wait()

    def landing(j, place):
        return out.at[aligned(j, block), aligned(place, columns)]

    def result(index, j, to):
        return remote(
            ys.at[j, aligned(to, block), :],
            landing(j, p),
            r_send.at[index, j],
            r_recv.at[p, j],
            at.mate(to),
        )

    def result_here(j):
        return pltpu.make_async_copy(ys.at[j, aligned(p, block), :], landing(j, p), r_local.at[j])

    def last_step(index, carry):
        j = steps - 1 - index
        for k in range(2):
            onward(k, j, at.dg, at.xn).wait_recv()
        over(3, j, at.dg, c).start()
        for place in range(4):
            over(0, j, place, 1 - c).wait_recv()
        total = None
        for i in range(8):
            first = 2 * i
            weight = ws_out[first // 4, first % 4 : first % 4 + 2].reshape(wide, columns)
            term = jnp.dot(ma[i, j], weight, preferred_element_type=jnp.float32)
            total = term if total is None else total + term
        ys[j] = total.astype(jnp.bfloat16)
        for k, to in enumerate(at.mates):
            result(k, j, to).start()
        result_here(j).start()
        return carry

    lax.fori_loop(0, steps, last_step, 0)

    def finish_step(j, carry):
        for k, to in enumerate(at.mates):
            remote(
                ys.at[j, pl.ds(0, block), :],
                landing(j, to),
                r_send.at[k, j],
                r_recv.at[to, j],
                at.mate(to),
            ).wait_recv()
        result_here(j).wait()
        for k, to in enumerate(at.mates):
            result(k, j, to).wait_send()
        to_mate(0, j, at.xn).wait_send()
        to_mate(1, j, at.yn).wait_send()
        onward(0, j, at.xn, at.yn).wait_send()
        onward(1, j, at.yn, at.xn).wait_send()
        for k, place in enumerate((p,) + at.mates):
            over(k, j, place, c).wait_send()
        return carry

    lax.fori_loop(0, steps, finish_step, 0)
    raw_away.wait_send()
    for index in range(6):
        tokens_to(index, *sent[index]).wait_send()
        tokens_over(index, *crossed[index], c).wait_send()

    @pl.when(at.has_above)
    def _():
        halo(0).wait_send()
        halo(1).wait_send()

    rows_in.finish()
    rows_out.finish()


def per_device_planes(
    tokens,
    norm_gain,
    w_query,
    w_key,
    w_value,
    w_pool_in,
    query_gain,
    key_gain,
    sinks,
    w_mix,
    pool_scale,
    w_out_attn,
    w_out_pool,
):
    planes = lax.axis_size("sp") // 4
    head = query_gain.shape[0]
    count, half = tokens.shape
    in_rows, out_rows = w_query.shape[0], 2 * w_out_attn.shape[0]
    width, channels = w_query.shape[1] // 4, w_pool_in.shape[1] // 4
    columns = w_out_attn.shape[1] // 4
    pair, deep, steps = 2 * head, 4 * in_rows, count // WINDOW
    in_width = width + pair + channels
    vmem = pl.BlockSpec(memory_space=pltpu.VMEM)
    anywhere = pl.BlockSpec(memory_space=pl.ANY)
    smem = pl.BlockSpec(memory_space=pltpu.SMEM)
    dma = pltpu.SemaphoreType.DMA

    def held(*shape):
        return pltpu.VMEM(shape, jnp.bfloat16)

    row_sems = [dma((3,)), dma((3,)), dma((planes, 4)), dma((planes, 4)), dma((planes, 4))]
    return pl.pallas_call(
        functools.partial(layer_kernel, planes, head),
        out_shape=jax.ShapeDtypeStruct(tokens.shape, jnp.bfloat16),
        in_specs=[anywhere, vmem, anywhere, vmem, vmem, anywhere, vmem, vmem]
        + [smem, vmem, vmem, anywhere, anywhere],
        out_specs=anywhere,
        scratch_shapes=[
            held(2, count, half),
            held(4, planes, count, deep),
            held(planes, 4, in_rows, in_width),
            held(4, in_rows, pair),
            pltpu.VMEM((4, count, in_width), jnp.float32),
            held(4 * count, width),
            held(4 * count, 2 * pair),
            held(4 * count, channels),
            held(WINDOW, 2 * pair),
            held(longest_lag + 1, channels),
            held(8, steps, 4 * WINDOW, width + channels),
            held(planes, 4, out_rows, columns),
            held(steps, 4 * WINDOW, columns),
        ]
        + row_sems
        + row_sems
        + [dma((3,)), dma((6,)), dma((4, 2)), dma((6,)), dma((4, 2)), dma((2,)), dma((2,))]
        + [dma((2, steps)), dma((4, steps)), dma((2, steps)), dma((2, steps))]
        + [dma((4, steps)), dma((4, steps)), dma((3, steps)), dma((4, steps)), dma((steps,))]
        + [held(2, WINDOW, 2 * pair), held(2, longest_lag + 1, channels)],
        compiler_params=pltpu.CompilerParams(
            collective_id=0, has_side_effects=True, vmem_limit_bytes=63 * 2**20
        ),
        name="layer",
    )(
        tokens,
        norm_gain.reshape(1, -1),
        w_query,
        w_key,
        w_value,
        w_pool_in,
        query_gain.reshape(1, -1),
        key_gain.reshape(1, -1),
        sinks,
        w_mix,
        pool_scale.reshape(1, -1),
        w_out_attn,
        w_out_pool,
    )


def suits_planes(mesh, args):
    sp, tp = mesh.shape["sp"], mesh.shape["tp"]
    tokens, w_query, w_key, w_pool_in = args[0], args[2], args[3], args[5]
    head, groups = args[6].shape[0], args[9].shape[0]
    w_out_attn, w_out_pool = args[11], args[12]
    if tp != 2 or sp % 4 or sp < 12 or 2 * head != 128:
        return False
    share = 4 * tp
    rows = tokens.shape[0] // sp
    width, channels = w_query.shape[1] // share, w_pool_in.shape[1] // share
    held = 2 * 4 * rows * tokens.shape[1] + 2 * w_query.shape[0] * (width + 128 + channels)
    return (
        w_key.shape[1] == share * head
        and groups == share
        and rows % (4 * WINDOW) == 0
        and width % 128 == 0
        and width == channels
        and 2 * w_out_attn.shape[0] // sp == width
        and 2 * w_out_pool.shape[0] // sp == channels
        and w_out_attn.shape[0] // sp == 2 * head
        and w_query.shape[0] // sp % 16 == 0
        and w_out_attn.shape[1] % (share * 128) == 0
        and held < 22 * 2**20
    )


def solution(mesh):
    sp, tp = mesh.shape["sp"], mesh.shape["tp"]

    def call(*args):
        if suits_planes(mesh, args):
            return jax.shard_map(
                per_device_planes,
                mesh=mesh,
                in_specs=(
                    P("sp", "tp"),
                    P(),
                    P("sp", "tp"),
                    P("sp", "tp"),
                    P("sp", "tp"),
                    P("sp", "tp"),
                    P(),
                    P(),
                    P("tp"),
                    P("tp", None, None),
                    P("tp"),
                    P("sp", "tp"),
                    P("sp", "tp"),
                ),
                out_specs=P("sp", "tp"),
                check_vma=False,
            )(*args)
        kv_local = args[3].shape[1] // args[6].shape[0] // tp
        groups_local = args[9].shape[0] // tp
        fits = sp % 2 == 0 and kv_local % 2 == 0 and groups_local % 2 == 0
        pair = 2 if fits else 1
        inner = Mesh(mesh.devices.reshape(sp // pair, pair, tp), ("so", "si", "tp"))
        rows = ("so", "si")
        return jax.shard_map(
            per_device,
            mesh=inner,
            in_specs=(
                P(rows, "tp"),
                P(),
                P(rows, "tp"),
                P(rows, "tp"),
                P(rows, "tp"),
                P(rows, "tp"),
                P(),
                P(),
                P("tp"),
                P("tp", None, None),
                P("tp"),
                P(rows, "tp"),
                P(rows, "tp"),
            ),
            out_specs=P(rows, "tp"),
            check_vma=False,
        )(*args)

    return call
```

```python
import functools

import jax
import jax.numpy as jnp
from jax import lax
from jax.experimental import pallas as pl
from jax.experimental.pallas import tpu as pltpu
from jax.sharding import Mesh
from jax.sharding import PartitionSpec as P

WINDOW = 128


epsilon = 1e-06
longest_lag = 15


def from_behind(block, axis):
    devices = range(lax.axis_size(axis))
    route = [(i - 1, i) for i in devices if i - 1 in devices]
    return lax.ppermute(block, axis, route)


def swap(block, axis):
    count = lax.axis_size(axis)
    return lax.ppermute(block, axis, [(i, count - 1 - i) for i in range(count)])


def row_norm(values, gain):
    return values * lax.rsqrt(jnp.mean(values * values, axis=-1, keepdims=True) + epsilon) * gain


def after(value, *others):
    return lax.optimization_barrier((value,) + others)[0]


def ordered(mine, theirs, index, dim):
    return jnp.where(
        index == 0,
        jnp.concatenate([mine, theirs], axis=dim),
        jnp.concatenate([theirs, mine], axis=dim),
    )


def both_cores(block, dim):
    if lax.axis_size("tp") == 2:
        return ordered(block, swap(block, "tp"), lax.axis_index("tp"), dim)
    return lax.all_gather(block, "tp", axis=dim, tiled=True)


def per_device(
    tokens,
    norm_gain,
    w_query,
    w_key,
    w_value,
    w_pool_in,
    query_gain,
    key_gain,
    sinks,
    w_mix,
    pool_scale,
    w_out_attn,
    w_out_pool,
):
    pair = lax.axis_size("si")
    place = lax.axis_index("si")
    outer = lax.axis_index("so")

    def share(array, owner, dim):
        size = array.shape[dim] // pair
        return lax.dynamic_slice_in_dim(array, owner * size, size, dim)

    def mine(arrays):
        return [share(a, place, 1) for a in arrays]

    def other(arrays):
        return [share(a, pair - 1 - place, 1) for a in arrays]

    def joined(own, came, dim):
        return own if pair == 1 else ordered(own, came, place, dim)

    def gathered(rows):
        return lax.all_gather(rows, "so", axis=0, tiled=True)

    qkv_parts = (w_query, w_key, w_value)
    qkv_own = jnp.concatenate(mine(qkv_parts), axis=1)
    if pair == 1:
        qkv_rows, pool_rows, attn_rows, mixed_rows = qkv_own, w_pool_in, w_out_attn, w_out_pool
        row_half = tokens
    else:
        qkv_came = swap(jnp.concatenate(other(qkv_parts), axis=1), "si")
        qkv_rows = joined(qkv_own, qkv_came, 0)
        late = lax.optimization_barrier((w_pool_in, w_out_attn, w_out_pool, qkv_came))[:3]
        came = [swap(share(w, pair - 1 - place, 1), "si") for w in late]
        pool_rows, attn_rows, mixed_rows = [
            joined(share(w, place, 1), c, 0) for w, c in zip((w_pool_in, w_out_attn, w_out_pool), came)
        ]
        row_half = joined(tokens, swap(after(tokens, qkv_came), "si"), 0)
    w_qkv = gathered(qkv_rows)
    w_pool = gathered(after(pool_rows, w_qkv))
    w_attn = gathered(after(attn_rows, w_pool))
    w_mixed = gathered(after(mixed_rows, w_attn))

    whole = both_cores(row_half, 1)
    row_count = whole.shape[0]
    normed = row_norm(whole.astype(jnp.float32), norm_gain).astype(jnp.bfloat16)
    qkv_raw = jnp.dot(normed, w_qkv, preferred_element_type=jnp.float32)
    head_size = query_gain.shape[0]
    query_width = w_query.shape[1] // pair
    kv_width = w_key.shape[1] // pair
    query_heads = query_width // head_size
    kv_local = kv_width // head_size
    per_kv = query_heads // kv_local
    query_raw = qkv_raw[:, :query_width]
    key_raw = qkv_raw[:, query_width : query_width + kv_width]
    value_raw = qkv_raw[:, query_width + kv_width :]
    queries = row_norm(query_raw.reshape(row_count, query_heads, head_size), query_gain).astype(
        jnp.bfloat16
    )
    key_rows = row_norm(key_raw.reshape(row_count, kv_local, head_size), key_gain).astype(
        jnp.bfloat16
    )
    values = value_raw.astype(jnp.bfloat16).reshape(row_count, kv_local, head_size)
    kv_tail = jnp.concatenate(
        [key_rows[-WINDOW:].reshape(WINDOW, -1), values[-WINDOW:].reshape(WINDOW, -1)], axis=1
    )
    kv_prev = from_behind(kv_tail, "so").reshape(WINDOW, 2, kv_local, head_size)
    offset = outer * row_count
    blocks = row_count // WINDOW

    def banded(previous, source):
        earlier = jnp.concatenate([previous, source[: row_count - WINDOW]], axis=0).reshape(
            blocks, WINDOW, kv_local, head_size
        )
        return jnp.concatenate(
            [earlier, source.reshape(blocks, WINDOW, kv_local, head_size)], axis=1
        )

    band_keys = banded(kv_prev[:, 0], key_rows)
    band_values = banded(kv_prev[:, 1], values)
    query_blocks = queries.reshape(blocks, WINDOW, kv_local, per_kv, head_size)
    scores = jnp.einsum(
        "bqkgd,bjkd->bkgqj", query_blocks, band_keys, preferred_element_type=jnp.float32
    ) * head_size ** (-0.5)
    query_index = jnp.arange(WINDOW)[:, None]
    key_index = jnp.arange(2 * WINDOW)[None, :]
    distance = query_index + WINDOW - key_index
    key_pos = offset + jnp.arange(blocks)[:, None, None] * WINDOW - WINDOW + key_index[None]
    valid = (distance[None] >= 0) & (distance[None] < WINDOW) & (key_pos >= 0)
    sink_logit = share(sinks, place, 0).reshape(kv_local, per_kv)[None, :, :, None, None]
    scores = jnp.where(valid[:, None, None], scores, -1e30)
    row_top = jnp.maximum(scores.max(axis=-1, keepdims=True), sink_logit)
    lifted = jnp.exp(scores - row_top)
    weights = (
        lifted / (lifted.sum(axis=-1, keepdims=True) + jnp.exp(sink_logit - row_top))
    ).astype(jnp.bfloat16)
    attended = (
        jnp.einsum("bkgqj,bjkd->bqkgd", weights, band_values, preferred_element_type=jnp.float32)
        .astype(jnp.bfloat16)
        .reshape(row_count, query_heads * head_size)
    )

    def all_heads(block):
        if pair == 2:
            block = joined(block, swap(block, "si"), 1)
        return both_cores(block, 1)

    attended_all = all_heads(attended)

    pool_in = jnp.dot(normed, w_pool, preferred_element_type=jnp.float32).astype(jnp.bfloat16)
    pool_prev = from_behind(pool_in[-longest_lag:], "so")
    mix = share(w_mix, place, 0)
    groups_local = mix.shape[0]
    group_dim = mix.shape[1]
    first_group = (lax.axis_index("tp") * pair + place) * groups_local
    group_ids = first_group + jnp.arange(groups_local, dtype=jnp.int32)
    spans = jnp.repeat(jnp.left_shift(jnp.int32(2), group_ids % 4), group_dim)
    extended = jnp.concatenate([pool_prev, pool_in], axis=0).astype(jnp.float32)
    window_sum = jnp.zeros((row_count, spans.shape[0]), jnp.float32)
    for back_step in range(longest_lag + 1):
        shifted = extended[longest_lag - back_step : longest_lag - back_step + row_count]
        window_sum = window_sum + jnp.where(back_step < spans[None, :], shifted, 0.0)
    positions = (offset + jnp.arange(1, row_count + 1, dtype=jnp.int32)).astype(jnp.float32)
    divisor = jnp.minimum(positions[:, None], spans.astype(jnp.float32)[None, :])
    contrast = (window_sum / divisor - extended[longest_lag:]).astype(jnp.bfloat16)
    mixed = jnp.einsum(
        "tgc,gcd->tgd",
        contrast.reshape(row_count, groups_local, group_dim),
        mix,
        preferred_element_type=jnp.float32,
    ).reshape(row_count, -1)
    pooled = (mixed * share(pool_scale, place, 0)).astype(jnp.bfloat16)
    pooled_all = all_heads(pooled)

    def project(owner):
        total = jnp.dot(share(attended_all, owner, 0), w_attn, preferred_element_type=jnp.float32)
        result = total + jnp.dot(
            share(pooled_all, owner, 0), w_mixed, preferred_element_type=jnp.float32
        )
        return result.astype(jnp.bfloat16)

    if pair == 1:
        return project(0)
    away = project(pair - 1 - place)
    came_back = swap(away, "si")
    return joined(project(place), came_back, 1)


MESH = pl.DeviceIdType.MESH
NEGATIVE = -1e30


def remote(src, dst, send_sem, recv_sem, device):
    return pltpu.make_async_remote_copy(
        src_ref=src,
        dst_ref=dst,
        send_sem=send_sem,
        recv_sem=recv_sem,
        device_id=device,
        device_id_type=MESH,
    )


def aligned(index, size):
    return pl.ds(pl.multiple_of(index * size, size), size)


class Place:
    def __init__(self, planes):
        self.sp, self.c = lax.axis_index("sp"), lax.axis_index("tp")
        self.planes = planes
        self.z, self.p = lax.div(self.sp, 4), lax.rem(self.sp, 4)
        x, y = lax.rem(self.p, 2), lax.div(self.p, 2)
        self.xn, self.yn, self.dg = self.p + 1 - 2 * x, self.p + 2 - 4 * y, 3 - self.p
        self.mates = (self.xn, self.yn, self.dg)
        self.has_above, self.has_below = self.z < planes - 1, self.z > 0

    def mate(self, p):
        return (self.z * 4 + p, self.c)

    def partner(self):
        return (self.sp, 1 - self.c)

    def above(self):
        return (lax.rem(self.sp + 4, 4 * self.planes), self.c)

    def below(self):
        return (lax.rem(self.sp + 4 * self.planes - 4, 4 * self.planes), self.c)

    def greet(self):
        sem = pltpu.get_barrier_semaphore()
        for p in self.mates:
            pl.semaphore_signal(sem, inc=1, device_id=self.mate(p), device_id_type=MESH)
        pl.semaphore_signal(sem, inc=1, device_id=self.partner(), device_id_type=MESH)

        @pl.when(self.has_above)
        def _():
            pl.semaphore_signal(sem, inc=1, device_id=self.above(), device_id_type=MESH)

        @pl.when(self.has_below)
        def _():
            pl.semaphore_signal(sem, inc=1, device_id=self.below(), device_id_type=MESH)

    def barrier(self):
        sem = pltpu.get_barrier_semaphore()
        inner = self.has_above & self.has_below

        @pl.when(inner)
        def _():
            pl.semaphore_wait(sem, 6)

        @pl.when(jnp.logical_not(inner))
        def _():
            pl.semaphore_wait(sem, 5)


class Rows:
    def __init__(self, at, own, held, sems):
        self.at, self.own, self.held = at, own, held
        self.local_sem, self.near, self.recv, self.up, self.down = sems

    def slot(self, plane, p, cut=None):
        if cut is None:
            return self.held.at[plane, p]
        return self.held.at[plane, p, cut[0], cut[1]]

    def to_mate(self, index, p):
        at = self.at
        return [
            remote(
                src,
                self.slot(at.z, at.p, cut),
                self.near.at[index],
                self.recv.at[at.z, at.p],
                at.mate(p),
            )
            for src, cut, _ in self.own(p)
        ]

    def here(self):
        at = self.at
        return [
            pltpu.make_async_copy(src, self.slot(at.z, at.p, cut), self.local_sem.at[k])
            for k, (src, cut, copied) in enumerate(self.own(at.p))
            if copied
        ]

    def hop(self, plane, p, upward, src=None, cut=None):
        at = self.at
        dst = self.slot(plane, p, cut)
        return remote(
            dst if src is None else src,
            dst,
            (self.up if upward else self.down).at[plane, p],
            self.recv.at[plane, p],
            at.above() if upward else at.below(),
        )

    def send(self, plane, p, upward):
        @pl.when(self.at.has_above if upward else self.at.has_below)
        def _():
            self.hop(plane, p, upward).start()

    def begin_far(self):
        at = self.at
        for upward in (True, False):

            @pl.when(at.has_above if upward else at.has_below)
            def _():
                for src, cut, _ in self.own(at.p):
                    self.hop(at.z, at.p, upward, src, cut).start()

    def begin_near(self):
        for index, p in enumerate(self.at.mates):
            for copy in self.to_mate(index, p):
                copy.start()
        for copy in self.here():
            copy.start()

    def arrived(self, plane, p):
        self.hop(plane, p, True).wait_recv()

    def pass_near(self):
        at = self.at
        for p in at.mates:
            self.arrived(at.z, p)
            self.send(at.z, p, True)
            self.send(at.z, p, False)

    def pass_far(self, distance, index):
        at = self.at
        p = ((at.p,) + at.mates)[index]
        low, high = at.z - distance, at.z + distance

        @pl.when(low >= 0)
        def _():
            self.arrived(low, p)
            self.send(low, p, True)

        @pl.when(high < at.planes)
        def _():
            self.arrived(high, p)
            self.send(high, p, False)

    def finish(self):
        at = self.at
        whole = self.slot(at.z, at.p)
        for index, p in enumerate(at.mates):
            remote(
                whole, whole, self.near.at[index], self.recv.at[at.z, at.p], at.mate(p)
            ).wait_send()
        for plane in range(at.planes):
            for p in range(4):

                @pl.when(at.has_above & (at.z >= plane))
                def _():
                    self.hop(plane, p, True).wait_send()

                @pl.when(at.has_below & (at.z <= plane))
                def _():
                    self.hop(plane, p, False).wait_send()


def layer_kernel(planes, head, *refs):
    (tok, w_query, w_pool, w_attn, w_mixed, sinks) = refs[:6]
    given, out = refs[6:13], refs[13]
    (raw, xs, ws, kvw, acc, q, kv, pool, ma, ws_out, ys) = refs[14:25]
    held_inputs, load_sems = refs[-8:-1], refs[-1]
    in_sems, out_sems = refs[25:30], refs[30:35]
    (raw_sems, t_send, t_recv, td_send, td_recv, h_send, h_recv) = refs[35:42]
    (m_send, m_recv, f_send, f_recv, d_send, d_recv, r_send, r_recv, r_local) = refs[42:-8]

    loads = [
        pltpu.make_async_copy(src, dst, load_sems.at[k])
        for k, (src, dst) in enumerate(zip(given, held_inputs))
    ]
    for load in loads:
        load.start()
    w_key, w_value, gain, query_gain, key_gain, pool_scale, mix = held_inputs
    at = Place(planes)
    at.greet()
    c, p, z = at.c, at.p, at.z
    pair = 2 * head
    count, half = tok.shape
    part = count // 2
    deep = xs.shape[3]
    blocks = half // deep
    width, channels = q.shape[1], pool.shape[1]
    steps, tall, wide = ma.shape[1:]
    block = tall // 4
    columns = ws_out.shape[3]
    lag_rows = pool.shape[0] - 4 * count

    for load in loads:
        load.wait()
    low_lane = lax.broadcasted_iota(jnp.int32, (w_key.shape[0], pair), 1) < head
    for k in range(4):
        tile = slice(k // 2 * pair, (k // 2 + 1) * pair)
        key_tile, value_tile = w_key[:, tile], w_value[:, tile]
        if k % 2:
            key_tile = pltpu.roll(key_tile.astype(jnp.float32), head, 1).astype(jnp.bfloat16)
        else:
            value_tile = pltpu.roll(value_tile.astype(jnp.float32), head, 1).astype(jnp.bfloat16)
        kvw[k] = jnp.where(low_lane, key_tile, value_tile)
    ws[z, p, :, width : width + pair] = kvw[p]

    every = pl.ds(0, w_query.shape[0])

    def own_in(place):
        return [
            (w_query.at[:, aligned(place, width)], (every, pl.ds(0, width)), True),
            (kvw.at[place], (every, pl.ds(width, pair)), False),
            (w_pool.at[:, aligned(place, channels)], (every, pl.ds(width + pair, channels)), True),
        ]

    def own_out(place):
        rows = w_attn.shape[0]
        return [
            (w_attn.at[:, aligned(place, columns)], (pl.ds(0, rows), pl.ds(0, columns)), True),
            (w_mixed.at[:, aligned(place, columns)], (pl.ds(rows, rows), pl.ds(0, columns)), True),
        ]

    rows_in = Rows(at, own_in, ws, in_sems)
    rows_out = Rows(at, own_out, ws_out, out_sems)

    at.barrier()
    raw_local = pltpu.make_async_copy(tok, raw.at[c], raw_sems.at[0])
    raw_away = remote(tok, raw.at[c], raw_sems.at[1], raw_sems.at[2], at.partner())
    raw_away.start()
    raw_local.start()
    rows_in.begin_far()
    rows_in.begin_near()
    raw_local.wait()
    raw_away.wait_recv()

    norm_rows = 32

    def norm_step(index, carry):
        span = aligned(index, norm_rows)
        halves = [raw[k, span, :].astype(jnp.float32) for k in range(2)]
        total = sum(jnp.sum(v * v, axis=-1, keepdims=True) for v in halves)
        scale = lax.rsqrt(total / (2 * half) + epsilon)
        for k in range(2):
            normed = halves[k] * scale * gain[:, k * half : (k + 1) * half]
            normed = normed.astype(jnp.bfloat16)
            for b in range(blocks):
                xs[p, k * blocks + b, span, :] = normed[:, b * deep : (b + 1) * deep]
        return carry

    lax.fori_loop(0, count // norm_rows, norm_step, 0)

    def piece(place, h, core):
        return xs.at[place, pl.ds(core * blocks, blocks), pl.ds(h * part, part), :]

    def tokens_to(index, place, h, to):
        ref = piece(place, h, c)
        return remote(ref, ref, t_send.at[index], t_recv.at[place, h], at.mate(to))

    def tokens_over(index, place, h, core):
        ref = piece(place, h, core)
        return remote(ref, ref, td_send.at[index], td_recv.at[place, h], at.partner())

    sent = [(p, 0, at.xn), (p, 1, at.yn), (p, 1, at.xn), (p, 0, at.yn)]
    sent += [(at.xn, 0, at.yn), (at.yn, 1, at.xn)]
    crossed = [(at.xn, 0), (at.yn, 1), (at.xn, 1), (at.yn, 0), (at.dg, 0), (at.dg, 1)]
    for index in range(4):
        tokens_to(index, *sent[index]).start()
    rows_in.pass_near()

    def take_tokens(index, onward=None):
        place, h = crossed[index]
        tokens_to(0, place, h, at.xn).wait_recv()
        if onward is not None:
            tokens_to(onward, *sent[onward]).start()
        tokens_over(index, place, h, c).start()

    def first_tokens():
        take_tokens(0, 4)
        take_tokens(1, 5)

    def second_tokens():
        take_tokens(2)
        take_tokens(3)
        rows_out.begin_far()
        rows_out.begin_near()
        for place, h in crossed[:4]:
            tokens_over(0, place, h, 1 - c).wait_recv()

    def product(place, b, span, slots):
        if slots is None:
            return jnp.dot(
                xs[place, b, span, :],
                ws[b].reshape(deep, ws.shape[3]),
                preferred_element_type=jnp.float32,
            )
        total = None
        for source in slots:
            term = jnp.dot(
                xs[place, b, span, aligned(source, deep // 4)],
                ws[b, source],
                preferred_element_type=jnp.float32,
            )
            total = term if total is None else total + term
        return total

    def place_of(k):
        return jnp.where(k == 0, p, jnp.where(k == 1, at.xn, jnp.where(k == 2, at.yn, at.dg)))

    def accumulate(b, places, slots=None, fresh=False, halves=(0, 2)):
        tall_count = halves[1] - halves[0]

        def one(index, carry):
            k = places[0] + lax.div(index, tall_count)
            span = aligned(halves[0] + lax.rem(index, tall_count), part)
            term = product(place_of(k), b, span, slots)
            acc[k, span, :] = term if fresh else acc[k, span, :] + term
            return carry

        lax.fori_loop(0, tall_count * (places[1] - places[0]), one, 0)

    mine, sides, near, everywhere = (0, 1), (1, 3), (0, 3), (0, 4)
    early, late = (p, at.xn, at.yn), (at.dg,)

    def far_unit(distance, places, slots=None, halves=(0, 2)):
        for b in (z - distance, z + distance):

            @pl.when((b >= 0) & (b < planes))
            def _():
                accumulate(b, places, slots, False, halves)

    def across(h):
        span = aligned(h, part)

        def whole(first, last, partial):
            total = None if partial is None else product(at.dg, partial, span, early)
            for b in range(first, last):
                term = product(at.dg, b, span, None)
                total = term if total is None else total + term
            acc[3, span, :] = total

        @pl.when(at.has_above & at.has_below)
        def _():
            whole(0, planes, None)

        @pl.when(jnp.logical_not(at.has_below))
        def _():
            whole(0, planes - 1, planes - 1)

        @pl.when(jnp.logical_not(at.has_above))
        def _():
            whole(1, planes, 0)

    def last_tokens():
        take_tokens(5)
        take_tokens(4)

    def last_crossed(h):
        tokens_over(0, at.dg, h, 1 - c).wait_recv()

    def start_mine():
        for copy in rows_in.here():
            copy.wait()
        accumulate(z, mine, fresh=True)

    def one_half(h, wait):
        if wait:
            last_tokens()
        far_unit(planes - 1, near, early, (h, h + 1))
        last_crossed(h)
        across(h)
        if wait:
            rows_in.pass_far(planes - 1, 3)
        far_unit(planes - 1, everywhere, late, (h, h + 1))
        settle_half(h)

    final = 4 * (planes - 1) - 1
    events = {}

    def plan(step, event):
        events.setdefault(min(step, final - 1), []).append(event)

    plan(4 * planes // 3 - 1, start_mine)
    plan(4 * planes // 3, first_tokens)
    for distance in range(1, planes - 1):
        plan(max(4 * planes // 3, 4 * distance - 1), functools.partial(far_unit, distance, mine))
    plan(2 * planes - 1, second_tokens)
    plan(2 * planes - 1, lambda: accumulate(z, sides, fresh=True))
    for distance in range(1, planes - 1):
        turn = max(2 * planes - 2 + distance, 4 * distance - 1)
        plan(turn, functools.partial(far_unit, distance, sides))
    for at_step in range(final):
        rows_in.pass_far(at_step // 4 + 1, at_step % 4)
        for event in events.get(at_step, []):
            event()

    low_part = lax.broadcasted_iota(jnp.int32, (part, pair), 1) < head
    query_pair = jnp.concatenate([query_gain[...]] * 2, axis=1)
    key_pair = jnp.concatenate([key_gain[...]] * 2, axis=1)

    def settle(total, place, h):
        span = aligned(place * 2 + h, part)
        for k in range(width // pair):
            v = total[:, pair * k : pair * (k + 1)]
            square = v * v
            lo = jnp.sum(jnp.where(low_part, square, 0.0), axis=-1, keepdims=True) / head
            hi = jnp.sum(jnp.where(low_part, 0.0, square), axis=-1, keepdims=True) / head
            scale = jnp.where(low_part, lax.rsqrt(lo + epsilon), lax.rsqrt(hi + epsilon))
            q[span, pair * k : pair * (k + 1)] = (v * scale * query_pair).astype(jnp.bfloat16)
        v = total[:, width : width + pair]
        lo = jnp.sum(jnp.where(low_part, v * v, 0.0), axis=-1, keepdims=True) / head
        both = jnp.where(low_part, v * lax.rsqrt(lo + epsilon) * key_pair, v)
        base = pl.multiple_of((place * 2 + h) * part, part)
        kv[pl.ds(base + block, part), :pair] = both.astype(jnp.bfloat16)
        kv[pl.ds(base + block, part), pair:] = pltpu.roll(both, head, 1).astype(jnp.bfloat16)
        pool[pl.ds(base + lag_rows, part), :] = total[:, width + pair :].astype(jnp.bfloat16)

    def settle_half(h):
        def one(k, carry):
            settle(acc[k, aligned(h, part), :], place_of(k), h)
            return carry

        lax.fori_loop(0, 4, one, 0)

    one_half(1, True)

    def halo(k):
        ref, rows = ((kv, block), (pool, lag_rows))[k]
        src, dst = ref.at[pl.ds(4 * count, rows), :], ref.at[pl.ds(0, rows), :]
        return remote(src, dst, h_send.at[k], h_recv.at[k], at.above())

    @pl.when(at.has_above)
    def _():
        halo(0).start()
        halo(1).start()

    @pl.when(z == 0)
    def _():
        kv[0:block, :] = jnp.zeros((block, kv.shape[1]), jnp.bfloat16)
        pool[0:lag_rows, :] = jnp.zeros((lag_rows, channels), jnp.bfloat16)

    heads = width // head
    pairs = heads // 2
    query = lax.rem(lax.broadcasted_iota(jnp.int32, (pairs * block, block), 0), block)
    key = lax.broadcasted_iota(jnp.int32, (pairs * block, block), 1)
    current = key <= query
    low_keys = lax.broadcasted_iota(jnp.int32, (2 * block, pair), 1) < head
    log2_e = 1.4426950408889634
    line = lax.broadcasted_iota(jnp.int32, (block, 1), 0)
    window = lax.shift_left(jnp.int32(2), p).astype(jnp.float32)
    slot = c * 4 + p

    def mixers(j, place):
        index = place * steps + j
        base = pl.multiple_of(index * block, block)
        first = index == 0
        kvs = kv[pl.ds(base, 2 * block), :]
        straight, turned = kvs[:, :pair], kvs[:, pair:]
        zero = jnp.zeros_like(straight)
        keys = (jnp.where(low_keys, straight, zero), jnp.where(low_keys, zero, turned))
        values = (jnp.where(low_keys, turned, zero), jnp.where(low_keys, zero, straight))
        absent = jnp.where((z == 0) & first, NEGATIVE, 0.0)
        span = aligned(place, block)
        q_pairs = [q[pl.ds(base, block), pair * k : pair * (k + 1)] for k in range(pairs)]
        q_stack = jnp.concatenate(q_pairs, axis=0)
        total = None
        for side in range(2):
            sink = jnp.concatenate(
                [
                    jnp.full((block, block), sinks[p * heads + 2 * k + side] * log2_e)
                    for k in range(pairs)
                ],
                axis=0,
            )
            scores = lax.dot_general(
                q_stack,
                keys[side],
                (((1,), (1,)), ((), ())),
                preferred_element_type=jnp.float32,
            )
            scores = jnp.where(current, scores[:, block:], scores[:, :block] + absent)
            scores = scores * (head ** (-0.5) * log2_e)
            top = jnp.maximum(jnp.max(scores, axis=-1, keepdims=True), sink)
            lifted = jnp.exp2(scores - top)
            under = jnp.sum(lifted, axis=-1, keepdims=True) + jnp.exp2(sink - top)
            weights = lifted * (1.0 / under)
            weights = jnp.concatenate(
                [jnp.where(current, 0.0, weights), jnp.where(current, weights, 0.0)], axis=1
            ).astype(jnp.bfloat16)
            term = jnp.dot(weights, values[side], preferred_element_type=jnp.float32)
            total = term if total is None else total + term
        for k in range(pairs):
            ma[slot, j, span, 2 * pair * k : 2 * pair * k + pair] = total[
                block * k : block * (k + 1)
            ].astype(jnp.bfloat16)
        series = pool[pl.ds(base, lag_rows + block), :].astype(jnp.float32)
        sums, lag = [series], 1
        while 2 * lag <= lag_rows:
            sums.append(sums[-1] + pltpu.roll(sums[-1], lag, 0))
            lag *= 2
        window_sum = sums[-1]
        for k in range(len(sums) - 2, 0, -1):
            window_sum = jnp.where(p == k - 1, sums[k], window_sum)
        position = (z * 4 * count + base + 1 + line).astype(jnp.float32)
        share = 1.0 / jnp.minimum(position, window)
        contrast = window_sum[lag_rows:] * share - series[lag_rows:]
        mixed = jnp.dot(contrast.astype(jnp.bfloat16), mix[p], preferred_element_type=jnp.float32)
        mixed = (mixed * pool_scale[:, aligned(p, channels)]).astype(jnp.bfloat16)
        for k in range(channels // pair):
            ma[slot, j, span, (2 * k + 1) * pair : (2 * k + 2) * pair] = mixed[
                :, pair * k : pair * (k + 1)
            ]

    def half_of(core, place, j, k):
        return ma.at[core * 4 + place, j, aligned(k, tall // 2), :]

    def to_mate(index, j, k, to):
        ref = half_of(c, p, j, k)
        return remote(ref, ref, m_send.at[index, j, k], m_recv.at[p, j, k], at.mate(to))

    def onward(k, j, place, to):
        ref = half_of(c, place, j, k)
        return remote(ref, ref, f_send.at[k, j], f_recv.at[k, j], at.mate(to))

    def over(index, j, place, core):
        ref = ma.at[core * 4 + place, j]
        return remote(ref, ref, d_send.at[index, j], d_recv.at[place, j], at.partner())

    def came(place, j, k):
        ref = half_of(c, place, j, k)
        remote(ref, ref, m_send.at[0, j, k], m_recv.at[place, j, k], at.partner()).wait_recv()

    def mix_step(index, carry):
        j = steps - 1 - index

        @pl.when(index == 1)
        def _():
            one_half(0, False)

        @pl.when((j == 0) & at.has_below)
        def _():
            halo(0).wait_recv()
            halo(1).wait_recv()

        def two(turn, inner):
            mixers(j, 2 * turn)
            mixers(j, 2 * turn + 1)
            for index, to in enumerate((at.xn, at.yn)):
                to_mate(index, j, turn, to).start()
            return inner

        lax.fori_loop(0, 2, two, 0)
        over(0, j, p, c).start()

        @pl.when(index == 0)
        def _():
            rows_out.pass_near()

        return carry

    lax.fori_loop(0, steps, mix_step, 0)

    def pass_on(j):
        came(at.xn, j, 0)
        onward(0, j, at.xn, at.yn).start()
        came(at.yn, j, 0)
        came(at.yn, j, 1)
        onward(1, j, at.yn, at.xn).start()
        over(2, j, at.yn, c).start()
        came(at.xn, j, 1)
        over(1, j, at.xn, c).start()

    waiting = list(range(steps - 1, -1, -1))
    total_far = 4 * (planes - 1)
    for at_step in range(total_far):
        rows_out.pass_far(at_step // 4 + 1, at_step % 4)
        passed = steps - len(waiting)
        while waiting and at_step + 1 >= (passed + 1) * total_far // (steps + 1):
            pass_on(waiting.pop(0))
            passed += 1
    for j in waiting:
        pass_on(j)
    for copy in rows_out.here():
        copy.wait()

    def landing(j, place):
        return out.at[aligned(j, block), aligned(place, columns)]

    def result(index, j, to):
        return remote(
            ys.at[j, aligned(to, block), :],
            landing(j, p),
            r_send.at[index, j],
            r_recv.at[p, j],
            at.mate(to),
        )

    def result_here(j):
        return pltpu.make_async_copy(ys.at[j, aligned(p, block), :], landing(j, p), r_local.at[j])

    def last_step(index, carry):
        j = steps - 1 - index
        for k in range(2):
            onward(k, j, at.dg, at.xn).wait_recv()
        over(3, j, at.dg, c).start()
        for place in range(4):
            over(0, j, place, 1 - c).wait_recv()
        total = None
        for i in range(8):
            first = 2 * i
            weight = ws_out[first // 4, first % 4 : first % 4 + 2].reshape(wide, columns)
            term = jnp.dot(ma[i, j], weight, preferred_element_type=jnp.float32)
            total = term if total is None else total + term
        ys[j] = total.astype(jnp.bfloat16)
        for k, to in enumerate(at.mates):
            result(k, j, to).start()
        result_here(j).start()
        return carry

    lax.fori_loop(0, steps, last_step, 0)

    def finish_step(j, carry):
        for k, to in enumerate(at.mates):
            remote(
                ys.at[j, pl.ds(0, block), :],
                landing(j, to),
                r_send.at[k, j],
                r_recv.at[to, j],
                at.mate(to),
            ).wait_recv()
        result_here(j).wait()
        for k, to in enumerate(at.mates):
            result(k, j, to).wait_send()
        for k in range(2):
            to_mate(0, j, k, at.xn).wait_send()
            to_mate(1, j, k, at.yn).wait_send()
        onward(0, j, at.xn, at.yn).wait_send()
        onward(1, j, at.yn, at.xn).wait_send()
        for k, place in enumerate((p,) + at.mates):
            over(k, j, place, c).wait_send()
        return carry

    lax.fori_loop(0, steps, finish_step, 0)
    raw_away.wait_send()
    for index in range(6):
        tokens_to(index, *sent[index]).wait_send()
        tokens_over(index, *crossed[index], c).wait_send()

    @pl.when(at.has_above)
    def _():
        halo(0).wait_send()
        halo(1).wait_send()

    rows_in.finish()
    rows_out.finish()


def per_device_planes(
    tokens,
    norm_gain,
    w_query,
    w_key,
    w_value,
    w_pool_in,
    query_gain,
    key_gain,
    sinks,
    w_mix,
    pool_scale,
    w_out_attn,
    w_out_pool,
):
    planes = lax.axis_size("sp") // 4
    head = query_gain.shape[0]
    count, half = tokens.shape
    in_rows, out_rows = w_query.shape[0], 2 * w_out_attn.shape[0]
    width, channels = w_query.shape[1] // 4, w_pool_in.shape[1] // 4
    columns = w_out_attn.shape[1] // 4
    pair, deep, steps = 2 * head, 4 * in_rows, count // WINDOW
    in_width = width + pair + channels
    lines = [a.reshape(1, -1) for a in (norm_gain, query_gain, key_gain, pool_scale)]
    given = (w_key, w_value, *lines, w_mix)
    anywhere = pl.BlockSpec(memory_space=pl.ANY)
    smem = pl.BlockSpec(memory_space=pltpu.SMEM)
    dma = pltpu.SemaphoreType.DMA

    def held(*shape):
        return pltpu.VMEM(shape, jnp.bfloat16)

    row_sems = [dma((3,)), dma((3,)), dma((planes, 4)), dma((planes, 4)), dma((planes, 4))]
    return pl.pallas_call(
        functools.partial(layer_kernel, planes, head),
        out_shape=jax.ShapeDtypeStruct(tokens.shape, jnp.bfloat16),
        in_specs=[anywhere] * 5 + [smem] + [anywhere] * 7,
        out_specs=anywhere,
        scratch_shapes=[
            held(2, count, half),
            held(4, planes, count, deep),
            held(planes, 4, in_rows, in_width),
            held(4, in_rows, pair),
            pltpu.VMEM((4, count, in_width), jnp.float32),
            held(4 * count, width),
            held(4 * count + WINDOW, 2 * pair),
            held(4 * count + longest_lag + 1, channels),
            held(8, steps, 4 * WINDOW, width + channels),
            held(planes, 4, out_rows, columns),
            held(steps, 4 * WINDOW, columns),
        ]
        + row_sems
        + row_sems
        + [dma((3,)), dma((6,)), dma((4, 2)), dma((6,)), dma((4, 2)), dma((2,)), dma((2,))]
        + [dma((2, steps, 2)), dma((4, steps, 2)), dma((2, steps)), dma((2, steps))]
        + [dma((4, steps)), dma((4, steps)), dma((3, steps)), dma((4, steps)), dma((steps,))]
        + [pltpu.VMEM(a.shape, a.dtype) for a in given]
        + [dma((len(given),))],
        compiler_params=pltpu.CompilerParams(
            collective_id=0, has_side_effects=True, vmem_limit_bytes=63 * 2**20
        ),
        name="layer",
    )(tokens, w_query, w_pool_in, w_out_attn, w_out_pool, sinks, *given)


def suits_planes(mesh, args):
    sp, tp = mesh.shape["sp"], mesh.shape["tp"]
    tokens, w_query, w_key, w_pool_in = args[0], args[2], args[3], args[5]
    head, groups = args[6].shape[0], args[9].shape[0]
    w_out_attn, w_out_pool = args[11], args[12]
    if tp != 2 or sp % 4 or sp < 12 or 2 * head != 128:
        return False
    share = 4 * tp
    rows = tokens.shape[0] // sp
    width, channels = w_query.shape[1] // share, w_pool_in.shape[1] // share
    held = 2 * 4 * rows * tokens.shape[1] + 2 * w_query.shape[0] * (width + 128 + channels)
    return (
        w_key.shape[1] == share * head
        and groups == share
        and rows % (4 * WINDOW) == 0
        and width % 128 == 0
        and width == channels
        and 2 * w_out_attn.shape[0] // sp == width
        and 2 * w_out_pool.shape[0] // sp == channels
        and w_out_attn.shape[0] // sp == 2 * head
        and w_query.shape[0] // sp % 16 == 0
        and w_out_attn.shape[1] % (share * 128) == 0
        and held < 22 * 2**20
    )


def solution(mesh):
    sp, tp = mesh.shape["sp"], mesh.shape["tp"]

    def call(*args):
        if suits_planes(mesh, args):
            return jax.shard_map(
                per_device_planes,
                mesh=mesh,
                in_specs=(
                    P("sp", "tp"),
                    P(),
                    P("sp", "tp"),
                    P("sp", "tp"),
                    P("sp", "tp"),
                    P("sp", "tp"),
                    P(),
                    P(),
                    P("tp"),
                    P("tp", None, None),
                    P("tp"),
                    P("sp", "tp"),
                    P("sp", "tp"),
                ),
                out_specs=P("sp", "tp"),
                check_vma=False,
            )(*args)
        kv_local = args[3].shape[1] // args[6].shape[0] // tp
        groups_local = args[9].shape[0] // tp
        fits = sp % 2 == 0 and kv_local % 2 == 0 and groups_local % 2 == 0
        pair = 2 if fits else 1
        inner = Mesh(mesh.devices.reshape(sp // pair, pair, tp), ("so", "si", "tp"))
        rows = ("so", "si")
        return jax.shard_map(
            per_device,
            mesh=inner,
            in_specs=(
                P(rows, "tp"),
                P(),
                P(rows, "tp"),
                P(rows, "tp"),
                P(rows, "tp"),
                P(rows, "tp"),
                P(),
                P(),
                P("tp"),
                P("tp", None, None),
                P("tp"),
                P(rows, "tp"),
                P(rows, "tp"),
            ),
            out_specs=P(rows, "tp"),
            check_vma=False,
        )(*args)

    return call
```

```python
import functools

import jax
import jax.numpy as jnp
from jax import lax
from jax.experimental import pallas as pl
from jax.experimental.pallas import tpu as pltpu
from jax.sharding import Mesh
from jax.sharding import PartitionSpec as P

WINDOW = 128


epsilon = 1e-06
longest_lag = 15


def from_behind(block, axis):
    devices = range(lax.axis_size(axis))
    route = [(i - 1, i) for i in devices if i - 1 in devices]
    return lax.ppermute(block, axis, route)


def swap(block, axis):
    count = lax.axis_size(axis)
    return lax.ppermute(block, axis, [(i, count - 1 - i) for i in range(count)])


def row_norm(values, gain):
    return values * lax.rsqrt(jnp.mean(values * values, axis=-1, keepdims=True) + epsilon) * gain


def after(value, *others):
    return lax.optimization_barrier((value,) + others)[0]


def ordered(mine, theirs, index, dim):
    return jnp.where(
        index == 0,
        jnp.concatenate([mine, theirs], axis=dim),
        jnp.concatenate([theirs, mine], axis=dim),
    )


def both_cores(block, dim):
    if lax.axis_size("tp") == 2:
        return ordered(block, swap(block, "tp"), lax.axis_index("tp"), dim)
    return lax.all_gather(block, "tp", axis=dim, tiled=True)


def per_device(
    tokens,
    norm_gain,
    w_query,
    w_key,
    w_value,
    w_pool_in,
    query_gain,
    key_gain,
    sinks,
    w_mix,
    pool_scale,
    w_out_attn,
    w_out_pool,
):
    pair = lax.axis_size("si")
    place = lax.axis_index("si")
    outer = lax.axis_index("so")

    def share(array, owner, dim):
        size = array.shape[dim] // pair
        return lax.dynamic_slice_in_dim(array, owner * size, size, dim)

    def mine(arrays):
        return [share(a, place, 1) for a in arrays]

    def other(arrays):
        return [share(a, pair - 1 - place, 1) for a in arrays]

    def joined(own, came, dim):
        return own if pair == 1 else ordered(own, came, place, dim)

    def gathered(rows):
        return lax.all_gather(rows, "so", axis=0, tiled=True)

    qkv_parts = (w_query, w_key, w_value)
    qkv_own = jnp.concatenate(mine(qkv_parts), axis=1)
    if pair == 1:
        qkv_rows, pool_rows, attn_rows, mixed_rows = qkv_own, w_pool_in, w_out_attn, w_out_pool
        row_half = tokens
    else:
        qkv_came = swap(jnp.concatenate(other(qkv_parts), axis=1), "si")
        qkv_rows = joined(qkv_own, qkv_came, 0)
        late = lax.optimization_barrier((w_pool_in, w_out_attn, w_out_pool, qkv_came))[:3]
        came = [swap(share(w, pair - 1 - place, 1), "si") for w in late]
        pool_rows, attn_rows, mixed_rows = [
            joined(share(w, place, 1), c, 0) for w, c in zip((w_pool_in, w_out_attn, w_out_pool), came)
        ]
        row_half = joined(tokens, swap(after(tokens, qkv_came), "si"), 0)
    w_qkv = gathered(qkv_rows)
    w_pool = gathered(after(pool_rows, w_qkv))
    w_attn = gathered(after(attn_rows, w_pool))
    w_mixed = gathered(after(mixed_rows, w_attn))

    whole = both_cores(row_half, 1)
    row_count = whole.shape[0]
    normed = row_norm(whole.astype(jnp.float32), norm_gain).astype(jnp.bfloat16)
    qkv_raw = jnp.dot(normed, w_qkv, preferred_element_type=jnp.float32)
    head_size = query_gain.shape[0]
    query_width = w_query.shape[1] // pair
    kv_width = w_key.shape[1] // pair
    query_heads = query_width // head_size
    kv_local = kv_width // head_size
    per_kv = query_heads // kv_local
    query_raw = qkv_raw[:, :query_width]
    key_raw = qkv_raw[:, query_width : query_width + kv_width]
    value_raw = qkv_raw[:, query_width + kv_width :]
    queries = row_norm(query_raw.reshape(row_count, query_heads, head_size), query_gain).astype(
        jnp.bfloat16
    )
    key_rows = row_norm(key_raw.reshape(row_count, kv_local, head_size), key_gain).astype(
        jnp.bfloat16
    )
    values = value_raw.astype(jnp.bfloat16).reshape(row_count, kv_local, head_size)
    kv_tail = jnp.concatenate(
        [key_rows[-WINDOW:].reshape(WINDOW, -1), values[-WINDOW:].reshape(WINDOW, -1)], axis=1
    )
    kv_prev = from_behind(kv_tail, "so").reshape(WINDOW, 2, kv_local, head_size)
    offset = outer * row_count
    blocks = row_count // WINDOW

    def banded(previous, source):
        earlier = jnp.concatenate([previous, source[: row_count - WINDOW]], axis=0).reshape(
            blocks, WINDOW, kv_local, head_size
        )
        return jnp.concatenate(
            [earlier, source.reshape(blocks, WINDOW, kv_local, head_size)], axis=1
        )

    band_keys = banded(kv_prev[:, 0], key_rows)
    band_values = banded(kv_prev[:, 1], values)
    query_blocks = queries.reshape(blocks, WINDOW, kv_local, per_kv, head_size)
    scores = jnp.einsum(
        "bqkgd,bjkd->bkgqj", query_blocks, band_keys, preferred_element_type=jnp.float32
    ) * head_size ** (-0.5)
    query_index = jnp.arange(WINDOW)[:, None]
    key_index = jnp.arange(2 * WINDOW)[None, :]
    distance = query_index + WINDOW - key_index
    key_pos = offset + jnp.arange(blocks)[:, None, None] * WINDOW - WINDOW + key_index[None]
    valid = (distance[None] >= 0) & (distance[None] < WINDOW) & (key_pos >= 0)
    sink_logit = share(sinks, place, 0).reshape(kv_local, per_kv)[None, :, :, None, None]
    scores = jnp.where(valid[:, None, None], scores, -1e30)
    row_top = jnp.maximum(scores.max(axis=-1, keepdims=True), sink_logit)
    lifted = jnp.exp(scores - row_top)
    weights = (
        lifted / (lifted.sum(axis=-1, keepdims=True) + jnp.exp(sink_logit - row_top))
    ).astype(jnp.bfloat16)
    attended = (
        jnp.einsum("bkgqj,bjkd->bqkgd", weights, band_values, preferred_element_type=jnp.float32)
        .astype(jnp.bfloat16)
        .reshape(row_count, query_heads * head_size)
    )

    def all_heads(block):
        if pair == 2:
            block = joined(block, swap(block, "si"), 1)
        return both_cores(block, 1)

    attended_all = all_heads(attended)

    pool_in = jnp.dot(normed, w_pool, preferred_element_type=jnp.float32).astype(jnp.bfloat16)
    pool_prev = from_behind(pool_in[-longest_lag:], "so")
    mix = share(w_mix, place, 0)
    groups_local = mix.shape[0]
    group_dim = mix.shape[1]
    first_group = (lax.axis_index("tp") * pair + place) * groups_local
    group_ids = first_group + jnp.arange(groups_local, dtype=jnp.int32)
    spans = jnp.repeat(jnp.left_shift(jnp.int32(2), group_ids % 4), group_dim)
    extended = jnp.concatenate([pool_prev, pool_in], axis=0).astype(jnp.float32)
    window_sum = jnp.zeros((row_count, spans.shape[0]), jnp.float32)
    for back_step in range(longest_lag + 1):
        shifted = extended[longest_lag - back_step : longest_lag - back_step + row_count]
        window_sum = window_sum + jnp.where(back_step < spans[None, :], shifted, 0.0)
    positions = (offset + jnp.arange(1, row_count + 1, dtype=jnp.int32)).astype(jnp.float32)
    divisor = jnp.minimum(positions[:, None], spans.astype(jnp.float32)[None, :])
    contrast = (window_sum / divisor - extended[longest_lag:]).astype(jnp.bfloat16)
    mixed = jnp.einsum(
        "tgc,gcd->tgd",
        contrast.reshape(row_count, groups_local, group_dim),
        mix,
        preferred_element_type=jnp.float32,
    ).reshape(row_count, -1)
    pooled = (mixed * share(pool_scale, place, 0)).astype(jnp.bfloat16)
    pooled_all = all_heads(pooled)

    def project(owner):
        total = jnp.dot(share(attended_all, owner, 0), w_attn, preferred_element_type=jnp.float32)
        result = total + jnp.dot(
            share(pooled_all, owner, 0), w_mixed, preferred_element_type=jnp.float32
        )
        return result.astype(jnp.bfloat16)

    if pair == 1:
        return project(0)
    away = project(pair - 1 - place)
    came_back = swap(away, "si")
    return joined(project(place), came_back, 1)


MESH = pl.DeviceIdType.MESH
NEGATIVE = -1e30


def remote(src, dst, send_sem, recv_sem, device):
    return pltpu.make_async_remote_copy(
        src_ref=src,
        dst_ref=dst,
        send_sem=send_sem,
        recv_sem=recv_sem,
        device_id=device,
        device_id_type=MESH,
    )


def aligned(index, size):
    return pl.ds(pl.multiple_of(index * size, size), size)


class Place:
    def __init__(self, planes):
        self.sp, self.c = lax.axis_index("sp"), lax.axis_index("tp")
        self.planes = planes
        self.z, self.p = lax.div(self.sp, 4), lax.rem(self.sp, 4)
        x, y = lax.rem(self.p, 2), lax.div(self.p, 2)
        self.xn, self.yn, self.dg = self.p + 1 - 2 * x, self.p + 2 - 4 * y, 3 - self.p
        self.mates = (self.xn, self.yn, self.dg)
        self.has_above, self.has_below = self.z < planes - 1, self.z > 0

    def mate(self, p):
        return (self.z * 4 + p, self.c)

    def partner(self):
        return (self.sp, 1 - self.c)

    def above(self):
        return (lax.rem(self.sp + 4, 4 * self.planes), self.c)

    def below(self):
        return (lax.rem(self.sp + 4 * self.planes - 4, 4 * self.planes), self.c)

    def greet(self):
        sem = pltpu.get_barrier_semaphore()
        for p in self.mates:
            pl.semaphore_signal(sem, inc=1, device_id=self.mate(p), device_id_type=MESH)
        pl.semaphore_signal(sem, inc=1, device_id=self.partner(), device_id_type=MESH)

        @pl.when(self.has_above)
        def _():
            pl.semaphore_signal(sem, inc=1, device_id=self.above(), device_id_type=MESH)

        @pl.when(self.has_below)
        def _():
            pl.semaphore_signal(sem, inc=1, device_id=self.below(), device_id_type=MESH)

    def barrier(self):
        sem = pltpu.get_barrier_semaphore()
        inner = self.has_above & self.has_below

        @pl.when(inner)
        def _():
            pl.semaphore_wait(sem, 6)

        @pl.when(jnp.logical_not(inner))
        def _():
            pl.semaphore_wait(sem, 5)


class Rows:
    def __init__(self, at, own, held, sems):
        self.at, self.own, self.held = at, own, held
        self.local_sem, self.near, self.recv, self.up, self.down = sems

    def slot(self, plane, p, cut=None):
        if cut is None:
            return self.held.at[plane, p]
        return self.held.at[plane, p, cut[0], cut[1]]

    def to_mate(self, index, p, ready):
        at = self.at
        return [
            remote(
                src,
                self.slot(at.z, at.p, cut),
                self.near.at[index],
                self.recv.at[at.z, at.p],
                at.mate(p),
            )
            for src, cut, copied in self.own(p)
            if copied == ready
        ]

    def here(self):
        at = self.at
        return [
            pltpu.make_async_copy(src, self.slot(at.z, at.p, cut), self.local_sem.at[k])
            for k, (src, cut, copied) in enumerate(self.own(at.p))
            if copied
        ]

    def hop(self, plane, p, upward, src=None, cut=None):
        at = self.at
        dst = self.slot(plane, p, cut)
        return remote(
            dst if src is None else src,
            dst,
            (self.up if upward else self.down).at[plane, p],
            self.recv.at[plane, p],
            at.above() if upward else at.below(),
        )

    def send(self, plane, p, upward):
        @pl.when(self.at.has_above if upward else self.at.has_below)
        def _():
            self.hop(plane, p, upward).start()

    def begin_far(self, ready=True):
        at = self.at
        for upward in (True, False):

            @pl.when(at.has_above if upward else at.has_below)
            def _():
                for src, cut, copied in self.own(at.p):
                    if copied == ready:
                        self.hop(at.z, at.p, upward, src, cut).start()

    def begin_near(self, index, ready=True):
        for copy in self.to_mate(index, self.at.mates[index], ready):
            copy.start()

    def begin_here(self):
        for copy in self.here():
            copy.start()

    def arrived(self, plane, p):
        self.hop(plane, p, True).wait_recv()

    def pass_near(self):
        at = self.at
        for p in at.mates:
            self.arrived(at.z, p)
            self.send(at.z, p, True)
            self.send(at.z, p, False)

    def pass_far(self, distance, index):
        at = self.at
        p = ((at.p,) + at.mates)[index]
        low, high = at.z - distance, at.z + distance

        @pl.when(low >= 0)
        def _():
            self.arrived(low, p)
            self.send(low, p, True)

        @pl.when(high < at.planes)
        def _():
            self.arrived(high, p)
            self.send(high, p, False)

    def finish(self):
        at = self.at
        whole = self.slot(at.z, at.p)
        for index, p in enumerate(at.mates):
            remote(
                whole, whole, self.near.at[index], self.recv.at[at.z, at.p], at.mate(p)
            ).wait_send()
        for plane in range(at.planes):
            for p in range(4):

                @pl.when(at.has_above & (at.z >= plane))
                def _():
                    self.hop(plane, p, True).wait_send()

                @pl.when(at.has_below & (at.z <= plane))
                def _():
                    self.hop(plane, p, False).wait_send()


def layer_kernel(planes, head, *refs):
    (tok, w_query, w_pool, w_attn, w_mixed, sinks) = refs[:6]
    given, out = refs[6:13], refs[13]
    (raw, xs, ws, kvw, acc, q, kv, pool, ma, ws_out, ys) = refs[14:25]
    held_inputs, load_sems = refs[-8:-1], refs[-1]
    in_sems, out_sems = refs[25:30], refs[30:35]
    (raw_sems, t_send, t_recv, td_send, td_recv, h_send, h_recv) = refs[35:42]
    (m_send, m_recv, f_send, f_recv, d_send, d_recv, r_send, r_recv, r_local) = refs[42:-8]

    loads = [
        pltpu.make_async_copy(src, dst, load_sems.at[k])
        for k, (src, dst) in enumerate(zip(given, held_inputs))
    ]
    for load in loads:
        load.start()
    w_key, w_value, gain, query_gain, key_gain, pool_scale, mix = held_inputs
    at = Place(planes)
    at.greet()
    c, p, z = at.c, at.p, at.z
    pair = 2 * head
    count, half = tok.shape
    part = count // 2
    deep = xs.shape[3]
    blocks = half // deep
    width, channels = q.shape[1], pool.shape[1]
    steps, tall, wide = ma.shape[1:]
    block = tall // 4
    columns = ws_out.shape[3]
    lag_rows = pool.shape[0] - 4 * count

    every = pl.ds(0, w_query.shape[0])

    def own_in(place):
        return [
            (w_query.at[:, aligned(place, width)], (every, pl.ds(0, width)), True),
            (kvw.at[place], (every, pl.ds(width, pair)), False),
            (w_pool.at[:, aligned(place, channels)], (every, pl.ds(width + pair, channels)), True),
        ]

    def own_out(place):
        rows = w_attn.shape[0]
        return [
            (w_attn.at[:, aligned(place, columns)], (pl.ds(0, rows), pl.ds(0, columns)), True),
            (w_mixed.at[:, aligned(place, columns)], (pl.ds(rows, rows), pl.ds(0, columns)), True),
        ]

    rows_in = Rows(at, own_in, ws, in_sems)
    rows_out = Rows(at, own_out, ws_out, out_sems)

    at.barrier()
    raw_local = pltpu.make_async_copy(tok, raw.at[c], raw_sems.at[0])
    raw_away = remote(tok, raw.at[c], raw_sems.at[1], raw_sems.at[2], at.partner())
    raw_away.start()
    raw_local.start()
    rows_in.begin_far()
    rows_in.begin_near(0)
    rows_in.begin_near(1)
    for load in loads:
        load.wait()
    low_lane = lax.broadcasted_iota(jnp.int32, (w_key.shape[0], pair), 1) < head
    for k in range(4):
        tile = slice(k // 2 * pair, (k // 2 + 1) * pair)
        key_tile, value_tile = w_key[:, tile], w_value[:, tile]
        if k % 2:
            key_tile = pltpu.roll(key_tile.astype(jnp.float32), head, 1).astype(jnp.bfloat16)
        else:
            value_tile = pltpu.roll(value_tile.astype(jnp.float32), head, 1).astype(jnp.bfloat16)
        kvw[k] = jnp.where(low_lane, key_tile, value_tile)
    ws[z, p, :, width : width + pair] = kvw[p]
    rows_in.begin_far(False)
    rows_in.begin_near(0, False)
    rows_in.begin_near(1, False)
    for ready in (True, False):
        rows_in.begin_near(2, ready)
    rows_in.begin_here()
    raw_local.wait()
    raw_away.wait_recv()

    norm_rows = 32

    def norm_step(index, carry):
        span = aligned(index, norm_rows)
        halves = [raw[k, span, :].astype(jnp.float32) for k in range(2)]
        total = sum(jnp.sum(v * v, axis=-1, keepdims=True) for v in halves)
        scale = lax.rsqrt(total / (2 * half) + epsilon)
        for k in range(2):
            normed = halves[k] * scale * gain[:, k * half : (k + 1) * half]
            normed = normed.astype(jnp.bfloat16)
            for b in range(blocks):
                xs[p, k * blocks + b, span, :] = normed[:, b * deep : (b + 1) * deep]
        return carry

    lax.fori_loop(0, count // norm_rows, norm_step, 0)

    def piece(place, h, core):
        return xs.at[place, pl.ds(core * blocks, blocks), pl.ds(h * part, part), :]

    def tokens_to(index, place, h, to):
        ref = piece(place, h, c)
        return remote(ref, ref, t_send.at[index], t_recv.at[place, h], at.mate(to))

    def tokens_over(index, place, h, core):
        ref = piece(place, h, core)
        return remote(ref, ref, td_send.at[index], td_recv.at[place, h], at.partner())

    sent = [(p, 0, at.xn), (p, 1, at.yn), (p, 1, at.xn), (p, 0, at.yn)]
    sent += [(at.xn, 0, at.yn), (at.yn, 1, at.xn)]
    crossed = [(at.xn, 0), (at.yn, 1), (at.xn, 1), (at.yn, 0), (at.dg, 0), (at.dg, 1)]
    for index in range(4):
        tokens_to(index, *sent[index]).start()
    rows_in.pass_near()

    def take_tokens(index, onward=None):
        place, h = crossed[index]
        tokens_to(0, place, h, at.xn).wait_recv()
        if onward is not None:
            tokens_to(onward, *sent[onward]).start()
        tokens_over(index, place, h, c).start()

    def first_tokens():
        take_tokens(0, 4)
        take_tokens(1, 5)

    def second_tokens():
        take_tokens(2)
        take_tokens(3)
        rows_out.begin_far()
        for index in range(3):
            rows_out.begin_near(index)
        rows_out.begin_here()
        for place, h in crossed[:4]:
            tokens_over(0, place, h, 1 - c).wait_recv()

    def product(place, b, span, slots):
        if slots is None:
            return jnp.dot(
                xs[place, b, span, :],
                ws[b].reshape(deep, ws.shape[3]),
                preferred_element_type=jnp.float32,
            )
        total = None
        for source in slots:
            term = jnp.dot(
                xs[place, b, span, aligned(source, deep // 4)],
                ws[b, source],
                preferred_element_type=jnp.float32,
            )
            total = term if total is None else total + term
        return total

    def place_of(k):
        return jnp.where(k == 0, p, jnp.where(k == 1, at.xn, jnp.where(k == 2, at.yn, at.dg)))

    def accumulate(b, places, slots=None, fresh=False, halves=(0, 2)):
        tall_count = halves[1] - halves[0]

        def one(index, carry):
            k = places[0] + lax.div(index, tall_count)
            span = aligned(halves[0] + lax.rem(index, tall_count), part)
            term = product(place_of(k), b, span, slots)
            acc[k, span, :] = term if fresh else acc[k, span, :] + term
            return carry

        lax.fori_loop(0, tall_count * (places[1] - places[0]), one, 0)

    mine, sides, near, everywhere = (0, 1), (1, 3), (0, 3), (0, 4)
    early, late = (p, at.xn, at.yn), (at.dg,)

    def far_unit(distance, places, slots=None, halves=(0, 2)):
        for b in (z - distance, z + distance):

            @pl.when((b >= 0) & (b < planes))
            def _():
                accumulate(b, places, slots, False, halves)

    def across(h):
        span = aligned(h, part)

        def whole(first, last, partial):
            total = None if partial is None else product(at.dg, partial, span, early)
            for b in range(first, last):
                term = product(at.dg, b, span, None)
                total = term if total is None else total + term
            acc[3, span, :] = total

        @pl.when(at.has_above & at.has_below)
        def _():
            whole(0, planes, None)

        @pl.when(jnp.logical_not(at.has_below))
        def _():
            whole(0, planes - 1, planes - 1)

        @pl.when(jnp.logical_not(at.has_above))
        def _():
            whole(1, planes, 0)

    def last_tokens():
        take_tokens(5)
        take_tokens(4)

    def last_crossed(h):
        tokens_over(0, at.dg, h, 1 - c).wait_recv()

    def start_mine():
        for copy in rows_in.here():
            copy.wait()
        accumulate(z, mine, fresh=True)

    def one_half(h, wait):
        if wait:
            last_tokens()
        far_unit(planes - 1, near, early, (h, h + 1))
        last_crossed(h)
        across(h)
        if wait:
            rows_in.pass_far(planes - 1, 3)
        far_unit(planes - 1, everywhere, late, (h, h + 1))
        settle_half(h)

    final = 4 * (planes - 1) - 1
    events = {}

    def plan(step, event):
        events.setdefault(min(step, final - 1), []).append(event)

    plan(4 * planes // 3 - 1, start_mine)
    plan(4 * planes // 3, first_tokens)
    for distance in range(1, planes - 1):
        plan(max(4 * planes // 3, 4 * distance - 1), functools.partial(far_unit, distance, mine))
    plan(2 * planes - 1, second_tokens)
    plan(2 * planes - 1, lambda: accumulate(z, sides, fresh=True))
    for distance in range(1, planes - 1):
        turn = max(2 * planes - 2 + distance, 4 * distance - 1)
        plan(turn, functools.partial(far_unit, distance, sides))
    for at_step in range(final):
        rows_in.pass_far(at_step // 4 + 1, at_step % 4)
        for event in events.get(at_step, []):
            event()

    low_part = lax.broadcasted_iota(jnp.int32, (part, pair), 1) < head
    query_pair = jnp.concatenate([query_gain[...]] * 2, axis=1)
    key_pair = jnp.concatenate([key_gain[...]] * 2, axis=1)

    def settle(total, place, h):
        span = aligned(place * 2 + h, part)
        for k in range(width // pair):
            v = total[:, pair * k : pair * (k + 1)]
            square = v * v
            lo = jnp.sum(jnp.where(low_part, square, 0.0), axis=-1, keepdims=True) / head
            hi = jnp.sum(jnp.where(low_part, 0.0, square), axis=-1, keepdims=True) / head
            scale = jnp.where(low_part, lax.rsqrt(lo + epsilon), lax.rsqrt(hi + epsilon))
            q[span, pair * k : pair * (k + 1)] = (v * scale * query_pair).astype(jnp.bfloat16)
        v = total[:, width : width + pair]
        lo = jnp.sum(jnp.where(low_part, v * v, 0.0), axis=-1, keepdims=True) / head
        both = jnp.where(low_part, v * lax.rsqrt(lo + epsilon) * key_pair, v)
        base = pl.multiple_of((place * 2 + h) * part, part)
        kv[pl.ds(base + block, part), :pair] = both.astype(jnp.bfloat16)
        kv[pl.ds(base + block, part), pair:] = pltpu.roll(both, head, 1).astype(jnp.bfloat16)
        pool[pl.ds(base + lag_rows, part), :] = total[:, width + pair :].astype(jnp.bfloat16)

    def settle_half(h):
        def one(k, carry):
            settle(acc[k, aligned(h, part), :], place_of(k), h)
            return carry

        lax.fori_loop(0, 4, one, 0)

    one_half(1, True)

    def halo(k):
        ref, rows = ((kv, block), (pool, lag_rows))[k]
        src, dst = ref.at[pl.ds(4 * count, rows), :], ref.at[pl.ds(0, rows), :]
        return remote(src, dst, h_send.at[k], h_recv.at[k], at.above())

    @pl.when(at.has_above)
    def _():
        halo(0).start()
        halo(1).start()

    @pl.when(z == 0)
    def _():
        kv[0:block, :] = jnp.zeros((block, kv.shape[1]), jnp.bfloat16)
        pool[0:lag_rows, :] = jnp.zeros((lag_rows, channels), jnp.bfloat16)

    heads = width // head
    pairs = heads // 2
    query = lax.rem(lax.broadcasted_iota(jnp.int32, (pairs * block, block), 0), block)
    key = lax.broadcasted_iota(jnp.int32, (pairs * block, block), 1)
    current = key <= query
    low_keys = lax.broadcasted_iota(jnp.int32, (2 * block, pair), 1) < head
    log2_e = 1.4426950408889634
    line = lax.broadcasted_iota(jnp.int32, (block, 1), 0)
    window = lax.shift_left(jnp.int32(2), p).astype(jnp.float32)
    slot = c * 4 + p

    def mixers(j, place):
        index = place * steps + j
        base = pl.multiple_of(index * block, block)
        first = index == 0
        kvs = kv[pl.ds(base, 2 * block), :]
        straight, turned = kvs[:, :pair], kvs[:, pair:]
        zero = jnp.zeros_like(straight)
        keys = (jnp.where(low_keys, straight, zero), jnp.where(low_keys, zero, turned))
        values = (jnp.where(low_keys, turned, zero), jnp.where(low_keys, zero, straight))
        absent = jnp.where((z == 0) & first, NEGATIVE, 0.0)
        span = aligned(place, block)
        q_pairs = [q[pl.ds(base, block), pair * k : pair * (k + 1)] for k in range(pairs)]
        q_stack = jnp.concatenate(q_pairs, axis=0)
        total = None
        for side in range(2):
            sink = jnp.concatenate(
                [
                    jnp.full((block, block), sinks[p * heads + 2 * k + side] * log2_e)
                    for k in range(pairs)
                ],
                axis=0,
            )
            scores = lax.dot_general(
                q_stack,
                keys[side],
                (((1,), (1,)), ((), ())),
                preferred_element_type=jnp.float32,
            )
            scores = jnp.where(current, scores[:, block:], scores[:, :block] + absent)
            scores = scores * (head ** (-0.5) * log2_e)
            top = jnp.maximum(jnp.max(scores, axis=-1, keepdims=True), sink)
            lifted = jnp.exp2(scores - top)
            under = jnp.sum(lifted, axis=-1, keepdims=True) + jnp.exp2(sink - top)
            weights = lifted * (1.0 / under)
            weights = jnp.concatenate(
                [jnp.where(current, 0.0, weights), jnp.where(current, weights, 0.0)], axis=1
            ).astype(jnp.bfloat16)
            term = jnp.dot(weights, values[side], preferred_element_type=jnp.float32)
            total = term if total is None else total + term
        for k in range(pairs):
            ma[slot, j, span, 2 * pair * k : 2 * pair * k + pair] = total[
                block * k : block * (k + 1)
            ].astype(jnp.bfloat16)
        series = pool[pl.ds(base, lag_rows + block), :].astype(jnp.float32)
        sums, lag = [series], 1
        while 2 * lag <= lag_rows:
            sums.append(sums[-1] + pltpu.roll(sums[-1], lag, 0))
            lag *= 2
        window_sum = sums[-1]
        for k in range(len(sums) - 2, 0, -1):
            window_sum = jnp.where(p == k - 1, sums[k], window_sum)
        position = (z * 4 * count + base + 1 + line).astype(jnp.float32)
        share = 1.0 / jnp.minimum(position, window)
        contrast = window_sum[lag_rows:] * share - series[lag_rows:]
        mixed = jnp.dot(contrast.astype(jnp.bfloat16), mix[p], preferred_element_type=jnp.float32)
        mixed = (mixed * pool_scale[:, aligned(p, channels)]).astype(jnp.bfloat16)
        for k in range(channels // pair):
            ma[slot, j, span, (2 * k + 1) * pair : (2 * k + 2) * pair] = mixed[
                :, pair * k : pair * (k + 1)
            ]

    def half_of(core, place, j, k):
        return ma.at[core * 4 + place, j, aligned(k, tall // 2), :]

    def to_mate(index, j, k, to):
        ref = half_of(c, p, j, k)
        return remote(ref, ref, m_send.at[index, j, k], m_recv.at[p, j, k], at.mate(to))

    def onward(k, j, place, to):
        ref = half_of(c, place, j, k)
        return remote(ref, ref, f_send.at[k, j], f_recv.at[k, j], at.mate(to))

    def over(index, j, place, core):
        ref = ma.at[core * 4 + place, j]
        return remote(ref, ref, d_send.at[index, j], d_recv.at[place, j], at.partner())

    def came(place, j, k):
        ref = half_of(c, place, j, k)
        remote(ref, ref, m_send.at[0, j, k], m_recv.at[place, j, k], at.partner()).wait_recv()

    def mix_step(index, carry):
        j = steps - 1 - index

        @pl.when(index == 1)
        def _():
            one_half(0, False)

        @pl.when((j == 0) & at.has_below)
        def _():
            halo(0).wait_recv()
            halo(1).wait_recv()

        def two(turn, inner):
            mixers(j, 2 * turn)
            mixers(j, 2 * turn + 1)
            for index, to in enumerate((at.xn, at.yn)):
                to_mate(index, j, turn, to).start()
            return inner

        lax.fori_loop(0, 2, two, 0)
        over(0, j, p, c).start()

        @pl.when(index == 0)
        def _():
            rows_out.pass_near()

        return carry

    lax.fori_loop(0, steps, mix_step, 0)

    def pass_on(j):
        came(at.xn, j, 0)
        onward(0, j, at.xn, at.yn).start()
        came(at.yn, j, 0)
        came(at.yn, j, 1)
        onward(1, j, at.yn, at.xn).start()
        over(2, j, at.yn, c).start()
        came(at.xn, j, 1)
        over(1, j, at.xn, c).start()

    waiting = list(range(steps - 1, -1, -1))
    total_far = 4 * (planes - 1)
    for at_step in range(total_far):
        rows_out.pass_far(at_step // 4 + 1, at_step % 4)
        passed = steps - len(waiting)
        while waiting and at_step + 1 >= (passed + 1) * total_far // (steps + 1):
            pass_on(waiting.pop(0))
            passed += 1
    for j in waiting:
        pass_on(j)
    for copy in rows_out.here():
        copy.wait()

    def landing(j, place):
        return out.at[aligned(j, block), aligned(place, columns)]

    def result(index, j, to):
        return remote(
            ys.at[j, aligned(to, block), :],
            landing(j, p),
            r_send.at[index, j],
            r_recv.at[p, j],
            at.mate(to),
        )

    def result_here(j):
        return pltpu.make_async_copy(ys.at[j, aligned(p, block), :], landing(j, p), r_local.at[j])

    def last_step(index, carry):
        j = steps - 1 - index
        for k in range(2):
            onward(k, j, at.dg, at.xn).wait_recv()
        over(3, j, at.dg, c).start()
        for place in range(4):
            over(0, j, place, 1 - c).wait_recv()
        total = None
        for i in range(8):
            first = 2 * i
            weight = ws_out[first // 4, first % 4 : first % 4 + 2].reshape(wide, columns)
            term = jnp.dot(ma[i, j], weight, preferred_element_type=jnp.float32)
            total = term if total is None else total + term
        ys[j] = total.astype(jnp.bfloat16)
        for k, to in enumerate(at.mates):
            result(k, j, to).start()
        result_here(j).start()
        return carry

    lax.fori_loop(0, steps, last_step, 0)

    def finish_step(j, carry):
        for k, to in enumerate(at.mates):
            remote(
                ys.at[j, pl.ds(0, block), :],
                landing(j, to),
                r_send.at[k, j],
                r_recv.at[to, j],
                at.mate(to),
            ).wait_recv()
        result_here(j).wait()
        for k, to in enumerate(at.mates):
            result(k, j, to).wait_send()
        for k in range(2):
            to_mate(0, j, k, at.xn).wait_send()
            to_mate(1, j, k, at.yn).wait_send()
        onward(0, j, at.xn, at.yn).wait_send()
        onward(1, j, at.yn, at.xn).wait_send()
        for k, place in enumerate((p,) + at.mates):
            over(k, j, place, c).wait_send()
        return carry

    lax.fori_loop(0, steps, finish_step, 0)
    raw_away.wait_send()
    for index in range(6):
        tokens_to(index, *sent[index]).wait_send()
        tokens_over(index, *crossed[index], c).wait_send()

    @pl.when(at.has_above)
    def _():
        halo(0).wait_send()
        halo(1).wait_send()

    rows_in.finish()
    rows_out.finish()


def copy_kernel(src, dst, held, in_sems, out_sems):
    count = held.shape[0] // in_sems.shape[0]
    parts = [pl.ds(k * count, count) for k in range(in_sems.shape[0])]
    taken = [pltpu.make_async_copy(src.at[r], held.at[r], in_sems.at[k]) for k, r in enumerate(parts)]
    given = [pltpu.make_async_copy(held.at[r], dst.at[r], out_sems.at[k]) for k, r in enumerate(parts)]
    for copy in taken:
        copy.start()
    for take, give in zip(taken, given):
        take.wait()
        give.start()
    for copy in given:
        copy.wait()


def per_device_planes(
    tokens,
    norm_gain,
    w_query,
    w_key,
    w_value,
    w_pool_in,
    query_gain,
    key_gain,
    sinks,
    w_mix,
    pool_scale,
    w_out_attn,
    w_out_pool,
):
    planes = lax.axis_size("sp") // 4
    head = query_gain.shape[0]
    count, half = tokens.shape
    in_rows, out_rows = w_query.shape[0], 2 * w_out_attn.shape[0]
    width, channels = w_query.shape[1] // 4, w_pool_in.shape[1] // 4
    columns = w_out_attn.shape[1] // 4
    pair, deep, steps = 2 * head, 4 * in_rows, count // WINDOW
    in_width = width + pair + channels
    lines = [a.reshape(1, -1) for a in (norm_gain, query_gain, key_gain, pool_scale)]
    given = (w_key, w_value, *lines, w_mix)
    anywhere = pl.BlockSpec(memory_space=pl.ANY)
    smem = pl.BlockSpec(memory_space=pltpu.SMEM)
    dma = pltpu.SemaphoreType.DMA

    def held(*shape):
        return pltpu.VMEM(shape, jnp.bfloat16)

    row_sems = [dma((3,)), dma((3,)), dma((planes, 4)), dma((planes, 4)), dma((planes, 4))]
    result = pl.pallas_call(
        functools.partial(layer_kernel, planes, head),
        out_shape=jax.ShapeDtypeStruct(tokens.shape, jnp.bfloat16),
        in_specs=[anywhere] * 5 + [smem] + [anywhere] * 7,
        out_specs=anywhere,
        scratch_shapes=[
            held(2, count, half),
            held(4, planes, count, deep),
            held(planes, 4, in_rows, in_width),
            held(4, in_rows, pair),
            pltpu.VMEM((4, count, in_width), jnp.float32),
            held(4 * count, width),
            held(4 * count + WINDOW, 2 * pair),
            held(4 * count + longest_lag + 1, channels),
            held(8, steps, 4 * WINDOW, width + channels),
            held(planes, 4, out_rows, columns),
            held(steps, 4 * WINDOW, columns),
        ]
        + row_sems
        + row_sems
        + [dma((3,)), dma((6,)), dma((4, 2)), dma((6,)), dma((4, 2)), dma((2,)), dma((2,))]
        + [dma((2, steps, 2)), dma((4, steps, 2)), dma((2, steps)), dma((2, steps))]
        + [dma((4, steps)), dma((4, steps)), dma((3, steps)), dma((4, steps)), dma((steps,))]
        + [pltpu.VMEM(a.shape, a.dtype) for a in given]
        + [dma((len(given),))],
        compiler_params=pltpu.CompilerParams(
            collective_id=0, has_side_effects=True, vmem_limit_bytes=63 * 2**20
        ),
        name="layer",
    )(tokens, w_query, w_pool_in, w_out_attn, w_out_pool, sinks, *given)
    return pl.pallas_call(
        copy_kernel,
        out_shape=jax.ShapeDtypeStruct(tokens.shape, jnp.bfloat16),
        in_specs=[anywhere],
        out_specs=anywhere,
        scratch_shapes=[held(*tokens.shape), dma((8,)), dma((8,))],
        compiler_params=pltpu.CompilerParams(vmem_limit_bytes=63 * 2**20),
        name="hand_over",
    )(result)


def suits_planes(mesh, args):
    sp, tp = mesh.shape["sp"], mesh.shape["tp"]
    tokens, w_query, w_key, w_pool_in = args[0], args[2], args[3], args[5]
    head, groups = args[6].shape[0], args[9].shape[0]
    w_out_attn, w_out_pool = args[11], args[12]
    if tp != 2 or sp % 4 or sp < 12 or 2 * head != 128:
        return False
    share = 4 * tp
    rows = tokens.shape[0] // sp
    width, channels = w_query.shape[1] // share, w_pool_in.shape[1] // share
    held = 2 * 4 * rows * tokens.shape[1] + 2 * w_query.shape[0] * (width + 128 + channels)
    return (
        w_key.shape[1] == share * head
        and groups == share
        and rows % (4 * WINDOW) == 0
        and width % 128 == 0
        and width == channels
        and 2 * w_out_attn.shape[0] // sp == width
        and 2 * w_out_pool.shape[0] // sp == channels
        and w_out_attn.shape[0] // sp == 2 * head
        and w_query.shape[0] // sp % 16 == 0
        and w_out_attn.shape[1] % (share * 128) == 0
        and held < 22 * 2**20
    )


def solution(mesh):
    sp, tp = mesh.shape["sp"], mesh.shape["tp"]

    def call(*args):
        if suits_planes(mesh, args):
            return jax.shard_map(
                per_device_planes,
                mesh=mesh,
                in_specs=(
                    P("sp", "tp"),
                    P(),
                    P("sp", "tp"),
                    P("sp", "tp"),
                    P("sp", "tp"),
                    P("sp", "tp"),
                    P(),
                    P(),
                    P("tp"),
                    P("tp", None, None),
                    P("tp"),
                    P("sp", "tp"),
                    P("sp", "tp"),
                ),
                out_specs=P("sp", "tp"),
                check_vma=False,
            )(*args)
        kv_local = args[3].shape[1] // args[6].shape[0] // tp
        groups_local = args[9].shape[0] // tp
        fits = sp % 2 == 0 and kv_local % 2 == 0 and groups_local % 2 == 0
        pair = 2 if fits else 1
        inner = Mesh(mesh.devices.reshape(sp // pair, pair, tp), ("so", "si", "tp"))
        rows = ("so", "si")
        return jax.shard_map(
            per_device,
            mesh=inner,
            in_specs=(
                P(rows, "tp"),
                P(),
                P(rows, "tp"),
                P(rows, "tp"),
                P(rows, "tp"),
                P(rows, "tp"),
                P(),
                P(),
                P("tp"),
                P("tp", None, None),
                P("tp"),
                P(rows, "tp"),
                P(rows, "tp"),
            ),
            out_specs=P(rows, "tp"),
            check_vma=False,
        )(*args)

    return call
```

```python
import functools

import jax
import jax.numpy as jnp
from jax import lax
from jax.experimental import pallas as pl
from jax.experimental.pallas import tpu as pltpu
from jax.sharding import Mesh
from jax.sharding import PartitionSpec as P

WINDOW = 128


epsilon = 1e-06
longest_lag = 15


def from_behind(block, axis):
    devices = range(lax.axis_size(axis))
    route = [(i - 1, i) for i in devices if i - 1 in devices]
    return lax.ppermute(block, axis, route)


def swap(block, axis):
    count = lax.axis_size(axis)
    return lax.ppermute(block, axis, [(i, count - 1 - i) for i in range(count)])


def row_norm(values, gain):
    return values * lax.rsqrt(jnp.mean(values * values, axis=-1, keepdims=True) + epsilon) * gain


def after(value, *others):
    return lax.optimization_barrier((value,) + others)[0]


def ordered(mine, theirs, index, dim):
    return jnp.where(
        index == 0,
        jnp.concatenate([mine, theirs], axis=dim),
        jnp.concatenate([theirs, mine], axis=dim),
    )


def both_cores(block, dim):
    if lax.axis_size("tp") == 2:
        return ordered(block, swap(block, "tp"), lax.axis_index("tp"), dim)
    return lax.all_gather(block, "tp", axis=dim, tiled=True)


def per_device(
    tokens,
    norm_gain,
    w_query,
    w_key,
    w_value,
    w_pool_in,
    query_gain,
    key_gain,
    sinks,
    w_mix,
    pool_scale,
    w_out_attn,
    w_out_pool,
):
    pair = lax.axis_size("si")
    place = lax.axis_index("si")
    outer = lax.axis_index("so")

    def share(array, owner, dim):
        size = array.shape[dim] // pair
        return lax.dynamic_slice_in_dim(array, owner * size, size, dim)

    def mine(arrays):
        return [share(a, place, 1) for a in arrays]

    def other(arrays):
        return [share(a, pair - 1 - place, 1) for a in arrays]

    def joined(own, came, dim):
        return own if pair == 1 else ordered(own, came, place, dim)

    def gathered(rows):
        return lax.all_gather(rows, "so", axis=0, tiled=True)

    qkv_parts = (w_query, w_key, w_value)
    qkv_own = jnp.concatenate(mine(qkv_parts), axis=1)
    if pair == 1:
        qkv_rows, pool_rows, attn_rows, mixed_rows = qkv_own, w_pool_in, w_out_attn, w_out_pool
        row_half = tokens
    else:
        qkv_came = swap(jnp.concatenate(other(qkv_parts), axis=1), "si")
        qkv_rows = joined(qkv_own, qkv_came, 0)
        late = lax.optimization_barrier((w_pool_in, w_out_attn, w_out_pool, qkv_came))[:3]
        came = [swap(share(w, pair - 1 - place, 1), "si") for w in late]
        pool_rows, attn_rows, mixed_rows = [
            joined(share(w, place, 1), c, 0) for w, c in zip((w_pool_in, w_out_attn, w_out_pool), came)
        ]
        row_half = joined(tokens, swap(after(tokens, qkv_came), "si"), 0)
    w_qkv = gathered(qkv_rows)
    w_pool = gathered(after(pool_rows, w_qkv))
    w_attn = gathered(after(attn_rows, w_pool))
    w_mixed = gathered(after(mixed_rows, w_attn))

    whole = both_cores(row_half, 1)
    row_count = whole.shape[0]
    normed = row_norm(whole.astype(jnp.float32), norm_gain).astype(jnp.bfloat16)
    qkv_raw = jnp.dot(normed, w_qkv, preferred_element_type=jnp.float32)
    head_size = query_gain.shape[0]
    query_width = w_query.shape[1] // pair
    kv_width = w_key.shape[1] // pair
    query_heads = query_width // head_size
    kv_local = kv_width // head_size
    per_kv = query_heads // kv_local
    query_raw = qkv_raw[:, :query_width]
    key_raw = qkv_raw[:, query_width : query_width + kv_width]
    value_raw = qkv_raw[:, query_width + kv_width :]
    queries = row_norm(query_raw.reshape(row_count, query_heads, head_size), query_gain).astype(
        jnp.bfloat16
    )
    key_rows = row_norm(key_raw.reshape(row_count, kv_local, head_size), key_gain).astype(
        jnp.bfloat16
    )
    values = value_raw.astype(jnp.bfloat16).reshape(row_count, kv_local, head_size)
    kv_tail = jnp.concatenate(
        [key_rows[-WINDOW:].reshape(WINDOW, -1), values[-WINDOW:].reshape(WINDOW, -1)], axis=1
    )
    kv_prev = from_behind(kv_tail, "so").reshape(WINDOW, 2, kv_local, head_size)
    offset = outer * row_count
    blocks = row_count // WINDOW

    def banded(previous, source):
        earlier = jnp.concatenate([previous, source[: row_count - WINDOW]], axis=0).reshape(
            blocks, WINDOW, kv_local, head_size
        )
        return jnp.concatenate(
            [earlier, source.reshape(blocks, WINDOW, kv_local, head_size)], axis=1
        )

    band_keys = banded(kv_prev[:, 0], key_rows)
    band_values = banded(kv_prev[:, 1], values)
    query_blocks = queries.reshape(blocks, WINDOW, kv_local, per_kv, head_size)
    scores = jnp.einsum(
        "bqkgd,bjkd->bkgqj", query_blocks, band_keys, preferred_element_type=jnp.float32
    ) * head_size ** (-0.5)
    query_index = jnp.arange(WINDOW)[:, None]
    key_index = jnp.arange(2 * WINDOW)[None, :]
    distance = query_index + WINDOW - key_index
    key_pos = offset + jnp.arange(blocks)[:, None, None] * WINDOW - WINDOW + key_index[None]
    valid = (distance[None] >= 0) & (distance[None] < WINDOW) & (key_pos >= 0)
    sink_logit = share(sinks, place, 0).reshape(kv_local, per_kv)[None, :, :, None, None]
    scores = jnp.where(valid[:, None, None], scores, -1e30)
    row_top = jnp.maximum(scores.max(axis=-1, keepdims=True), sink_logit)
    lifted = jnp.exp(scores - row_top)
    weights = (
        lifted / (lifted.sum(axis=-1, keepdims=True) + jnp.exp(sink_logit - row_top))
    ).astype(jnp.bfloat16)
    attended = (
        jnp.einsum("bkgqj,bjkd->bqkgd", weights, band_values, preferred_element_type=jnp.float32)
        .astype(jnp.bfloat16)
        .reshape(row_count, query_heads * head_size)
    )

    def all_heads(block):
        if pair == 2:
            block = joined(block, swap(block, "si"), 1)
        return both_cores(block, 1)

    attended_all = all_heads(attended)

    pool_in = jnp.dot(normed, w_pool, preferred_element_type=jnp.float32).astype(jnp.bfloat16)
    pool_prev = from_behind(pool_in[-longest_lag:], "so")
    mix = share(w_mix, place, 0)
    groups_local = mix.shape[0]
    group_dim = mix.shape[1]
    first_group = (lax.axis_index("tp") * pair + place) * groups_local
    group_ids = first_group + jnp.arange(groups_local, dtype=jnp.int32)
    spans = jnp.repeat(jnp.left_shift(jnp.int32(2), group_ids % 4), group_dim)
    extended = jnp.concatenate([pool_prev, pool_in], axis=0).astype(jnp.float32)
    window_sum = jnp.zeros((row_count, spans.shape[0]), jnp.float32)
    for back_step in range(longest_lag + 1):
        shifted = extended[longest_lag - back_step : longest_lag - back_step + row_count]
        window_sum = window_sum + jnp.where(back_step < spans[None, :], shifted, 0.0)
    positions = (offset + jnp.arange(1, row_count + 1, dtype=jnp.int32)).astype(jnp.float32)
    divisor = jnp.minimum(positions[:, None], spans.astype(jnp.float32)[None, :])
    contrast = (window_sum / divisor - extended[longest_lag:]).astype(jnp.bfloat16)
    mixed = jnp.einsum(
        "tgc,gcd->tgd",
        contrast.reshape(row_count, groups_local, group_dim),
        mix,
        preferred_element_type=jnp.float32,
    ).reshape(row_count, -1)
    pooled = (mixed * share(pool_scale, place, 0)).astype(jnp.bfloat16)
    pooled_all = all_heads(pooled)

    def project(owner):
        total = jnp.dot(share(attended_all, owner, 0), w_attn, preferred_element_type=jnp.float32)
        result = total + jnp.dot(
            share(pooled_all, owner, 0), w_mixed, preferred_element_type=jnp.float32
        )
        return result.astype(jnp.bfloat16)

    if pair == 1:
        return project(0)
    away = project(pair - 1 - place)
    came_back = swap(away, "si")
    return joined(project(place), came_back, 1)


MESH = pl.DeviceIdType.MESH
NEGATIVE = -1e30


def remote(src, dst, send_sem, recv_sem, device):
    return pltpu.make_async_remote_copy(
        src_ref=src,
        dst_ref=dst,
        send_sem=send_sem,
        recv_sem=recv_sem,
        device_id=device,
        device_id_type=MESH,
    )


def aligned(index, size):
    return pl.ds(pl.multiple_of(index * size, size), size)


class Place:
    def __init__(self, planes):
        self.sp, self.c = lax.axis_index("sp"), lax.axis_index("tp")
        self.planes = planes
        self.z, self.p = lax.div(self.sp, 4), lax.rem(self.sp, 4)
        x, y = lax.rem(self.p, 2), lax.div(self.p, 2)
        self.xn, self.yn, self.dg = self.p + 1 - 2 * x, self.p + 2 - 4 * y, 3 - self.p
        self.mates = (self.xn, self.yn, self.dg)
        self.has_above, self.has_below = self.z < planes - 1, self.z > 0

    def mate(self, p):
        return (self.z * 4 + p, self.c)

    def partner(self):
        return (self.sp, 1 - self.c)

    def above(self):
        return (lax.rem(self.sp + 4, 4 * self.planes), self.c)

    def below(self):
        return (lax.rem(self.sp + 4 * self.planes - 4, 4 * self.planes), self.c)

    def greet(self):
        sem = pltpu.get_barrier_semaphore()
        for p in self.mates:
            pl.semaphore_signal(sem, inc=1, device_id=self.mate(p), device_id_type=MESH)
        pl.semaphore_signal(sem, inc=1, device_id=self.partner(), device_id_type=MESH)

        @pl.when(self.has_above)
        def _():
            pl.semaphore_signal(sem, inc=1, device_id=self.above(), device_id_type=MESH)

        @pl.when(self.has_below)
        def _():
            pl.semaphore_signal(sem, inc=1, device_id=self.below(), device_id_type=MESH)

    def barrier(self):
        sem = pltpu.get_barrier_semaphore()
        inner = self.has_above & self.has_below

        @pl.when(inner)
        def _():
            pl.semaphore_wait(sem, 6)

        @pl.when(jnp.logical_not(inner))
        def _():
            pl.semaphore_wait(sem, 5)


class Rows:
    def __init__(self, at, own, held, sems):
        self.at, self.own, self.held = at, own, held
        self.local_sem, self.near, self.recv, self.up, self.down = sems

    def slot(self, plane, p, cut=None):
        if cut is None:
            return self.held.at[plane, p]
        return self.held.at[plane, p, cut[0], cut[1]]

    def to_mate(self, index, p, ready):
        at = self.at
        return [
            remote(
                src,
                self.slot(at.z, at.p, cut),
                self.near.at[index],
                self.recv.at[at.z, at.p],
                at.mate(p),
            )
            for src, cut, copied in self.own(p)
            if copied == ready
        ]

    def here(self):
        at = self.at
        return [
            pltpu.make_async_copy(src, self.slot(at.z, at.p, cut), self.local_sem.at[k])
            for k, (src, cut, copied) in enumerate(self.own(at.p))
            if copied
        ]

    def hop(self, plane, p, upward, src=None, cut=None):
        at = self.at
        dst = self.slot(plane, p, cut)
        return remote(
            dst if src is None else src,
            dst,
            (self.up if upward else self.down).at[plane, p],
            self.recv.at[plane, p],
            at.above() if upward else at.below(),
        )

    def send(self, plane, p, upward):
        @pl.when(self.at.has_above if upward else self.at.has_below)
        def _():
            self.hop(plane, p, upward).start()

    def begin_far(self, ready=True):
        at = self.at
        for upward in (True, False):

            @pl.when(at.has_above if upward else at.has_below)
            def _():
                for src, cut, copied in self.own(at.p):
                    if copied == ready:
                        self.hop(at.z, at.p, upward, src, cut).start()

    def begin_near(self, index, ready=True):
        for copy in self.to_mate(index, self.at.mates[index], ready):
            copy.start()

    def begin_here(self):
        for copy in self.here():
            copy.start()

    def arrived(self, plane, p):
        self.hop(plane, p, True).wait_recv()

    def pass_near(self):
        at = self.at
        for p in at.mates:
            self.arrived(at.z, p)
            self.send(at.z, p, True)
            self.send(at.z, p, False)

    def pass_far(self, distance, index):
        at = self.at
        p = ((at.p,) + at.mates)[index]
        low, high = at.z - distance, at.z + distance

        @pl.when(low >= 0)
        def _():
            self.arrived(low, p)
            self.send(low, p, True)

        @pl.when(high < at.planes)
        def _():
            self.arrived(high, p)
            self.send(high, p, False)

    def finish(self):
        at = self.at
        whole = self.slot(at.z, at.p)
        for index, p in enumerate(at.mates):
            remote(
                whole, whole, self.near.at[index], self.recv.at[at.z, at.p], at.mate(p)
            ).wait_send()
        for plane in range(at.planes):
            for p in range(4):

                @pl.when(at.has_above & (at.z >= plane))
                def _():
                    self.hop(plane, p, True).wait_send()

                @pl.when(at.has_below & (at.z <= plane))
                def _():
                    self.hop(plane, p, False).wait_send()


def layer_kernel(planes, head, *refs):
    (tok, w_query, w_pool, w_attn, w_mixed, sinks) = refs[:6]
    given, out = refs[6:13], refs[13]
    (raw, xs, ws, kvw, acc, q, kv, pool, ma, ws_out, ys) = refs[14:25]
    held_inputs, load_sems = refs[-8:-1], refs[-1]
    in_sems, out_sems = refs[25:30], refs[30:35]
    (raw_sems, t_send, t_recv, td_send, td_recv, h_send, h_recv) = refs[35:42]
    (m_send, m_recv, f_send, f_recv, d_send, d_recv, r_send, r_recv, r_local) = refs[42:-8]

    loads = [
        pltpu.make_async_copy(src, dst, load_sems.at[k])
        for k, (src, dst) in enumerate(zip(given, held_inputs))
    ]
    for load in loads:
        load.start()
    w_key, w_value, gain, query_gain, key_gain, pool_scale, mix = held_inputs
    at = Place(planes)
    at.greet()
    c, p, z = at.c, at.p, at.z
    pair = 2 * head
    count, half = tok.shape
    part = count // 2
    deep = xs.shape[3]
    blocks = half // deep
    width, channels = q.shape[1], pool.shape[1]
    steps, tall, wide = ma.shape[1:]
    block = tall // 4
    columns = ws_out.shape[3]
    lag_rows = pool.shape[0] - 4 * count

    every = pl.ds(0, w_query.shape[0])

    def own_in(place):
        return [
            (w_query.at[:, aligned(place, width)], (every, pl.ds(0, width)), True),
            (kvw.at[place], (every, pl.ds(width, pair)), False),
            (w_pool.at[:, aligned(place, channels)], (every, pl.ds(width + pair, channels)), True),
        ]

    def own_out(place):
        rows = w_attn.shape[0]
        return [
            (w_attn.at[:, aligned(place, columns)], (pl.ds(0, rows), pl.ds(0, columns)), True),
            (w_mixed.at[:, aligned(place, columns)], (pl.ds(rows, rows), pl.ds(0, columns)), True),
        ]

    rows_in = Rows(at, own_in, ws, in_sems)
    rows_out = Rows(at, own_out, ws_out, out_sems)

    at.barrier()
    raw_local = pltpu.make_async_copy(tok, raw.at[c], raw_sems.at[0])
    raw_away = remote(tok, raw.at[c], raw_sems.at[1], raw_sems.at[2], at.partner())
    raw_away.start()
    raw_local.start()
    rows_in.begin_far()
    rows_in.begin_near(0)
    rows_in.begin_near(1)
    for load in loads:
        load.wait()
    low_lane = lax.broadcasted_iota(jnp.int32, (w_key.shape[0], pair), 1) < head
    for k in range(4):
        tile = slice(k // 2 * pair, (k // 2 + 1) * pair)
        key_tile, value_tile = w_key[:, tile], w_value[:, tile]
        if k % 2:
            key_tile = pltpu.roll(key_tile.astype(jnp.float32), head, 1).astype(jnp.bfloat16)
        else:
            value_tile = pltpu.roll(value_tile.astype(jnp.float32), head, 1).astype(jnp.bfloat16)
        kvw[k] = jnp.where(low_lane, key_tile, value_tile)
    ws[z, p, :, width : width + pair] = kvw[p]
    rows_in.begin_far(False)
    rows_in.begin_near(0, False)
    rows_in.begin_near(1, False)
    for ready in (True, False):
        rows_in.begin_near(2, ready)
    rows_in.begin_here()
    raw_local.wait()
    raw_away.wait_recv()

    norm_rows = 32

    def norm_step(index, carry):
        span = aligned(index, norm_rows)
        halves = [raw[k, span, :].astype(jnp.float32) for k in range(2)]
        total = sum(jnp.sum(v * v, axis=-1, keepdims=True) for v in halves)
        scale = lax.rsqrt(total / (2 * half) + epsilon)
        for k in range(2):
            normed = halves[k] * scale * gain[:, k * half : (k + 1) * half]
            normed = normed.astype(jnp.bfloat16)
            for b in range(blocks):
                xs[p, k * blocks + b, span, :] = normed[:, b * deep : (b + 1) * deep]
        return carry

    lax.fori_loop(0, count // norm_rows, norm_step, 0)

    def piece(place, h, core):
        return xs.at[place, pl.ds(core * blocks, blocks), pl.ds(h * part, part), :]

    def tokens_to(index, place, h, to):
        ref = piece(place, h, c)
        return remote(ref, ref, t_send.at[index], t_recv.at[place, h], at.mate(to))

    def tokens_over(index, place, h, core):
        ref = piece(place, h, core)
        return remote(ref, ref, td_send.at[index], td_recv.at[place, h], at.partner())

    sent = [(p, 0, at.xn), (p, 1, at.yn), (p, 1, at.xn), (p, 0, at.yn)]
    sent += [(at.xn, 0, at.yn), (at.yn, 1, at.xn)]
    crossed = [(at.xn, 0), (at.yn, 1), (at.xn, 1), (at.yn, 0), (at.dg, 0), (at.dg, 1)]
    for index in range(4):
        tokens_to(index, *sent[index]).start()
    rows_in.pass_near()

    def take_tokens(index, onward=None):
        place, h = crossed[index]
        tokens_to(0, place, h, at.xn).wait_recv()
        if onward is not None:
            tokens_to(onward, *sent[onward]).start()
        tokens_over(index, place, h, c).start()

    def first_tokens():
        take_tokens(0, 4)
        take_tokens(1, 5)

    def second_tokens():
        take_tokens(2)
        take_tokens(3)
        rows_out.begin_far()
        for index in range(3):
            rows_out.begin_near(index)
        rows_out.begin_here()
        for place, h in crossed[:4]:
            tokens_over(0, place, h, 1 - c).wait_recv()

    def product(place, b, span, slots):
        if slots is None:
            return jnp.dot(
                xs[place, b, span, :],
                ws[b].reshape(deep, ws.shape[3]),
                preferred_element_type=jnp.float32,
            )
        total = None
        for source in slots:
            term = jnp.dot(
                xs[place, b, span, aligned(source, deep // 4)],
                ws[b, source],
                preferred_element_type=jnp.float32,
            )
            total = term if total is None else total + term
        return total

    def place_of(k):
        return jnp.where(k == 0, p, jnp.where(k == 1, at.xn, jnp.where(k == 2, at.yn, at.dg)))

    def accumulate(b, places, slots=None, fresh=False, halves=(0, 2)):
        tall_count = halves[1] - halves[0]

        def one(index, carry):
            k = places[0] + lax.div(index, tall_count)
            span = aligned(halves[0] + lax.rem(index, tall_count), part)
            term = product(place_of(k), b, span, slots)
            acc[k, span, :] = term if fresh else acc[k, span, :] + term
            return carry

        lax.fori_loop(0, tall_count * (places[1] - places[0]), one, 0)

    mine, sides, near, everywhere = (0, 1), (1, 3), (0, 3), (0, 4)
    early, late = (p, at.xn, at.yn), (at.dg,)

    def far_unit(distance, places, slots=None, halves=(0, 2)):
        for b in (z - distance, z + distance):

            @pl.when((b >= 0) & (b < planes))
            def _():
                accumulate(b, places, slots, False, halves)

    def across(h):
        span = aligned(h, part)

        def whole(first, last, partial):
            total = None if partial is None else product(at.dg, partial, span, early)
            for b in range(first, last):
                term = product(at.dg, b, span, None)
                total = term if total is None else total + term
            acc[3, span, :] = total

        @pl.when(at.has_above & at.has_below)
        def _():
            whole(0, planes, None)

        @pl.when(jnp.logical_not(at.has_below))
        def _():
            whole(0, planes - 1, planes - 1)

        @pl.when(jnp.logical_not(at.has_above))
        def _():
            whole(1, planes, 0)

    def last_tokens():
        take_tokens(5)
        take_tokens(4)

    def last_crossed(h):
        tokens_over(0, at.dg, h, 1 - c).wait_recv()

    def start_mine():
        for copy in rows_in.here():
            copy.wait()
        accumulate(z, mine, fresh=True)

    def one_half(h, wait):
        if wait:
            last_tokens()
        far_unit(planes - 1, near, early, (h, h + 1))
        last_crossed(h)
        across(h)
        if wait:
            rows_in.pass_far(planes - 1, 3)
        far_unit(planes - 1, everywhere, late, (h, h + 1))
        settle_half(h)

    final = 4 * (planes - 1) - 1
    events = {}

    def plan(step, event):
        events.setdefault(min(step, final - 1), []).append(event)

    plan(4 * planes // 3 - 1, start_mine)
    plan(4 * planes // 3, first_tokens)
    for distance in range(1, planes - 1):
        plan(max(4 * planes // 3, 4 * distance - 1), functools.partial(far_unit, distance, mine))
    plan(2 * planes - 1, second_tokens)
    plan(2 * planes - 1, lambda: accumulate(z, sides, fresh=True))
    for distance in range(1, planes - 1):
        turn = max(2 * planes - 2 + distance, 4 * distance - 1)
        plan(turn, functools.partial(far_unit, distance, sides))
    for at_step in range(final):
        rows_in.pass_far(at_step // 4 + 1, at_step % 4)
        for event in events.get(at_step, []):
            event()

    low_part = lax.broadcasted_iota(jnp.int32, (part, pair), 1) < head
    query_pair = jnp.concatenate([query_gain[...]] * 2, axis=1)
    key_pair = jnp.concatenate([key_gain[...]] * 2, axis=1)

    def settle(total, place, h):
        span = aligned(place * 2 + h, part)
        for k in range(width // pair):
            v = total[:, pair * k : pair * (k + 1)]
            square = v * v
            lo = jnp.sum(jnp.where(low_part, square, 0.0), axis=-1, keepdims=True) / head
            hi = jnp.sum(jnp.where(low_part, 0.0, square), axis=-1, keepdims=True) / head
            scale = jnp.where(low_part, lax.rsqrt(lo + epsilon), lax.rsqrt(hi + epsilon))
            q[span, pair * k : pair * (k + 1)] = (v * scale * query_pair).astype(jnp.bfloat16)
        v = total[:, width : width + pair]
        lo = jnp.sum(jnp.where(low_part, v * v, 0.0), axis=-1, keepdims=True) / head
        both = jnp.where(low_part, v * lax.rsqrt(lo + epsilon) * key_pair, v)
        base = pl.multiple_of((place * 2 + h) * part, part)
        kv[pl.ds(base + block, part), :pair] = both.astype(jnp.bfloat16)
        kv[pl.ds(base + block, part), pair:] = pltpu.roll(both, head, 1).astype(jnp.bfloat16)
        pool[pl.ds(base + lag_rows, part), :] = total[:, width + pair :].astype(jnp.bfloat16)

    def settle_half(h):
        def one(k, carry):
            settle(acc[k, aligned(h, part), :], place_of(k), h)
            return carry

        lax.fori_loop(0, 4, one, 0)

    one_half(1, True)

    def halo(k):
        ref, rows = ((kv, block), (pool, lag_rows))[k]
        src, dst = ref.at[pl.ds(4 * count, rows), :], ref.at[pl.ds(0, rows), :]
        return remote(src, dst, h_send.at[k], h_recv.at[k], at.above())

    @pl.when(at.has_above)
    def _():
        halo(0).start()
        halo(1).start()

    @pl.when(z == 0)
    def _():
        kv[0:block, :] = jnp.zeros((block, kv.shape[1]), jnp.bfloat16)
        pool[0:lag_rows, :] = jnp.zeros((lag_rows, channels), jnp.bfloat16)

    heads = width // head
    pairs = heads // 2
    query = lax.rem(lax.broadcasted_iota(jnp.int32, (pairs * block, block), 0), block)
    key = lax.broadcasted_iota(jnp.int32, (pairs * block, block), 1)
    current = key <= query
    low_keys = lax.broadcasted_iota(jnp.int32, (2 * block, pair), 1) < head
    log2_e = 1.4426950408889634
    line = lax.broadcasted_iota(jnp.int32, (block, 1), 0)
    window = lax.shift_left(jnp.int32(2), p).astype(jnp.float32)
    slot = c * 4 + p

    def mixers(j, place):
        index = place * steps + j
        base = pl.multiple_of(index * block, block)
        first = index == 0
        kvs = kv[pl.ds(base, 2 * block), :]
        straight, turned = kvs[:, :pair], kvs[:, pair:]
        zero = jnp.zeros_like(straight)
        keys = (jnp.where(low_keys, straight, zero), jnp.where(low_keys, zero, turned))
        values = (jnp.where(low_keys, turned, zero), jnp.where(low_keys, zero, straight))
        absent = jnp.where((z == 0) & first, NEGATIVE, 0.0)
        span = aligned(place, block)
        q_pairs = [q[pl.ds(base, block), pair * k : pair * (k + 1)] for k in range(pairs)]
        q_stack = jnp.concatenate(q_pairs, axis=0)
        total = None
        for side in range(2):
            sink = jnp.concatenate(
                [
                    jnp.full((block, block), sinks[p * heads + 2 * k + side] * log2_e)
                    for k in range(pairs)
                ],
                axis=0,
            )
            scores = lax.dot_general(
                q_stack,
                keys[side],
                (((1,), (1,)), ((), ())),
                preferred_element_type=jnp.float32,
            )
            scores = jnp.where(current, scores[:, block:], scores[:, :block] + absent)
            scores = scores * (head ** (-0.5) * log2_e)
            top = jnp.maximum(jnp.max(scores, axis=-1, keepdims=True), sink)
            lifted = jnp.exp2(scores - top)
            under = jnp.sum(lifted, axis=-1, keepdims=True) + jnp.exp2(sink - top)
            weights = lifted * (1.0 / under)
            weights = jnp.concatenate(
                [jnp.where(current, 0.0, weights), jnp.where(current, weights, 0.0)], axis=1
            ).astype(jnp.bfloat16)
            term = jnp.dot(weights, values[side], preferred_element_type=jnp.float32)
            total = term if total is None else total + term
        for k in range(pairs):
            ma[slot, j, span, 2 * pair * k : 2 * pair * k + pair] = total[
                block * k : block * (k + 1)
            ].astype(jnp.bfloat16)
        series = pool[pl.ds(base, lag_rows + block), :].astype(jnp.float32)
        sums, lag = [series], 1
        while 2 * lag <= lag_rows:
            sums.append(sums[-1] + pltpu.roll(sums[-1], lag, 0))
            lag *= 2
        window_sum = sums[-1]
        for k in range(len(sums) - 2, 0, -1):
            window_sum = jnp.where(p == k - 1, sums[k], window_sum)
        position = (z * 4 * count + base + 1 + line).astype(jnp.float32)
        share = 1.0 / jnp.minimum(position, window)
        contrast = window_sum[lag_rows:] * share - series[lag_rows:]
        mixed = jnp.dot(contrast.astype(jnp.bfloat16), mix[p], preferred_element_type=jnp.float32)
        mixed = (mixed * pool_scale[:, aligned(p, channels)]).astype(jnp.bfloat16)
        for k in range(channels // pair):
            ma[slot, j, span, (2 * k + 1) * pair : (2 * k + 2) * pair] = mixed[
                :, pair * k : pair * (k + 1)
            ]

    def half_of(core, place, j, k):
        return ma.at[core * 4 + place, j, aligned(k, tall // 2), :]

    def to_mate(index, j, k, to):
        ref = half_of(c, p, j, k)
        return remote(ref, ref, m_send.at[index, j, k], m_recv.at[p, j, k], at.mate(to))

    def onward(k, j, place, to):
        ref = half_of(c, place, j, k)
        return remote(ref, ref, f_send.at[k, j], f_recv.at[k, j], at.mate(to))

    def over(index, j, place, core):
        ref = ma.at[core * 4 + place, j]
        return remote(ref, ref, d_send.at[index, j], d_recv.at[place, j], at.partner())

    def came(place, j, k):
        ref = half_of(c, place, j, k)
        remote(ref, ref, m_send.at[0, j, k], m_recv.at[place, j, k], at.partner()).wait_recv()

    def mix_step(index, carry):
        j = steps - 1 - index

        @pl.when(index == 1)
        def _():
            one_half(0, False)

        @pl.when((j == 0) & at.has_below)
        def _():
            halo(0).wait_recv()
            halo(1).wait_recv()

        def two(turn, inner):
            mixers(j, 2 * turn)
            mixers(j, 2 * turn + 1)
            for index, to in enumerate((at.xn, at.yn)):
                to_mate(index, j, turn, to).start()
            return inner

        lax.fori_loop(0, 2, two, 0)
        over(0, j, p, c).start()

        @pl.when(index == 0)
        def _():
            rows_out.pass_near()

        return carry

    lax.fori_loop(0, steps, mix_step, 0)

    def pass_on(j):
        came(at.xn, j, 0)
        onward(0, j, at.xn, at.yn).start()
        came(at.yn, j, 0)
        came(at.yn, j, 1)
        onward(1, j, at.yn, at.xn).start()
        over(2, j, at.yn, c).start()
        came(at.xn, j, 1)
        over(1, j, at.xn, c).start()

    waiting = list(range(steps - 1, -1, -1))
    total_far = 4 * (planes - 1)
    for at_step in range(total_far):
        rows_out.pass_far(at_step // 4 + 1, at_step % 4)
        passed = steps - len(waiting)
        while waiting and at_step + 1 >= (passed + 1) * total_far // (steps + 1):
            pass_on(waiting.pop(0))
            passed += 1
    for j in waiting:
        pass_on(j)
    for copy in rows_out.here():
        copy.wait()

    def landing(j, place):
        return out.at[aligned(j, block), aligned(place, columns)]

    def result(index, j, to):
        return remote(
            ys.at[j, aligned(to, block), :],
            landing(j, p),
            r_send.at[index, j],
            r_recv.at[p, j],
            at.mate(to),
        )

    def result_here(j):
        return pltpu.make_async_copy(ys.at[j, aligned(p, block), :], landing(j, p), r_local.at[j])

    def last_step(index, carry):
        j = steps - 1 - index
        for k in range(2):
            onward(k, j, at.dg, at.xn).wait_recv()
        over(3, j, at.dg, c).start()
        for place in range(4):
            over(0, j, place, 1 - c).wait_recv()
        total = None
        for i in range(8):
            first = 2 * i
            weight = ws_out[first // 4, first % 4 : first % 4 + 2].reshape(wide, columns)
            term = jnp.dot(ma[i, j], weight, preferred_element_type=jnp.float32)
            total = term if total is None else total + term
        ys[j] = total.astype(jnp.bfloat16)
        for k, to in enumerate(at.mates):
            result(k, j, to).start()
        result_here(j).start()
        return carry

    lax.fori_loop(0, steps, last_step, 0)

    def sent_step(j, carry):
        for k in range(2):
            to_mate(0, j, k, at.xn).wait_send()
            to_mate(1, j, k, at.yn).wait_send()
        onward(0, j, at.xn, at.yn).wait_send()
        onward(1, j, at.yn, at.xn).wait_send()
        for k, place in enumerate((p,) + at.mates):
            over(k, j, place, c).wait_send()
        return carry

    raw_away.wait_send()
    for index in range(6):
        tokens_to(index, *sent[index]).wait_send()
        tokens_over(index, *crossed[index], c).wait_send()

    @pl.when(at.has_above)
    def _():
        halo(0).wait_send()
        halo(1).wait_send()

    rows_in.finish()
    rows_out.finish()
    lax.fori_loop(0, steps, sent_step, 0)

    def finish_step(index, carry):
        j = steps - 1 - index
        result_here(j).wait()
        for k, to in enumerate(at.mates):
            result(k, j, to).wait_send()
            remote(
                ys.at[j, pl.ds(0, block), :],
                landing(j, to),
                r_send.at[k, j],
                r_recv.at[to, j],
                at.mate(to),
            ).wait_recv()
        return carry

    lax.fori_loop(0, steps, finish_step, 0)


def copy_kernel(src, dst, held, in_sems, out_sems):
    count = held.shape[0] // in_sems.shape[0]
    parts = [pl.ds(k * count, count) for k in range(in_sems.shape[0])]
    taken = [pltpu.make_async_copy(src.at[r], held.at[r], in_sems.at[k]) for k, r in enumerate(parts)]
    given = [pltpu.make_async_copy(held.at[r], dst.at[r], out_sems.at[k]) for k, r in enumerate(parts)]
    for copy in taken:
        copy.start()
    for take, give in zip(taken, given):
        take.wait()
        give.start()
    for copy in given:
        copy.wait()


def per_device_planes(
    tokens,
    norm_gain,
    w_query,
    w_key,
    w_value,
    w_pool_in,
    query_gain,
    key_gain,
    sinks,
    w_mix,
    pool_scale,
    w_out_attn,
    w_out_pool,
):
    planes = lax.axis_size("sp") // 4
    head = query_gain.shape[0]
    count, half = tokens.shape
    in_rows, out_rows = w_query.shape[0], 2 * w_out_attn.shape[0]
    width, channels = w_query.shape[1] // 4, w_pool_in.shape[1] // 4
    columns = w_out_attn.shape[1] // 4
    pair, deep, steps = 2 * head, 4 * in_rows, count // WINDOW
    in_width = width + pair + channels
    lines = [a.reshape(1, -1) for a in (norm_gain, query_gain, key_gain, pool_scale)]
    given = (w_key, w_value, *lines, w_mix)
    anywhere = pl.BlockSpec(memory_space=pl.ANY)
    smem = pl.BlockSpec(memory_space=pltpu.SMEM)
    dma = pltpu.SemaphoreType.DMA

    def held(*shape):
        return pltpu.VMEM(shape, jnp.bfloat16)

    row_sems = [dma((3,)), dma((3,)), dma((planes, 4)), dma((planes, 4)), dma((planes, 4))]
    result = pl.pallas_call(
        functools.partial(layer_kernel, planes, head),
        out_shape=jax.ShapeDtypeStruct(tokens.shape, jnp.bfloat16),
        in_specs=[anywhere] * 5 + [smem] + [anywhere] * 7,
        out_specs=anywhere,
        scratch_shapes=[
            held(2, count, half),
            held(4, planes, count, deep),
            held(planes, 4, in_rows, in_width),
            held(4, in_rows, pair),
            pltpu.VMEM((4, count, in_width), jnp.float32),
            held(4 * count, width),
            held(4 * count + WINDOW, 2 * pair),
            held(4 * count + longest_lag + 1, channels),
            held(8, steps, 4 * WINDOW, width + channels),
            held(planes, 4, out_rows, columns),
            held(steps, 4 * WINDOW, columns),
        ]
        + row_sems
        + row_sems
        + [dma((3,)), dma((6,)), dma((4, 2)), dma((6,)), dma((4, 2)), dma((2,)), dma((2,))]
        + [dma((2, steps, 2)), dma((4, steps, 2)), dma((2, steps)), dma((2, steps))]
        + [dma((4, steps)), dma((4, steps)), dma((3, steps)), dma((4, steps)), dma((steps,))]
        + [pltpu.VMEM(a.shape, a.dtype) for a in given]
        + [dma((len(given),))],
        compiler_params=pltpu.CompilerParams(
            collective_id=0, has_side_effects=True, vmem_limit_bytes=63 * 2**20
        ),
        name="layer",
    )(tokens, w_query, w_pool_in, w_out_attn, w_out_pool, sinks, *given)
    return pl.pallas_call(
        copy_kernel,
        out_shape=jax.ShapeDtypeStruct(tokens.shape, jnp.bfloat16),
        in_specs=[anywhere],
        out_specs=anywhere,
        scratch_shapes=[held(*tokens.shape), dma((8,)), dma((8,))],
        compiler_params=pltpu.CompilerParams(vmem_limit_bytes=63 * 2**20),
        name="hand_over",
    )(result)


def suits_planes(mesh, args):
    sp, tp = mesh.shape["sp"], mesh.shape["tp"]
    tokens, w_query, w_key, w_pool_in = args[0], args[2], args[3], args[5]
    head, groups = args[6].shape[0], args[9].shape[0]
    w_out_attn, w_out_pool = args[11], args[12]
    if tp != 2 or sp % 4 or sp < 12 or 2 * head != 128:
        return False
    share = 4 * tp
    rows = tokens.shape[0] // sp
    width, channels = w_query.shape[1] // share, w_pool_in.shape[1] // share
    held = 2 * 4 * rows * tokens.shape[1] + 2 * w_query.shape[0] * (width + 128 + channels)
    return (
        w_key.shape[1] == share * head
        and groups == share
        and rows % (4 * WINDOW) == 0
        and width % 128 == 0
        and width == channels
        and 2 * w_out_attn.shape[0] // sp == width
        and 2 * w_out_pool.shape[0] // sp == channels
        and w_out_attn.shape[0] // sp == 2 * head
        and w_query.shape[0] // sp % 16 == 0
        and w_out_attn.shape[1] % (share * 128) == 0
        and held < 22 * 2**20
    )


def solution(mesh):
    sp, tp = mesh.shape["sp"], mesh.shape["tp"]

    def call(*args):
        if suits_planes(mesh, args):
            return jax.shard_map(
                per_device_planes,
                mesh=mesh,
                in_specs=(
                    P("sp", "tp"),
                    P(),
                    P("sp", "tp"),
                    P("sp", "tp"),
                    P("sp", "tp"),
                    P("sp", "tp"),
                    P(),
                    P(),
                    P("tp"),
                    P("tp", None, None),
                    P("tp"),
                    P("sp", "tp"),
                    P("sp", "tp"),
                ),
                out_specs=P("sp", "tp"),
                check_vma=False,
            )(*args)
        kv_local = args[3].shape[1] // args[6].shape[0] // tp
        groups_local = args[9].shape[0] // tp
        fits = sp % 2 == 0 and kv_local % 2 == 0 and groups_local % 2 == 0
        pair = 2 if fits else 1
        inner = Mesh(mesh.devices.reshape(sp // pair, pair, tp), ("so", "si", "tp"))
        rows = ("so", "si")
        return jax.shard_map(
            per_device,
            mesh=inner,
            in_specs=(
                P(rows, "tp"),
                P(),
                P(rows, "tp"),
                P(rows, "tp"),
                P(rows, "tp"),
                P(rows, "tp"),
                P(),
                P(),
                P("tp"),
                P("tp", None, None),
                P("tp"),
                P(rows, "tp"),
                P(rows, "tp"),
            ),
            out_specs=P(rows, "tp"),
            check_vma=False,
        )(*args)

    return call
```
